32 devices in a mesh: sp: 8 (over z, x), dp: 4 (over y, core).
Axes of the slice: x: 2, y: 2, z: 4, core: 2. Of those that a mesh axis runs over, the one named last changes fastest.
Arguments:
- queries: bfloat16 [4, 1024, 16, 128], P('dp', 'sp'), may hold values from -3.5 to 2
- key_rows: bfloat16 [4, 1024, 16, 128], P('dp', 'sp'), may hold values from -4 to 5.3
- values: bfloat16 [4, 1024, 16, 128], P('dp', 'sp'), may hold values from -6 to 6
- residual: bfloat16 [4, 1024, 4096], P('dp', 'sp'), may hold values from -6 to 6
- out_weight: bfloat16 [2048, 4096], P(None, 'dp'), may hold values from -0.125 to 0.125
- mixer_gain: float32 [4096], replicated, may hold values from 0.1 to 1.9
- expert_gain: float32 [4096], replicated, may hold values from 0.1 to 1.9
- gate_weight: bfloat16 [32, 4096, 512], P(('sp', 'dp')), may hold values from -0.09375 to 0.09375
- up_weight: bfloat16 [32, 4096, 512], P(('sp', 'dp')), may hold values from -0.09375 to 0.09375
- expert_down_matrix: bfloat16 [32, 512, 4096], P(('sp', 'dp')), may hold values from -0.25 to 0.25
- routes: int32 [4, 1024, 2], P('dp', 'sp'), may hold values from 0 to 31, all different within a row; in each aligned block of 128 rows (0 to 127, 128 to 255, ..., all dimensions but the last counted through in order) at most 12 rows name the same one
- route_weight: float32 [4, 1024, 2], P('dp', 'sp'), may hold values from 0.1 to 1
- output_gain: float32 [4096], replicated, may hold values from 0.1 to 1.9
Outputs:
- output: bfloat16 [4, 1024, 4096], P('dp', 'sp')
The draws below stay inside these ranges and needn't reach their ends.
Inputs may be any that keep to these rules, and one draw needn't show every extreme that they name: `routes`: each row names 2 different experts. Among the rows of one device no expert is named more than 12 times, and in every draw some device names some expert exactly 12 times.
All inputs are finite; a program needn't handle non-finite values.
Results may differ from the reference program's by a relative error of at most 0.009.
Values may be sent and summed in bfloat16 or wider, within the bound.
A program may use at most 192 MiB of HBM per device.

```python
import math
import jax
import jax.numpy as jnp
import numpy as np
from jax import lax

D = 4096
HEADS = 16
HD = 128
FF = 512
TOP = 2
SEG_DEV = 128
BATCH_SEQUENCES = 4
SEQUENCE_LENGTH = 1024
EXPERTS = 32
CAP = 12
N_SP = 8
N_DP = 4


def draw_queries(key, part):
    head_key = jax.random.fold_in(key, 11)
    noise_key = jax.random.fold_in(key, 12)
    spread_key = jax.random.fold_in(key, 13)
    shape = (BATCH_SEQUENCES, SEQUENCE_LENGTH, HEADS, HD)
    slow_level = (math.log(SEQUENCE_LENGTH) + 0.5) / math.sqrt(HD)
    fast_level = (math.log(40.0) + 0.5) / math.sqrt(HD)
    fast_heads = jax.random.uniform(head_key, (HEADS,), jnp.float32) < 0.5
    noise = 0.5 * jax.random.truncated_normal(noise_key, -4.0, 4.0, shape, jnp.float32)
    spread = jax.random.uniform(spread_key, (HEADS,), jnp.float32, 0.9, 1.1)
    tier_value = -jnp.where(fast_heads, fast_level, slow_level) * spread
    return (noise + tier_value[None, None, :, None]).astype(jnp.bfloat16)


def draw_key_rows(key, part):
    noise_key = jax.random.fold_in(key, 21)
    level_key = jax.random.fold_in(key, 22)
    spike_random_key = jax.random.fold_in(key, 23)
    shape = (BATCH_SEQUENCES, SEQUENCE_LENGTH, HEADS, HD)
    blocks = SEQUENCE_LENGTH // SEG_DEV
    noise = jax.random.truncated_normal(noise_key, -4.0, 4.0, shape, jnp.float32)
    tier_value = jnp.exp(jax.random.uniform(level_key, (BATCH_SEQUENCES, blocks), jnp.float32, math.log(0.85), math.log(1.18)))
    tier_value = jnp.repeat(tier_value, SEG_DEV, axis=1)
    sudden_spike = jax.random.uniform(spike_random_key, (BATCH_SEQUENCES, SEQUENCE_LENGTH), jnp.float32) < 6.0 / SEQUENCE_LENGTH
    tier_value = jnp.where(sudden_spike, 0.1, tier_value)
    return (noise + tier_value[:, :, None, None]).astype(jnp.bfloat16)


def shard_levels(stream_key, shape, shards, smallest, largest):
    level, own = 1.0, jax.random.fold_in(stream_key, 6)
    for position, blocks in shards:
        steps = jnp.exp(jax.random.uniform(jax.random.fold_in(own, position), (blocks,), jnp.float32, smallest / len(shards), largest / len(shards)))
        level = level * jnp.repeat(steps, shape[position] // blocks).reshape([-1 if axis == position else 1 for axis in range(len(shape))])
    return level


def shared_out(stream_key, own, number, rows, count, top, limit, lean):
    order = jax.random.permutation(stream_key, count)
    heavy_load, common = load_shares(count, rows * top, limit, lean, True), load_shares(count, rows * top, limit, lean, False)
    places = jnp.arange(count)

    def named(lengths, turn):
        used = int((lengths > 0).sum())
        fixed = max(1, used // 4)
        shifted = fixed + (places - fixed + turn * (used - fixed)) % max(1, count - fixed)
        return jnp.zeros((count,), jnp.int32).at[order[jnp.where(places < fixed, places, shifted)]].set(jnp.asarray(lengths, jnp.int32))

    lengths = jnp.where(number % 4 == 0, named(heavy_load, number // 4), named(common, number - number // 4 - 1))
    mixed = jax.random.permutation(jax.random.fold_in(own, 3), count)
    source_of, taker = mixed[0:count // 2 * 2:2], mixed[1:count // 2 * 2:2]
    margin = jnp.minimum(lengths[source_of] - 1, limit - lengths[taker]) // 2
    margin = jnp.where((source_of == order[0]) | (taker == order[0]) | (lengths[taker] == 0), 0, jnp.maximum(margin, 0))
    shifted = jax.random.randint(jax.random.fold_in(own, 4), (count // 2,), 0, 1 << 20) % (margin + 1)
    lengths = lengths.at[source_of].add(-shifted).at[taker].add(shifted)
    members = jnp.searchsorted(jnp.cumsum(lengths), jnp.arange(rows * top), side="right").astype(jnp.int32)
    grid = members.reshape(top, rows).T
    grid = grid[jax.random.permutation(jax.random.fold_in(own, 1), rows)]
    turn = jax.random.randint(jax.random.fold_in(own, 2), (rows, 1), 0, top)
    return jnp.take_along_axis(grid, (jnp.arange(top)[None, :] + turn) % top, axis=1)


def load_shares(count, total, reach, slope, full):
    weights = [(1 << 20) // math.isqrt(grade ** slope) + 1 for grade in range(1, count + 1)]
    largest = reach if full else min(reach, max(-(-total // count), total * weights[0] // sum(weights)))
    least = 1 if total - largest >= count - 1 else 0
    given, rest = [largest] + [least] * (count - 1), total - largest - least * (count - 1)
    while rest > 0:
        free = [i for i in range(1, count) if given[i] < largest] or [i for i in range(1, count) if given[i] < reach]
        whole, remaining = sum([weights[i] for i in free]), rest
        for i in free:
            addition = min(reach - given[i], max(1, remaining * weights[i] // whole), rest)
            given[i] = given[i] + addition
            rest = rest - addition
    return np.array(given)


def bell_draw(own_key, dims, deviation, bound, shards=(), held_as=jnp.bfloat16):
    loudness = shard_levels(own_key, dims, shards, -0.22, 0.18) if shards else 1.0
    array = jax.random.normal(own_key, dims, jnp.float32) * deviation * loudness
    return jnp.minimum(jnp.maximum(array, -bound), bound).astype(held_as)


def setup_inputs(seed: int = 0) -> dict:
    keys = jax.random.split(jax.random.key(seed), 14)
    queries = draw_queries(jax.random.fold_in(keys[13], 71), 0)
    key_rows = draw_key_rows(jax.random.fold_in(keys[13], 71), 0)
    values = bell_draw(keys[2], (BATCH_SEQUENCES, SEQUENCE_LENGTH, HEADS, HD), 1.0, 6.0, ((0, 4), (1, 8)))
    residual = bell_draw(keys[3], (BATCH_SEQUENCES, SEQUENCE_LENGTH, D), 1.0, 6.0, ((0, 4), (1, 8)))
    out_weight = bell_draw(keys[4], (HEADS * HD, D), (HEADS * HD) ** -0.5, 0.125, ((1, 4),))
    mixer_gain = jnp.clip(1.0 + 0.18 * jax.random.normal(keys[5], (D,), jnp.float32), 0.1, 1.9)
    expert_gain = jnp.clip(1.0 + 0.18 * jax.random.normal(keys[6], (D,), jnp.float32), 0.1, 1.9)
    gate_weight = bell_draw(keys[7], (EXPERTS, D, FF), D ** -0.5, 0.09375, ((0, 32),))
    up_weight = bell_draw(keys[8], (EXPERTS, D, FF), D ** -0.5, 0.09375, ((0, 32),))
    expert_down_matrix = bell_draw(keys[9], (EXPERTS, FF, D), FF ** -0.5, 0.25, ((0, 32),))
    routes_keys = jax.random.split(jax.random.fold_in(keys[10], 1), BATCH_SEQUENCES * SEQUENCE_LENGTH // SEG_DEV)
    routes_turns = jax.random.permutation(jax.random.fold_in(keys[10], 3), BATCH_SEQUENCES * SEQUENCE_LENGTH // SEG_DEV)
    routes = jax.vmap(lambda own, number: shared_out(jax.random.fold_in(keys[10], 2), own, number, SEG_DEV, EXPERTS, TOP, CAP, 2))(routes_keys, routes_turns).reshape((BATCH_SEQUENCES, SEQUENCE_LENGTH, TOP))
    route_weight = jnp.clip(0.1 + 0.9 * jax.random.uniform(keys[11], (BATCH_SEQUENCES, SEQUENCE_LENGTH, TOP), jnp.float32) ** shard_levels(keys[11], (BATCH_SEQUENCES, SEQUENCE_LENGTH, TOP), ((0, 4), (1, 8)), -0.2, 0.2), 0.1, 1.0)
    output_gain = jnp.clip(1.0 + 0.18 * jax.random.normal(keys[12], (D,), jnp.float32), 0.1, 1.9)
    return dict(queries=queries, key_rows=key_rows, values=values, residual=residual, out_weight=out_weight, mixer_gain=mixer_gain, expert_gain=expert_gain, gate_weight=gate_weight, up_weight=up_weight, expert_down_matrix=expert_down_matrix, routes=routes, route_weight=route_weight, output_gain=output_gain)


EPSILON = 1e-06

def normed_token_rows(matrix, gain):
    return matrix * lax.rsqrt(lax.optimization_barrier(jnp.mean(matrix * matrix, axis=-1, keepdims=True)) + EPSILON) * gain

def stick_head(query_rows, key_part, value_part):
    length = query_rows.shape[0]
    block_rows = min(512, length)
    score_scale = HD ** (-0.5)
    pieces = []
    for block_index in range(length // block_rows):
        row_start = block_index * block_rows
        row_stop = row_start + block_rows
        scores = jnp.dot(query_rows[row_start:row_stop], key_part[:row_stop].T, preferred_element_type=jnp.float32) * score_scale
        key_pos = lax.broadcasted_iota(jnp.int32, (block_rows, row_stop), 1)
        query_pos = lax.broadcasted_iota(jnp.int32, (block_rows, row_stop), 0) + row_start
        is_past = key_pos < query_pos
        log_keep = jnp.where(is_past, -jax.nn.softplus(scores), jnp.float32(0.0))
        suffix = lax.cumsum(log_keep, axis=1, reverse=True) - log_keep
        weights = jnp.where(is_past, jnp.exp(jax.nn.log_sigmoid(scores) + suffix), jnp.float32(0.0)).astype(jnp.bfloat16)
        pieces.append(jnp.dot(weights, value_part[:row_stop], preferred_element_type=jnp.float32).astype(jnp.bfloat16))
    return jnp.concatenate(pieces, axis=0)

def reference(queries, key_rows, values, residual, out_weight, mixer_gain, expert_gain, gate_weight, up_weight, expert_down_matrix, routes, route_weight, output_gain):

    def by_head(tensor):
        return jnp.transpose(tensor, (0, 2, 1, 3)).reshape(BATCH_SEQUENCES * HEADS, SEQUENCE_LENGTH, HD)

    def per_pair(operands):
        return stick_head(operands[0], operands[1], operands[2])
    attended = lax.map(per_pair, (by_head(queries), by_head(key_rows), by_head(values)))
    attended = attended.reshape(BATCH_SEQUENCES, HEADS, SEQUENCE_LENGTH, HD).transpose(0, 2, 1, 3).reshape(BATCH_SEQUENCES, SEQUENCE_LENGTH, HEADS * HD)

    def token_side(operands):
        attn_rows, resid_rows = operands
        projected = jnp.dot(attn_rows, out_weight, preferred_element_type=jnp.float32)
        stream = (resid_rows.astype(jnp.float32) + normed_token_rows(projected, mixer_gain)).astype(jnp.bfloat16)
        expert_in = normed_token_rows(stream.astype(jnp.float32), expert_gain).astype(jnp.bfloat16)
        return (stream, expert_in)
    stream, expert_in = lax.map(token_side, (attended, residual))
    tokens = BATCH_SEQUENCES * SEQUENCE_LENGTH
    sources = N_SP * N_DP
    picked_experts = routes.reshape(BATCH_SEQUENCES, N_SP, SEG_DEV * TOP).astype(jnp.int32)
    onehot = (picked_experts[..., None] == jnp.arange(EXPERTS, dtype=jnp.int32)).astype(jnp.int32)
    before = jnp.cumsum(onehot, axis=2) - onehot
    slot_rank = lax.optimization_barrier(jnp.sum(before * onehot, axis=3)).astype(jnp.int32)
    source_id = jnp.arange(N_SP, dtype=jnp.int32)[None, :, None] * N_DP + jnp.arange(BATCH_SEQUENCES, dtype=jnp.int32)[:, None, None]
    token_id = jnp.arange(BATCH_SEQUENCES, dtype=jnp.int32)[:, None, None] * SEQUENCE_LENGTH + jnp.arange(N_SP, dtype=jnp.int32)[None, :, None] * SEG_DEV + jnp.arange(SEG_DEV * TOP, dtype=jnp.int32)[None, None, :] // TOP
    token_id = jnp.broadcast_to(token_id, picked_experts.shape).reshape(-1)
    dest_slot = (source_id * CAP + slot_rank).reshape(-1).astype(jnp.int32)
    expert_flat = picked_experts.reshape(-1)
    expert_slot_tokens = jnp.full((EXPERTS, sources * CAP), tokens, jnp.int32).at[expert_flat, dest_slot].set(token_id)
    padded = jnp.concatenate([expert_in.reshape(tokens, D), jnp.zeros((1, D), jnp.bfloat16)], axis=0)

    def per_expert(operands):
        token_list, gate_part, up_part, down_part = operands
        flat_rows = jnp.take(padded, token_list, axis=0)
        gate_out = jnp.dot(flat_rows, gate_part, preferred_element_type=jnp.float32)
        upward = jnp.dot(flat_rows, up_part, preferred_element_type=jnp.float32)
        hidden = (jax.nn.silu(gate_out) * upward).astype(jnp.bfloat16)
        return jnp.dot(hidden, down_part, preferred_element_type=jnp.float32).astype(jnp.bfloat16)
    served = lax.map(per_expert, (expert_slot_tokens, gate_weight, up_weight, expert_down_matrix))
    gathered = served[expert_flat, dest_slot]
    order = jnp.argsort(token_id * TOP + jnp.arange(tokens * TOP, dtype=jnp.int32) % TOP)
    gathered = gathered[order].reshape(tokens, TOP, D)
    combined = lax.optimization_barrier(jnp.sum(gathered.astype(jnp.float32) * route_weight.reshape(tokens, TOP)[:, :, None], axis=1))
    output = (stream.reshape(tokens, D).astype(jnp.float32) + normed_token_rows(combined, output_gain)).astype(jnp.bfloat16)
    return output.reshape(BATCH_SEQUENCES, SEQUENCE_LENGTH, D)
```

```python
import functools

import jax
import jax.numpy as jnp
from jax import lax
from jax.experimental import pallas as pl
from jax.experimental.pallas import tpu as pltpu
from jax.sharding import PartitionSpec as P

EPSILON = 1e-06
MESH = pl.DeviceIdType.MESH
VMEM_LIMIT = 56 * 1024 * 1024


def normed_token_rows(matrix, gain):
    return matrix * lax.rsqrt(jnp.mean(matrix * matrix, axis=-1, keepdims=True) + EPSILON) * gain


def peer_id(axes, sizes, flat):
    if len(axes) == 1:
        return {axes[0]: flat}
    return {axes[0]: lax.div(flat, sizes[1]), axes[1]: lax.rem(flat, sizes[1])}


def exchange_kernel(axes, sizes, n, count, *refs):
    ins, outs = refs[:count], refs[count : 2 * count]
    stages = refs[2 * count : 3 * count]
    send_sem, recv_sem, local_sem = refs[3 * count :]
    me = lax.axis_index(axes[0])
    if len(axes) == 2:
        me = me * sizes[1] + lax.axis_index(axes[1])

    barrier = pltpu.get_barrier_semaphore()

    def greet(k, carry):
        pl.semaphore_signal(
            barrier, inc=1, device_id=peer_id(axes, sizes, lax.rem(me + k, n)), device_id_type=MESH
        )
        return carry

    lax.fori_loop(1, n, greet, 0)
    loads = [
        pltpu.make_async_copy(ins[a].at[me], stages[a], local_sem.at[a]) for a in range(count)
    ]
    for load in loads:
        load.start()
    pl.semaphore_wait(barrier, n - 1)

    def copies(k):
        target = lax.rem(me + k, n)
        return [
            pltpu.make_async_remote_copy(
                src_ref=ins[a].at[target],
                dst_ref=outs[a].at[me],
                send_sem=send_sem.at[a, k],
                recv_sem=recv_sem.at[a, k],
                device_id=peer_id(axes, sizes, target),
                device_id_type=MESH,
            )
            for a in range(count)
        ]

    def push(i, carry):
        k = n // 2 + (1 - 2 * lax.rem(i, 2)) * lax.div(i + 1, 2)
        for copy in copies(k):
            copy.start()
        return carry

    lax.fori_loop(0, n - 1, push, 0)
    stores = [
        pltpu.make_async_copy(stages[a], outs[a].at[me], local_sem.at[a]) for a in range(count)
    ]
    for load in loads:
        load.wait()
    for store in stores:
        store.start()
    for store in stores:
        store.wait()

    def finish(k, carry):
        for copy in copies(k):
            copy.wait()
        return carry

    lax.fori_loop(1, n, finish, 0)


def exchange(arrays, axes, collective_id):
    sizes = [lax.axis_size(a) for a in axes]
    n = arrays[0].shape[0]
    count = len(arrays)
    moved = sum(a.size * 2 for a in arrays)
    return pl.pallas_call(
        functools.partial(exchange_kernel, axes, sizes, n, count),
        out_shape=[jax.ShapeDtypeStruct(a.shape, a.dtype) for a in arrays],
        in_specs=[pl.BlockSpec(memory_space=pl.ANY)] * count,
        out_specs=[pl.BlockSpec(memory_space=pl.ANY)] * count,
        scratch_shapes=[pltpu.VMEM(a.shape[1:], a.dtype) for a in arrays]
        + [
            pltpu.SemaphoreType.DMA((count, n)),
            pltpu.SemaphoreType.DMA((count, n)),
            pltpu.SemaphoreType.DMA((count,)),
        ],
        compiler_params=pltpu.CompilerParams(
            collective_id=collective_id, has_side_effects=True, vmem_limit_bytes=VMEM_LIMIT
        ),
        cost_estimate=pl.CostEstimate(flops=0, bytes_accessed=moved * 20, transcendentals=0),
    )(*arrays)


CHUNKS = 8
RELAYED = 3
DIRECT = 2


def front_kernel(sp, dp, groups, *refs):
    q_ref, k_ref, v_ref, weight_ref, resid_ref, mixer_ref, expert_ref, pick_ref = refs[:8]
    stream_ref = refs[8]
    sent_refs = refs[9 : 9 + groups]
    (
        stage, arrived, out_heads, in_heads, flat, full, projected, tokens,
        q_send, q_recv, a_send, a_recv, near_sem, far_send, far_recv, relay_send, relay_recv,
        twin_send, twin_recv, last_send, last_recv, local_sem,
    ) = refs[9 + groups :]
    rows, heads, width = q_ref.shape
    local_heads = heads // sp
    depth, columns = weight_ref.shape
    me, mate = lax.axis_index("sp"), lax.axis_index("dp")
    parity, core = lax.rem(me, 2), lax.rem(mate, 2)
    side, twin = me + 1 - 2 * parity, mate + 1 - 2 * core
    ys = dp // 2
    own_y = lax.div(mate, 2)

    def signal(device):
        pl.semaphore_signal(barrier, inc=1, device_id=device, device_id_type=MESH)

    barrier = pltpu.get_barrier_semaphore()

    def greet_sp(k, carry):
        signal({"sp": lax.rem(me + k, sp)})
        return carry

    lax.fori_loop(1, sp, greet_sp, 0)
    signal({"dp": twin})
    for d in range(1, ys):
        signal({"dp": lax.rem(own_y + d, ys) * 2 + core})
    load = pltpu.make_async_copy(weight_ref, full.at[mate], local_sem.at[0])
    load.start()
    stage[0] = jnp.transpose(q_ref[...], (1, 0, 2))
    stage[1] = jnp.transpose(k_ref[...], (1, 0, 2))
    pl.semaphore_wait(barrier, sp - 1 + 1 + ys - 1)

    def head_copy(t, h, k):
        target = lax.rem(me + k, sp)
        return pltpu.make_async_remote_copy(
            src_ref=stage.at[t, target * local_heads + h],
            dst_ref=arrived.at[t, me, h],
            send_sem=q_send.at[t, h, k],
            recv_sem=q_recv.at[t, h, k],
            device_id={"sp": target},
            device_id_type=MESH,
        )

    def send_heads(t, h):
        def push(i, carry):
            k = sp // 2 + (1 - 2 * lax.rem(i, 2)) * lax.div(i + 1, 2)
            head_copy(t, h, k).start()
            return carry

        lax.fori_loop(0, sp - 1, push, 0)

    def finish(make, low, high):
        def body(k, carry):
            make(k).wait()
            return carry

        lax.fori_loop(low, high, body, 0)

    span = depth // CHUNKS

    def chunk(owner_parity, j):
        if j < RELAYED:
            return pl.ds(pl.multiple_of((owner_parity * (RELAYED + DIRECT) + j) * span, span), span)
        return pl.ds(j * span, span)

    def shift(src, dst, sends, recvs, index, device):
        return pltpu.make_async_remote_copy(
            src_ref=src, dst_ref=dst, send_sem=sends.at[index], recv_sem=recvs.at[index],
            device_id=device, device_id_type=MESH,
        )

    def far(d, j):
        where = chunk(parity, j)
        return shift(
            weight_ref.at[where], full.at[mate, where], far_send, far_recv, (d - 1, j),
            {"dp": lax.rem(own_y + d, ys) * 2 + core},
        )

    def relay(d, j):
        origin = lax.rem(own_y + ys - d, ys) * 2 + core
        where = chunk(parity, j)
        block = full.at[origin, where]
        return shift(block, block, relay_send, relay_recv, (d - 1, j), {"sp": side})

    def to_twin(d, j):
        origin = lax.rem(own_y + ys - d, ys) * 2 + core
        block = full.at[origin, chunk(parity, j)]
        return shift(block, block, twin_send, twin_recv, (d - 1, j), {"dp": twin})

    def to_twin_last(d, j):
        origin = lax.rem(own_y + ys - d, ys) * 2 + core
        block = full.at[origin, chunk(1 - parity, j)]
        return shift(block, block, last_send, last_recv, (d - 1, j), {"dp": twin})

    near = pltpu.make_async_remote_copy(
        src_ref=weight_ref, dst_ref=full.at[mate], send_sem=near_sem.at[0], recv_sem=near_sem.at[1],
        device_id={"dp": twin}, device_id_type=MESH,
    )
    for d in range(1, ys):
        far(d, 0).start()
    for h in range(local_heads):
        send_heads(0, h)
    for d in range(1, ys):
        for j in range(1, RELAYED + DIRECT):
            far(d, j).start()
    near.start()
    stage[2] = jnp.transpose(v_ref[...], (1, 0, 2))
    own = [
        pltpu.make_async_copy(
            stage.at[t, pl.ds(me * local_heads, local_heads)], arrived.at[t, me], local_sem.at[1 + t]
        )
        for t in range(3)
    ]
    for h in range(local_heads):
        send_heads(1, h)
    for copy in own[:2]:
        copy.start()
    for h in range(local_heads):
        send_heads(2, h)
    own[2].start()

    block = rows * max(1, min(sp, 256 // rows))
    per = block // rows
    length = sp * rows
    scale = width ** (-0.5)
    tri_row = lax.broadcasted_iota(jnp.int32, (block, block), 0)
    tri_col = lax.broadcasted_iota(jnp.int32, (block, block), 1)
    suffix_ones = (tri_row >= tri_col).astype(jnp.bfloat16)
    is_past = tri_col < tri_row

    def answer(h, target):
        return pltpu.make_async_remote_copy(
            src_ref=out_heads.at[h, target],
            dst_ref=in_heads.at[me, h],
            send_sem=a_send.at[h, target],
            recv_sem=a_recv.at[h, me],
            device_id={"sp": target},
            device_id_type=MESH,
        )

    def expect(h, source):
        return pltpu.make_async_remote_copy(
            src_ref=out_heads.at[h, source],
            dst_ref=in_heads.at[source, h],
            send_sem=a_send.at[h, source],
            recv_sem=a_recv.at[h, source],
            device_id={"sp": source},
            device_id_type=MESH,
        )

    def attend_head(h):
        def piece(t, index):
            return arrived[t, index * per : (index + 1) * per, h].reshape(block, width)

        for q_block in range(length // block):
            query = piece(0, q_block)
            total = jnp.zeros((block, width), jnp.float32)
            later = jnp.zeros((block, 1), jnp.float32)
            for k_block in range(q_block, -1, -1):
                scores = (
                    lax.dot_general(
                        query, piece(1, k_block), (((1,), (1,)), ((), ())),
                        preferred_element_type=jnp.float32,
                    )
                    * scale
                )
                soft = jnp.maximum(scores, 0.0) + jnp.log(1.0 + jnp.exp(-jnp.abs(scores)))
                if k_block == q_block:
                    soft = jnp.where(is_past, soft, 0.0)
                high = soft.astype(jnp.bfloat16)
                low = (soft - high.astype(jnp.float32)).astype(jnp.bfloat16)
                suffix = jnp.dot(high, suffix_ones, preferred_element_type=jnp.float32) + jnp.dot(
                    low, suffix_ones, preferred_element_type=jnp.float32
                )
                weights = jnp.exp(scores - suffix - later)
                if k_block == q_block:
                    weights = jnp.where(is_past, weights, 0.0)
                total = total + jnp.dot(
                    weights.astype(jnp.bfloat16), piece(2, k_block), preferred_element_type=jnp.float32
                )
                if k_block > 0:
                    later = later + suffix[:, :1]
            out_heads[h, q_block * per : (q_block + 1) * per] = total.astype(jnp.bfloat16).reshape(
                per, rows, width
            )

    def send_answers(h):
        def push(k, carry):
            answer(h, lax.rem(me + k, sp)).start()
            return carry

        lax.fori_loop(1, sp, push, 0)
        pltpu.make_async_copy(out_heads.at[h, me], in_heads.at[me, h], local_sem.at[4 + h]).start()

    def pass_on(j):
        for d in range(1, ys):
            far(d, j).wait_recv()
            if j < RELAYED:
                relay(d, j).start()
            to_twin(d, j).start()

    def pass_last(j):
        for d in range(1, ys):
            pltpu.make_async_remote_copy(
                src_ref=full.at[0, chunk(1 - parity, j)],
                dst_ref=full.at[0, chunk(1 - parity, j)],
                send_sem=relay_send.at[d - 1, j], recv_sem=relay_recv.at[d - 1, j],
                device_id={"sp": side}, device_id_type=MESH,
            ).wait_recv()
            to_twin_last(d, j).start()

    pass_on(0)
    for h in range(local_heads):
        if h == 0:
            for copy in own:
                copy.wait()
        for t in range(3):
            finish(lambda k: head_copy(t, h, k), 1, sp)
        attend_head(h)
        send_answers(h)
        if h == 0:
            pass_on(1)
    pass_last(0)
    pass_on(2)
    pass_last(1)
    for j in range(RELAYED, RELAYED + DIRECT):
        pass_on(j)
        if j == RELAYED:
            pass_last(2)

    for h in range(local_heads):
        finish(lambda k: expect(h, lax.rem(me + k, sp)), 1, sp)
        pltpu.make_async_copy(out_heads.at[h, me], in_heads.at[me, h], local_sem.at[4 + h]).wait()
    for source in range(sp):
        for h in range(local_heads):
            place = (source * local_heads + h) * width
            flat[:, place : place + width] = in_heads[source, h]
    load.wait()
    near.wait()
    for d in range(1, ys):
        for j in range(RELAYED + DIRECT):
            far(d, j).wait_send()
            to_twin(d, j).wait()
            if j < RELAYED:
                relay(d, j).wait_send()
                to_twin_last(d, j).wait()

    tile = min(columns, 512)
    many = columns // tile

    @pl.loop(0, dp * many)
    def _(i):
        inner = pl.ds(pl.multiple_of(lax.rem(i, many) * tile, tile), tile)
        outer = pl.ds(pl.multiple_of(i * tile, tile), tile)
        projected[:, outer] = jnp.dot(
            flat[...], full[lax.div(i, many), :, inner], preferred_element_type=jnp.float32
        )

    @pl.loop(0, rows // 16)
    def _(i):
        part = pl.ds(pl.multiple_of(i * 16, 16), 16)
        stream = (
            resid_ref[part].astype(jnp.float32) + normed_token_rows(projected[part], mixer_ref[...])
        ).astype(jnp.bfloat16)
        stream_ref[part] = stream
        tokens[part] = normed_token_rows(stream.astype(jnp.float32), expert_ref[...]).astype(jnp.bfloat16)

    features = projected.shape[1]

    @pl.loop(0, features // 512)
    def _(i):
        part = pl.ds(pl.multiple_of(i * 512, 512), 512)
        row = 0
        for ref in sent_refs:
            many_rows = ref.shape[0] * ref.shape[1]
            ref[:, :, part] = (
                jnp.dot(pick_ref[row : row + many_rows], tokens[:, part], preferred_element_type=jnp.float32)
                .astype(jnp.bfloat16)
                .reshape(ref.shape[0], ref.shape[1], 512)
            )
            row += many_rows


def front(query, key, value, weight, residual, mixer_gain, expert_gain, pick, experts, groups):
    sp, dp = lax.axis_size("sp"), lax.axis_size("dp")
    rows, heads, width = query.shape
    depth, columns = weight.shape
    features = residual.shape[1]
    local_heads = heads // sp
    ys = max(dp // 2 - 1, 1)
    whole = pl.BlockSpec(memory_space=pltpu.VMEM)
    dma = pltpu.SemaphoreType.DMA
    bf16 = jnp.bfloat16
    return pl.pallas_call(
        functools.partial(front_kernel, sp, dp, len(groups)),
        out_shape=[jax.ShapeDtypeStruct((rows, features), bf16)]
        + [jax.ShapeDtypeStruct((experts, g, features), bf16) for g in groups],
        in_specs=[whole] * 3 + [pl.BlockSpec(memory_space=pl.ANY)] + [whole] * 4,
        out_specs=[whole] * (1 + len(groups)),
        scratch_shapes=[
            pltpu.VMEM((3, heads, rows, width), bf16),
            pltpu.VMEM((3, sp, local_heads, rows, width), bf16),
            pltpu.VMEM((local_heads, sp, rows, width), bf16),
            pltpu.VMEM((sp, local_heads, rows, width), bf16),
            pltpu.VMEM((rows, depth), bf16),
            pltpu.VMEM((dp, depth, columns), bf16),
            pltpu.VMEM((rows, features), jnp.float32),
            pltpu.VMEM((rows, features), bf16),
            dma((3, local_heads, sp)),
            dma((3, local_heads, sp)),
            dma((local_heads, sp)),
            dma((local_heads, sp)),
            dma((2,)),
            dma((ys, RELAYED + DIRECT)),
            dma((ys, RELAYED + DIRECT)),
            dma((ys, RELAYED)),
            dma((ys, RELAYED)),
            dma((ys, RELAYED + DIRECT)),
            dma((ys, RELAYED + DIRECT)),
            dma((ys, RELAYED)),
            dma((ys, RELAYED)),
            dma((4 + local_heads,)),
        ],
        compiler_params=pltpu.CompilerParams(
            collective_id=0, has_side_effects=True, vmem_limit_bytes=VMEM_LIMIT
        ),
    )(query, key, value, weight, residual, mixer_gain[None], expert_gain[None], pick)


def expert_kernel(count, *refs):
    ins, (gate_ref, up_ref, down_ref) = refs[:count], refs[count : count + 3]
    outs = refs[count + 3 :]
    for a in range(count):
        rows = ins[a][...]
        gate = jnp.dot(rows, gate_ref[...], preferred_element_type=jnp.float32)
        upward = jnp.dot(rows, up_ref[...], preferred_element_type=jnp.float32)
        hidden = (gate / (1.0 + jnp.exp(-gate)) * upward).astype(jnp.bfloat16)
        outs[a][...] = jnp.dot(
            hidden, down_ref[...], preferred_element_type=jnp.float32
        ).astype(jnp.bfloat16)


def serve(arrays, gate, up, down):
    return pl.pallas_call(
        functools.partial(expert_kernel, len(arrays)),
        out_shape=[jax.ShapeDtypeStruct(a.shape, a.dtype) for a in arrays],
        in_specs=[pl.BlockSpec(memory_space=pltpu.VMEM)] * (len(arrays) + 3),
        out_specs=[pl.BlockSpec(memory_space=pltpu.VMEM)] * len(arrays),
        compiler_params=pltpu.CompilerParams(vmem_limit_bytes=VMEM_LIMIT),
    )(*arrays, gate, up, down)


def combine_kernel(count, *refs):
    ins = refs[:count]
    high_ref, low_ref, stream_ref, gain_ref, out_ref = refs[count:]
    combined, row = 0.0, 0
    for ref in ins:
        many = ref.shape[0]
        for share in (high_ref, low_ref):
            combined = combined + jnp.dot(
                share[:, row : row + many], ref[...], preferred_element_type=jnp.float32
            )
        row += many
    out_ref[...] = (
        stream_ref[...].astype(jnp.float32) + normed_token_rows(combined, gain_ref[...])
    ).astype(jnp.bfloat16)


def combine(arrays, high, low, stream, gain):
    return pl.pallas_call(
        functools.partial(combine_kernel, len(arrays)),
        out_shape=jax.ShapeDtypeStruct(stream.shape, jnp.bfloat16),
        in_specs=[pl.BlockSpec(memory_space=pltpu.VMEM)] * (len(arrays) + 4),
        out_specs=pl.BlockSpec(memory_space=pltpu.VMEM),
        compiler_params=pltpu.CompilerParams(vmem_limit_bytes=VMEM_LIMIT),
    )(*arrays, high, low, stream, gain[None])


def local(
    queries,
    key_rows,
    values,
    residual,
    out_weight,
    mixer_gain,
    expert_gain,
    gate_weight,
    up_weight,
    expert_down_matrix,
    routes,
    route_weight,
    output_gain,
):
    sp = lax.axis_size("sp")
    _, local_rows, heads, width = queries.shape
    features = residual.shape[2]

    dp = lax.axis_size("dp")
    experts = sp * dp
    top_count = routes.shape[2]
    capacity = max(2, 3 * local_rows // experts)
    picked = routes[0].reshape(local_rows * top_count)
    onehot = (
        picked[:, None] == lax.broadcasted_iota(jnp.int32, (picked.shape[0], experts), 1)
    ).astype(jnp.bfloat16)
    count = picked.shape[0]
    earlier = (
        lax.broadcasted_iota(jnp.int32, (count, count), 1)
        < lax.broadcasted_iota(jnp.int32, (count, count), 0)
    ).astype(jnp.bfloat16)
    before = jnp.dot(earlier, onehot, preferred_element_type=jnp.float32)
    rank = jnp.sum(before * onehot.astype(jnp.float32), axis=1).astype(jnp.int32)
    groups = [g for g in (capacity // 8 * 8, capacity % 8) if g]
    splits = [g * experts for g in groups]
    slot, first, base = jnp.full((count,), -1, jnp.int32), 0, 0
    for g in groups:
        inside = (rank >= first) & (rank < first + g)
        slot = jnp.where(inside, base + picked * g + rank - first, slot)
        first, base = first + g, base + g * experts
    slot = slot.reshape(local_rows, top_count)
    slot_ids = lax.broadcasted_iota(jnp.int32, (local_rows, base), 1)
    hits = [slot[:, k : k + 1] == slot_ids for k in range(top_count)]
    pick = functools.reduce(jnp.logical_or, hits).astype(jnp.bfloat16).T
    share = sum(jnp.where(hits[k], route_weight[0][:, k : k + 1], 0.0) for k in range(top_count))
    share_high = share.astype(jnp.bfloat16)
    share_low = (share - share_high.astype(jnp.float32)).astype(jnp.bfloat16)

    stream, *outgoing = front(
        queries[0], key_rows[0], values[0], out_weight, residual[0], mixer_gain, expert_gain, pick, experts, groups
    )

    def blocks(arrays):
        return [a.reshape(experts, g, features) for a, g in zip(arrays, groups)]

    def flat(arrays):
        return [a.reshape(-1, features) for a in arrays]

    arrived = exchange(outgoing, ("sp", "dp"), 2)
    results = serve(flat(arrived), gate_weight[0], up_weight[0], expert_down_matrix[0])
    returned = exchange(blocks(results), ("sp", "dp"), 3)
    output = combine(flat(returned), share_high, share_low, stream, output_gain)
    return output[None]


def solution(mesh):
    in_specs = (
        P("dp", "sp", None, None),
        P("dp", "sp", None, None),
        P("dp", "sp", None, None),
        P("dp", "sp", None),
        P(None, "dp"),
        P(),
        P(),
        P(("sp", "dp"), None, None),
        P(("sp", "dp"), None, None),
        P(("sp", "dp"), None, None),
        P("dp", "sp", None),
        P("dp", "sp", None),
        P(),
    )
    out_specs = P("dp", "sp", None)
    return jax.shard_map(local, mesh=mesh, in_specs=in_specs, out_specs=out_specs, check_vma=False)
```

```python
import functools

import jax
import jax.numpy as jnp
from jax import lax
from jax.experimental import pallas as pl
from jax.experimental.pallas import tpu as pltpu
from jax.sharding import PartitionSpec as P

EPSILON = 1e-06
MESH = pl.DeviceIdType.MESH
VMEM_LIMIT = 56 * 1024 * 1024


def normed_token_rows(matrix, gain):
    return matrix * lax.rsqrt(jnp.mean(matrix * matrix, axis=-1, keepdims=True) + EPSILON) * gain


def peer_id(axes, sizes, flat):
    if len(axes) == 1:
        return {axes[0]: flat}
    return {axes[0]: lax.div(flat, sizes[1]), axes[1]: lax.rem(flat, sizes[1])}


CHUNKS = 8
RELAYED = 3
DIRECT = 2


def front_kernel(sp, dp, groups, *refs):
    q_ref, k_ref, v_ref, weight_ref, resid_ref, mixer_ref, expert_ref, pick_ref = refs[:8]
    stream_ref = refs[8]
    sent_refs = refs[9 : 9 + groups]
    (
        stage, arrived, out_heads, in_heads, flat, full, projected, tokens,
        q_send, q_recv, a_send, a_recv, near_sem, far_send, far_recv, relay_send, relay_recv,
        twin_send, twin_recv, last_send, last_recv, local_sem,
    ) = refs[9 + groups :]
    rows, heads, width = q_ref.shape
    local_heads = heads // sp
    depth, columns = weight_ref.shape
    me, mate = lax.axis_index("sp"), lax.axis_index("dp")
    parity, core = lax.rem(me, 2), lax.rem(mate, 2)
    side, twin = me + 1 - 2 * parity, mate + 1 - 2 * core
    ys = dp // 2
    own_y = lax.div(mate, 2)

    def signal(device):
        pl.semaphore_signal(barrier, inc=1, device_id=device, device_id_type=MESH)

    barrier = pltpu.get_barrier_semaphore()

    def greet_sp(k, carry):
        signal({"sp": lax.rem(me + k, sp)})
        return carry

    lax.fori_loop(1, sp, greet_sp, 0)
    signal({"dp": twin})
    for d in range(1, ys):
        signal({"dp": lax.rem(own_y + d, ys) * 2 + core})
    load = pltpu.make_async_copy(weight_ref, full.at[mate], local_sem.at[0])
    load.start()
    stage[0] = jnp.transpose(q_ref[...], (1, 0, 2))
    stage[1] = jnp.transpose(k_ref[...], (1, 0, 2))
    pl.semaphore_wait(barrier, sp - 1 + 1 + ys - 1)

    def head_copy(t, h, k):
        target = lax.rem(me + k, sp)
        return pltpu.make_async_remote_copy(
            src_ref=stage.at[t, target * local_heads + h],
            dst_ref=arrived.at[t, me, h],
            send_sem=q_send.at[t, h, k],
            recv_sem=q_recv.at[t, h, k],
            device_id={"sp": target},
            device_id_type=MESH,
        )

    def send_heads(t, h):
        def push(i, carry):
            k = sp // 2 + (1 - 2 * lax.rem(i, 2)) * lax.div(i + 1, 2)
            head_copy(t, h, k).start()
            return carry

        lax.fori_loop(0, sp - 1, push, 0)

    def finish(make, low, high):
        def body(k, carry):
            make(k).wait()
            return carry

        lax.fori_loop(low, high, body, 0)

    span = depth // CHUNKS

    def chunk(owner_parity, j):
        if j < RELAYED:
            return pl.ds(pl.multiple_of((owner_parity * (RELAYED + DIRECT) + j) * span, span), span)
        return pl.ds(j * span, span)

    def shift(src, dst, sends, recvs, index, device):
        return pltpu.make_async_remote_copy(
            src_ref=src, dst_ref=dst, send_sem=sends.at[index], recv_sem=recvs.at[index],
            device_id=device, device_id_type=MESH,
        )

    def far(d, j):
        where = chunk(parity, j)
        return shift(
            weight_ref.at[where], full.at[mate, where], far_send, far_recv, (d - 1, j),
            {"dp": lax.rem(own_y + d, ys) * 2 + core},
        )

    def relay(d, j):
        origin = lax.rem(own_y + ys - d, ys) * 2 + core
        where = chunk(parity, j)
        block = full.at[origin, where]
        return shift(block, block, relay_send, relay_recv, (d - 1, j), {"sp": side})

    def to_twin(d, j):
        origin = lax.rem(own_y + ys - d, ys) * 2 + core
        block = full.at[origin, chunk(parity, j)]
        return shift(block, block, twin_send, twin_recv, (d - 1, j), {"dp": twin})

    def to_twin_last(d, j):
        origin = lax.rem(own_y + ys - d, ys) * 2 + core
        block = full.at[origin, chunk(1 - parity, j)]
        return shift(block, block, last_send, last_recv, (d - 1, j), {"dp": twin})

    near = pltpu.make_async_remote_copy(
        src_ref=weight_ref, dst_ref=full.at[mate], send_sem=near_sem.at[0], recv_sem=near_sem.at[1],
        device_id={"dp": twin}, device_id_type=MESH,
    )
    for d in range(1, ys):
        far(d, 0).start()
    for h in range(local_heads):
        send_heads(0, h)
    for d in range(1, ys):
        for j in range(1, RELAYED + DIRECT):
            far(d, j).start()
    near.start()
    stage[2] = jnp.transpose(v_ref[...], (1, 0, 2))
    own = [
        pltpu.make_async_copy(
            stage.at[t, pl.ds(me * local_heads, local_heads)], arrived.at[t, me], local_sem.at[1 + t]
        )
        for t in range(3)
    ]
    for h in range(local_heads):
        send_heads(1, h)
    for copy in own[:2]:
        copy.start()
    for h in range(local_heads):
        send_heads(2, h)
    own[2].start()

    block = rows * max(1, min(sp, 256 // rows))
    per = block // rows
    length = sp * rows
    scale = width ** (-0.5)
    tri_row = lax.broadcasted_iota(jnp.int32, (block, block), 0)
    tri_col = lax.broadcasted_iota(jnp.int32, (block, block), 1)
    suffix_ones = (tri_row >= tri_col).astype(jnp.bfloat16)
    is_past = tri_col < tri_row

    def answer(h, target):
        return pltpu.make_async_remote_copy(
            src_ref=out_heads.at[h, target],
            dst_ref=in_heads.at[me, h],
            send_sem=a_send.at[h, target],
            recv_sem=a_recv.at[h, me],
            device_id={"sp": target},
            device_id_type=MESH,
        )

    def expect(h, source):
        return pltpu.make_async_remote_copy(
            src_ref=out_heads.at[h, source],
            dst_ref=in_heads.at[source, h],
            send_sem=a_send.at[h, source],
            recv_sem=a_recv.at[h, source],
            device_id={"sp": source},
            device_id_type=MESH,
        )

    def attend_head(h):
        def piece(t, index):
            return arrived[t, index * per : (index + 1) * per, h].reshape(block, width)

        for q_block in range(length // block):
            query = piece(0, q_block)
            total = jnp.zeros((block, width), jnp.float32)
            later = jnp.zeros((block, 1), jnp.float32)
            for k_block in range(q_block, -1, -1):
                scores = (
                    lax.dot_general(
                        query, piece(1, k_block), (((1,), (1,)), ((), ())),
                        preferred_element_type=jnp.float32,
                    )
                    * scale
                )
                soft = jnp.maximum(scores, 0.0) + jnp.log(1.0 + jnp.exp(-jnp.abs(scores)))
                if k_block == q_block:
                    soft = jnp.where(is_past, soft, 0.0)
                high = soft.astype(jnp.bfloat16)
                low = (soft - high.astype(jnp.float32)).astype(jnp.bfloat16)
                suffix = jnp.dot(high, suffix_ones, preferred_element_type=jnp.float32) + jnp.dot(
                    low, suffix_ones, preferred_element_type=jnp.float32
                )
                weights = jnp.exp(scores - suffix - later)
                if k_block == q_block:
                    weights = jnp.where(is_past, weights, 0.0)
                total = total + jnp.dot(
                    weights.astype(jnp.bfloat16), piece(2, k_block), preferred_element_type=jnp.float32
                )
                if k_block > 0:
                    later = later + suffix[:, :1]
            out_heads[h, q_block * per : (q_block + 1) * per] = total.astype(jnp.bfloat16).reshape(
                per, rows, width
            )

    def send_answers(h):
        def push(k, carry):
            answer(h, lax.rem(me + k, sp)).start()
            return carry

        lax.fori_loop(1, sp, push, 0)
        pltpu.make_async_copy(out_heads.at[h, me], in_heads.at[me, h], local_sem.at[4 + h]).start()

    def pass_on(j):
        for d in range(1, ys):
            far(d, j).wait_recv()
            if j < RELAYED:
                relay(d, j).start()
            to_twin(d, j).start()

    def pass_last(j):
        for d in range(1, ys):
            pltpu.make_async_remote_copy(
                src_ref=full.at[0, chunk(1 - parity, j)],
                dst_ref=full.at[0, chunk(1 - parity, j)],
                send_sem=relay_send.at[d - 1, j], recv_sem=relay_recv.at[d - 1, j],
                device_id={"sp": side}, device_id_type=MESH,
            ).wait_recv()
            to_twin_last(d, j).start()

    pass_on(0)
    for h in range(local_heads):
        if h == 0:
            for copy in own:
                copy.wait()
        for t in range(3):
            finish(lambda k: head_copy(t, h, k), 1, sp)
        attend_head(h)
        send_answers(h)
        if h == 0:
            pass_on(1)
    pass_last(0)
    pass_on(2)
    pass_last(1)
    for j in range(RELAYED, RELAYED + DIRECT):
        pass_on(j)
        if j == RELAYED:
            pass_last(2)

    for h in range(local_heads):
        finish(lambda k: expect(h, lax.rem(me + k, sp)), 1, sp)
        pltpu.make_async_copy(out_heads.at[h, me], in_heads.at[me, h], local_sem.at[4 + h]).wait()
    for source in range(sp):
        for h in range(local_heads):
            place = (source * local_heads + h) * width
            flat[:, place : place + width] = in_heads[source, h]
    load.wait()
    near.wait()
    for d in range(1, ys):
        for j in range(RELAYED + DIRECT):
            far(d, j).wait_send()
            to_twin(d, j).wait()
            if j < RELAYED:
                relay(d, j).wait_send()
                to_twin_last(d, j).wait()

    tile = min(columns, 512)
    many = columns // tile

    @pl.loop(0, dp * many)
    def _(i):
        inner = pl.ds(pl.multiple_of(lax.rem(i, many) * tile, tile), tile)
        outer = pl.ds(pl.multiple_of(i * tile, tile), tile)
        projected[:, outer] = jnp.dot(
            flat[...], full[lax.div(i, many), :, inner], preferred_element_type=jnp.float32
        )

    @pl.loop(0, rows // 16)
    def _(i):
        part = pl.ds(pl.multiple_of(i * 16, 16), 16)
        stream = (
            resid_ref[part].astype(jnp.float32) + normed_token_rows(projected[part], mixer_ref[...])
        ).astype(jnp.bfloat16)
        stream_ref[part] = stream
        tokens[part] = normed_token_rows(stream.astype(jnp.float32), expert_ref[...]).astype(jnp.bfloat16)

    features = projected.shape[1]

    @pl.loop(0, features // 512)
    def _(i):
        part = pl.ds(pl.multiple_of(i * 512, 512), 512)
        row = 0
        for ref in sent_refs:
            many_rows = ref.shape[0] * ref.shape[1]
            ref[:, :, part] = (
                jnp.dot(pick_ref[row : row + many_rows], tokens[:, part], preferred_element_type=jnp.float32)
                .astype(jnp.bfloat16)
                .reshape(ref.shape[0], ref.shape[1], 512)
            )
            row += many_rows


def front(query, key, value, weight, residual, mixer_gain, expert_gain, pick, experts, groups):
    sp, dp = lax.axis_size("sp"), lax.axis_size("dp")
    rows, heads, width = query.shape
    depth, columns = weight.shape
    features = residual.shape[1]
    local_heads = heads // sp
    ys = max(dp // 2 - 1, 1)
    whole = pl.BlockSpec(memory_space=pltpu.VMEM)
    dma = pltpu.SemaphoreType.DMA
    bf16 = jnp.bfloat16
    return pl.pallas_call(
        functools.partial(front_kernel, sp, dp, len(groups)),
        out_shape=[jax.ShapeDtypeStruct((rows, features), bf16)]
        + [jax.ShapeDtypeStruct((experts, g, features), bf16) for g in groups],
        in_specs=[whole] * 3 + [pl.BlockSpec(memory_space=pl.ANY)] + [whole] * 4,
        out_specs=[whole] * (1 + len(groups)),
        scratch_shapes=[
            pltpu.VMEM((3, heads, rows, width), bf16),
            pltpu.VMEM((3, sp, local_heads, rows, width), bf16),
            pltpu.VMEM((local_heads, sp, rows, width), bf16),
            pltpu.VMEM((sp, local_heads, rows, width), bf16),
            pltpu.VMEM((rows, depth), bf16),
            pltpu.VMEM((dp, depth, columns), bf16),
            pltpu.VMEM((rows, features), jnp.float32),
            pltpu.VMEM((rows, features), bf16),
            dma((3, local_heads, sp)),
            dma((3, local_heads, sp)),
            dma((local_heads, sp)),
            dma((local_heads, sp)),
            dma((2,)),
            dma((ys, RELAYED + DIRECT)),
            dma((ys, RELAYED + DIRECT)),
            dma((ys, RELAYED)),
            dma((ys, RELAYED)),
            dma((ys, RELAYED + DIRECT)),
            dma((ys, RELAYED + DIRECT)),
            dma((ys, RELAYED)),
            dma((ys, RELAYED)),
            dma((4 + local_heads,)),
        ],
        compiler_params=pltpu.CompilerParams(
            collective_id=0, has_side_effects=True, vmem_limit_bytes=VMEM_LIMIT
        ),
    )(query, key, value, weight, residual, mixer_gain[None], expert_gain[None], pick)


def back_kernel(axes, sizes, n, count, *refs):
    sent = refs[:count]
    gate_hbm, up_hbm, down_hbm, high_ref, low_ref, stream_ref, gain_ref, out_ref = refs[count : count + 8]
    rest = refs[count + 8 :]
    arrived, results, returned = rest[:count], rest[count : 2 * count], rest[2 * count : 3 * count]
    (
        gate_ref, up_ref, down_ref, combined,
        send_sem, recv_sem, back_send, back_recv, local_sem, weight_sem,
    ) = rest[3 * count :]
    me = lax.axis_index(axes[0]) * sizes[1] + lax.axis_index(axes[1])
    features = stream_ref.shape[1]
    tile = min(features, 512)

    barrier = pltpu.get_barrier_semaphore()

    def greet(k, carry):
        pl.semaphore_signal(
            barrier, inc=1, device_id=peer_id(axes, sizes, lax.rem(me + k, n)), device_id_type=MESH
        )
        return carry

    lax.fori_loop(1, n, greet, 0)
    loads = [pltpu.make_async_copy(sent[a].at[me], arrived[a].at[me], local_sem.at[a]) for a in range(count)]
    keeps = [
        pltpu.make_async_copy(results[a].at[me], returned[a].at[me], local_sem.at[count + a])
        for a in range(count)
    ]
    fetches = [
        pltpu.make_async_copy(src, dst, weight_sem.at[i])
        for i, (src, dst) in enumerate(((gate_hbm, gate_ref), (up_hbm, up_ref), (down_hbm, down_ref)))
    ]
    for copy in loads + fetches:
        copy.start()
    pl.semaphore_wait(barrier, n - 1)

    def move(sources, targets, sends, recvs, a, k):
        target = lax.rem(me + k, n)
        return pltpu.make_async_remote_copy(
            src_ref=sources[a].at[target],
            dst_ref=targets[a].at[me],
            send_sem=sends.at[a, k],
            recv_sem=recvs.at[a, k],
            device_id=peer_id(axes, sizes, target),
            device_id_type=MESH,
        )

    def outward(a, k):
        return move(sent, arrived, send_sem, recv_sem, a, k)

    def homeward(a, k):
        return move(results, returned, back_send, back_recv, a, k)

    def start_all(make, a):
        def push(i, carry):
            k = n // 2 + (1 - 2 * lax.rem(i, 2)) * lax.div(i + 1, 2)
            make(a, k).start()
            return carry

        lax.fori_loop(0, n - 1, push, 0)

    def wait_all(make, a):
        def body(k, carry):
            make(a, k).wait()
            return carry

        lax.fori_loop(1, n, body, 0)

    for a in range(count):
        start_all(outward, a)
    for a in range(count):
        loads[a].wait()
        wait_all(outward, a)
        if a == 0:
            for copy in fetches:
                copy.wait()
        experts, many, _ = arrived[a].shape
        rows = arrived[a][...].reshape(experts * many, features)
        gate = jnp.dot(rows, gate_ref[...], preferred_element_type=jnp.float32)
        upward = jnp.dot(rows, up_ref[...], preferred_element_type=jnp.float32)
        hidden = (gate / (1.0 + jnp.exp(-gate)) * upward).astype(jnp.bfloat16)

        for i in range(features // tile):
            part = slice(i * tile, (i + 1) * tile)
            results[a][:, :, part] = (
                jnp.dot(hidden, down_ref[:, part], preferred_element_type=jnp.float32)
                .astype(jnp.bfloat16)
                .reshape(experts, many, tile)
            )
        start_all(homeward, a)
        keeps[a].start()

    row = 0
    for a in range(count):
        keeps[a].wait()
        wait_all(homeward, a)
        experts, many, _ = returned[a].shape
        span = slice(row, row + experts * many)

        @pl.loop(0, features // tile)
        def _(i):
            part = pl.ds(pl.multiple_of(i * tile, tile), tile)
            block = returned[a][:, :, part].reshape(experts * many, tile)
            total = jnp.dot(high_ref[:, span], block, preferred_element_type=jnp.float32) + jnp.dot(
                low_ref[:, span], block, preferred_element_type=jnp.float32
            )
            combined[:, part] = total if a == 0 else combined[:, part] + total

        row += experts * many

    @pl.loop(0, stream_ref.shape[0] // 16)
    def _(i):
        part = pl.ds(pl.multiple_of(i * 16, 16), 16)
        out_ref[part] = (
            stream_ref[part].astype(jnp.float32) + normed_token_rows(combined[part], gain_ref[...])
        ).astype(jnp.bfloat16)


def back(sent, gate, up, down, high, low, stream, gain):
    axes = ("sp", "dp")
    sizes = [lax.axis_size(a) for a in axes]
    n = sent[0].shape[0]
    count = len(sent)
    whole, anywhere = pl.BlockSpec(memory_space=pltpu.VMEM), pl.BlockSpec(memory_space=pl.ANY)
    dma = pltpu.SemaphoreType.DMA
    return pl.pallas_call(
        functools.partial(back_kernel, axes, sizes, n, count),
        out_shape=jax.ShapeDtypeStruct(stream.shape, stream.dtype),
        in_specs=[anywhere] * (count + 3) + [whole] * 4,
        out_specs=whole,
        scratch_shapes=[pltpu.VMEM(a.shape, a.dtype) for _ in range(3) for a in sent]
        + [pltpu.VMEM(w.shape, w.dtype) for w in (gate, up, down)]
        + [pltpu.VMEM(stream.shape, jnp.float32)]
        + [dma((count, n))] * 4
        + [dma((2 * count,)), dma((3,))],
        compiler_params=pltpu.CompilerParams(
            collective_id=1, has_side_effects=True, vmem_limit_bytes=VMEM_LIMIT
        ),
    )(*sent, gate, up, down, high, low, stream, gain[None])


def local(
    queries,
    key_rows,
    values,
    residual,
    out_weight,
    mixer_gain,
    expert_gain,
    gate_weight,
    up_weight,
    expert_down_matrix,
    routes,
    route_weight,
    output_gain,
):
    sp = lax.axis_size("sp")
    _, local_rows, heads, width = queries.shape
    dp = lax.axis_size("dp")
    experts = sp * dp
    top_count = routes.shape[2]
    capacity = max(2, 3 * local_rows // experts)
    picked = routes[0].reshape(local_rows * top_count)
    onehot = (
        picked[:, None] == lax.broadcasted_iota(jnp.int32, (picked.shape[0], experts), 1)
    ).astype(jnp.bfloat16)
    count = picked.shape[0]
    earlier = (
        lax.broadcasted_iota(jnp.int32, (count, count), 1)
        < lax.broadcasted_iota(jnp.int32, (count, count), 0)
    ).astype(jnp.bfloat16)
    before = jnp.dot(earlier, onehot, preferred_element_type=jnp.float32)
    rank = jnp.sum(before * onehot.astype(jnp.float32), axis=1).astype(jnp.int32)
    groups = [g for g in (capacity // 8 * 8, capacity % 8) if g]
    slot, first, base = jnp.full((count,), -1, jnp.int32), 0, 0
    for g in groups:
        inside = (rank >= first) & (rank < first + g)
        slot = jnp.where(inside, base + picked * g + rank - first, slot)
        first, base = first + g, base + g * experts
    slot = slot.reshape(local_rows, top_count)
    slot_ids = lax.broadcasted_iota(jnp.int32, (local_rows, base), 1)
    hits = [slot[:, k : k + 1] == slot_ids for k in range(top_count)]
    pick = functools.reduce(jnp.logical_or, hits).astype(jnp.bfloat16).T
    share = sum(jnp.where(hits[k], route_weight[0][:, k : k + 1], 0.0) for k in range(top_count))
    share_high = share.astype(jnp.bfloat16)
    share_low = (share - share_high.astype(jnp.float32)).astype(jnp.bfloat16)

    stream, *outgoing = front(
        queries[0], key_rows[0], values[0], out_weight, residual[0], mixer_gain, expert_gain, pick, experts, groups
    )

    output = back(
        outgoing, gate_weight[0], up_weight[0], expert_down_matrix[0], share_high, share_low, stream, output_gain
    )
    return output[None]


def solution(mesh):
    in_specs = (
        P("dp", "sp", None, None),
        P("dp", "sp", None, None),
        P("dp", "sp", None, None),
        P("dp", "sp", None),
        P(None, "dp"),
        P(),
        P(),
        P(("sp", "dp"), None, None),
        P(("sp", "dp"), None, None),
        P(("sp", "dp"), None, None),
        P("dp", "sp", None),
        P("dp", "sp", None),
        P(),
    )
    out_specs = P("dp", "sp", None)
    return jax.shard_map(local, mesh=mesh, in_specs=in_specs, out_specs=out_specs, check_vma=False)
```

```python
import functools

import jax
import jax.numpy as jnp
from jax import lax
from jax.experimental import pallas as pl
from jax.experimental.pallas import tpu as pltpu
from jax.sharding import PartitionSpec as P

EPSILON = 1e-06
MESH = pl.DeviceIdType.MESH
VMEM_LIMIT = 63 * 1024 * 1024


def normed_token_rows(matrix, gain):
    return matrix * lax.rsqrt(jnp.mean(matrix * matrix, axis=-1, keepdims=True) + EPSILON) * gain


CHUNKS = 8
RELAYED = 3
DIRECT = 2


def place_slots(rows, experts, groups, routes_ref, shares_ref, pick_ref, high_ref, low_ref):
    top_count = routes_ref.shape[0]

    def column(row):
        return jnp.transpose(jnp.broadcast_to(row, (rows, rows)))[:, :1]

    lanes = lax.broadcasted_iota(jnp.int32, (rows, max(experts, 128)), 1).astype(jnp.float32)
    names = [column(routes_ref[k : k + 1].astype(jnp.float32)) for k in range(top_count)]
    shares = [column(shares_ref[k : k + 1]) for k in range(top_count)]
    marks = [jnp.where(name == lanes, 1.0, 0.0) for name in names]
    earlier = lax.broadcasted_iota(jnp.int32, (rows, rows), 1) < lax.broadcasted_iota(jnp.int32, (rows, rows), 0)
    before = jnp.dot(
        jnp.where(earlier, 1.0, 0.0).astype(jnp.bfloat16),
        sum(marks).astype(jnp.bfloat16),
        preferred_element_type=jnp.float32,
    )
    slot_ids = lax.broadcasted_iota(jnp.int32, (rows, experts * sum(groups)), 1).astype(jnp.float32)
    picked, share = 0.0, 0.0
    for k in range(top_count):
        rank = jnp.sum(before * marks[k], axis=1, keepdims=True)
        slot, first, base = jnp.full((rows, 1), -1.0, jnp.float32), 0, 0
        for g in groups:
            inside = (rank >= first) & (rank < first + g)
            slot = jnp.where(inside, base + names[k] * g + rank - first, slot)
            first, base = first + g, base + g * experts
        picked = picked + jnp.where(slot == slot_ids, 1.0, 0.0)
        share = share + jnp.where(slot == slot_ids, shares[k], 0.0)
    pick_ref[...] = jnp.transpose(picked).astype(jnp.bfloat16)
    high = share.astype(jnp.bfloat16)
    high_ref[...] = high
    low_ref[...] = (share - high.astype(jnp.float32)).astype(jnp.bfloat16)


def layer_kernel(sp, dp, count, *refs):
    (
        q_ref, k_ref, v_ref, weight_ref, resid_ref, mixer_ref, expert_ref, routes_ref, shares_ref,
        gate_hbm, up_hbm, down_hbm, gain_ref, out_ref,
    ) = refs[:14]
    boxes = refs[14 : 14 + 4 * count]
    sent, served = boxes[:count], boxes[count : 2 * count]
    results, returned = boxes[2 * count : 3 * count], boxes[3 * count :]
    (
        stage, arrived, out_heads, in_heads, flat, full, projected, tokens, stream_ref,
        pick_ref, high_ref, low_ref, gate_ref, up_ref, down_ref,
        q_send, q_recv, a_send, a_recv, near_sem, far_send, far_recv, relay_send, relay_recv,
        twin_send, twin_recv, last_send, last_recv, local_sem,
        send_sem, recv_sem, back_send, back_recv, keep_sem, fetch_sem,
    ) = refs[14 + 4 * count :]
    rows, heads, width = q_ref.shape
    local_heads = heads // sp
    depth, columns = weight_ref.shape
    me, mate = lax.axis_index("sp"), lax.axis_index("dp")
    parity, core = lax.rem(me, 2), lax.rem(mate, 2)
    side, twin = me + 1 - 2 * parity, mate + 1 - 2 * core
    ys = dp // 2
    own_y = lax.div(mate, 2)
    n, own = sp * dp, me * dp + mate

    def signal(device):
        pl.semaphore_signal(barrier, inc=1, device_id=device, device_id_type=MESH)

    barrier = pltpu.get_barrier_semaphore()

    def greet(k, carry):
        other = lax.rem(own + k, n)
        signal({"sp": lax.div(other, dp), "dp": lax.rem(other, dp)})
        return carry

    lax.fori_loop(1, n, greet, 0)
    load = pltpu.make_async_copy(weight_ref, full.at[mate], local_sem.at[0])
    load.start()
    stage[0] = jnp.transpose(q_ref[...], (1, 0, 2))
    stage[1] = jnp.transpose(k_ref[...], (1, 0, 2))
    pl.semaphore_wait(barrier, n - 1)

    def head_copy(t, h, k):
        target = lax.rem(me + k, sp)
        return pltpu.make_async_remote_copy(
            src_ref=stage.at[t, target * local_heads + h],
            dst_ref=arrived.at[t, me, h],
            send_sem=q_send.at[t, h, k],
            recv_sem=q_recv.at[t, h, k],
            device_id={"sp": target},
            device_id_type=MESH,
        )

    def send_heads(t, h):
        def push(i, carry):
            k = sp // 2 + (1 - 2 * lax.rem(i, 2)) * lax.div(i + 1, 2)
            head_copy(t, h, k).start()
            return carry

        lax.fori_loop(0, sp - 1, push, 0)

    def finish(make, low, high):
        def body(k, carry):
            make(k).wait()
            return carry

        lax.fori_loop(low, high, body, 0)

    span = depth // CHUNKS

    def chunk(owner_parity, j):
        if j < RELAYED:
            return pl.ds(pl.multiple_of((owner_parity * (RELAYED + DIRECT) + j) * span, span), span)
        return pl.ds(j * span, span)

    def shift(src, dst, sends, recvs, index, device):
        return pltpu.make_async_remote_copy(
            src_ref=src, dst_ref=dst, send_sem=sends.at[index], recv_sem=recvs.at[index],
            device_id=device, device_id_type=MESH,
        )

    def far(d, j):
        where = chunk(parity, j)
        return shift(
            weight_ref.at[where], full.at[mate, where], far_send, far_recv, (d - 1, j),
            {"dp": lax.rem(own_y + d, ys) * 2 + core},
        )

    def relay(d, j):
        origin = lax.rem(own_y + ys - d, ys) * 2 + core
        where = chunk(parity, j)
        block = full.at[origin, where]
        return shift(block, block, relay_send, relay_recv, (d - 1, j), {"sp": side})

    def to_twin(d, j):
        origin = lax.rem(own_y + ys - d, ys) * 2 + core
        block = full.at[origin, chunk(parity, j)]
        return shift(block, block, twin_send, twin_recv, (d - 1, j), {"dp": twin})

    def to_twin_last(d, j):
        origin = lax.rem(own_y + ys - d, ys) * 2 + core
        block = full.at[origin, chunk(1 - parity, j)]
        return shift(block, block, last_send, last_recv, (d - 1, j), {"dp": twin})

    near = pltpu.make_async_remote_copy(
        src_ref=weight_ref, dst_ref=full.at[mate], send_sem=near_sem.at[0], recv_sem=near_sem.at[1],
        device_id={"dp": twin}, device_id_type=MESH,
    )
    for d in range(1, ys):
        far(d, 0).start()
    send_heads(0, 0)
    send_heads(1, 0)
    for d in range(1, ys):
        for j in range(1, RELAYED + DIRECT):
            far(d, j).start()
    near.start()
    stage[2] = jnp.transpose(v_ref[...], (1, 0, 2))
    keep_heads = [
        pltpu.make_async_copy(
            stage.at[t, pl.ds(me * local_heads, local_heads)], arrived.at[t, me], local_sem.at[1 + t]
        )
        for t in range(3)
    ]
    for copy in keep_heads[:2]:
        copy.start()
    fetches = [
        pltpu.make_async_copy(src, dst, fetch_sem.at[i])
        for i, (src, dst) in enumerate(((gate_hbm, gate_ref), (up_hbm, up_ref), (down_hbm, down_ref)))
    ]
    for copy in fetches:
        copy.start()
    send_heads(2, 0)
    keep_heads[2].start()
    for h in range(1, local_heads):
        for t in range(3):
            send_heads(t, h)

    place_slots(rows, n, [box.shape[1] for box in sent], routes_ref, shares_ref, pick_ref, high_ref, low_ref)

    block = rows * max(1, min(sp, 256 // rows))
    per = block // rows
    length = sp * rows
    scale = width ** (-0.5)
    tri_row = lax.broadcasted_iota(jnp.int32, (block, block), 0)
    tri_col = lax.broadcasted_iota(jnp.int32, (block, block), 1)
    suffix_ones = (tri_row >= tri_col).astype(jnp.bfloat16)
    is_past = tri_col < tri_row

    def answer(h, target):
        return pltpu.make_async_remote_copy(
            src_ref=out_heads.at[h, target],
            dst_ref=in_heads.at[me, h],
            send_sem=a_send.at[h, target],
            recv_sem=a_recv.at[h, me],
            device_id={"sp": target},
            device_id_type=MESH,
        )

    def expect(h, source):
        return pltpu.make_async_remote_copy(
            src_ref=out_heads.at[h, source],
            dst_ref=in_heads.at[source, h],
            send_sem=a_send.at[h, source],
            recv_sem=a_recv.at[h, source],
            device_id={"sp": source},
            device_id_type=MESH,
        )

    def attend_head(h):
        def piece(t, index):
            return arrived[t, index * per : (index + 1) * per, h].reshape(block, width)

        for q_block in range(length // block):
            query = piece(0, q_block)
            total = jnp.zeros((block, width), jnp.float32)
            later = jnp.zeros((block, 1), jnp.float32)
            for k_block in range(q_block, -1, -1):
                scores = (
                    lax.dot_general(
                        query, piece(1, k_block), (((1,), (1,)), ((), ())),
                        preferred_element_type=jnp.float32,
                    )
                    * scale
                )
                soft = jnp.maximum(scores, 0.0) + jnp.log(1.0 + jnp.exp(-jnp.abs(scores)))
                if k_block == q_block:
                    soft = jnp.where(is_past, soft, 0.0)
                high = soft.astype(jnp.bfloat16)
                low = (soft - high.astype(jnp.float32)).astype(jnp.bfloat16)
                suffix = jnp.dot(high, suffix_ones, preferred_element_type=jnp.float32) + jnp.dot(
                    low, suffix_ones, preferred_element_type=jnp.float32
                )
                weights = jnp.exp(scores - suffix - later)
                if k_block == q_block:
                    weights = jnp.where(is_past, weights, 0.0)
                total = total + jnp.dot(
                    weights.astype(jnp.bfloat16), piece(2, k_block), preferred_element_type=jnp.float32
                )
                if k_block > 0:
                    later = later + suffix[:, :1]
            out_heads[h, q_block * per : (q_block + 1) * per] = total.astype(jnp.bfloat16).reshape(
                per, rows, width
            )

    def send_answers(h):
        def push(k, carry):
            answer(h, lax.rem(me + k, sp)).start()
            return carry

        lax.fori_loop(1, sp, push, 0)
        pltpu.make_async_copy(out_heads.at[h, me], in_heads.at[me, h], local_sem.at[4 + h]).start()

    def pass_on(j):
        for d in range(1, ys):
            far(d, j).wait_recv()
            if j < RELAYED:
                relay(d, j).start()
            to_twin(d, j).start()

    def pass_last(j):
        for d in range(1, ys):
            pltpu.make_async_remote_copy(
                src_ref=full.at[0, chunk(1 - parity, j)],
                dst_ref=full.at[0, chunk(1 - parity, j)],
                send_sem=relay_send.at[d - 1, j], recv_sem=relay_recv.at[d - 1, j],
                device_id={"sp": side}, device_id_type=MESH,
            ).wait_recv()
            to_twin_last(d, j).start()

    pass_on(0)
    for h in range(local_heads):
        if h == 0:
            for copy in keep_heads:
                copy.wait()
        for t in range(3):
            finish(lambda k: head_copy(t, h, k), 1, sp)
        attend_head(h)
        send_answers(h)
        if h == 0:
            pass_on(1)
    pass_on(2)
    for j in range(RELAYED - 1):
        pass_last(j)
    pass_on(RELAYED)
    pass_last(RELAYED - 1)

    for h in range(local_heads):
        finish(lambda k: expect(h, lax.rem(me + k, sp)), 1, sp)
        pltpu.make_async_copy(out_heads.at[h, me], in_heads.at[me, h], local_sem.at[4 + h]).wait()
    for source in range(sp):
        for h in range(local_heads):
            place = (source * local_heads + h) * width
            flat[:, place : place + width] = in_heads[source, h]

    def settle(j):
        for d in range(1, ys):
            far(d, j).wait_send()
            to_twin(d, j).wait()
            if j < RELAYED:
                relay(d, j).wait_send()
                to_twin_last(d, j).wait()

    load.wait()
    near.wait()
    for j in range(RELAYED + DIRECT - 1):
        settle(j)

    tile = min(columns, 512)
    many = columns // tile
    late = (RELAYED + DIRECT - 1) * span
    after = late + span

    def project(combine):
        @pl.loop(0, dp * many)
        def _(i):
            inner = pl.ds(pl.multiple_of(lax.rem(i, many) * tile, tile), tile)
            outer = pl.ds(pl.multiple_of(i * tile, tile), tile)
            combine(lax.div(i, many), inner, outer)

    def early(owner, inner, outer):
        projected[:, outer] = jnp.dot(
            flat[:, :late], full[owner, :late, inner], preferred_element_type=jnp.float32
        ) + jnp.dot(flat[:, after:], full[owner, after:, inner], preferred_element_type=jnp.float32)

    def finally_add(owner, inner, outer):
        projected[:, outer] += jnp.dot(
            flat[:, late:after], full[owner, late:after, inner], preferred_element_type=jnp.float32
        )

    project(early)
    pass_on(RELAYED + DIRECT - 1)
    settle(RELAYED + DIRECT - 1)
    project(finally_add)

    @pl.loop(0, rows // 16)
    def _(i):
        part = pl.ds(pl.multiple_of(i * 16, 16), 16)
        stream = (
            resid_ref[part].astype(jnp.float32) + normed_token_rows(projected[part], mixer_ref[...])
        ).astype(jnp.bfloat16)
        stream_ref[part] = stream
        tokens[part] = normed_token_rows(stream.astype(jnp.float32), expert_ref[...]).astype(jnp.bfloat16)

    features = projected.shape[1]
    tile = 512

    def move(sources, targets, sends, recvs, a, target, slot):
        return pltpu.make_async_remote_copy(
            src_ref=sources[a].at[target],
            dst_ref=targets[a].at[own],
            send_sem=sends.at[a, target],
            recv_sem=recvs.at[a, slot],
            device_id={"sp": lax.div(target, dp), "dp": lax.rem(target, dp)},
            device_id_type=MESH,
        )

    def outward(a, target, slot):
        return move(sent, served, send_sem, recv_sem, a, target, slot)

    def homeward(a, target, slot):
        return move(results, returned, back_send, back_recv, a, target, slot)

    def start_all(make, a, first, number):
        def push(i, carry):
            target = first + lax.rem(lax.rem(own, number) + number // 2 + i, number)

            @pl.when(target != own)
            def _():
                make(a, target, own).start()

            return carry

        lax.fori_loop(0, number, push, 0)

    def wait_all(make, a):
        def body(k, carry):
            other = lax.rem(own + k, n)
            make(a, other, other).wait()
            return carry

        lax.fori_loop(1, n, body, 0)

    half = n // 2
    far_half = (1 - lax.div(own, half)) * half
    loads = [pltpu.make_async_copy(sent[a].at[own], served[a].at[own], keep_sem.at[a]) for a in range(count)]
    keeps = [
        pltpu.make_async_copy(results[a].at[own], returned[a].at[own], keep_sem.at[count + a])
        for a in range(count)
    ]
    row = 0
    for a in range(count):
        many = sent[a].shape[1]
        for first in (far_half, half - far_half):
            wanted = pick_ref[pl.ds(pl.multiple_of(row + first * many, half * many), half * many)]

            @pl.loop(0, features // tile)
            def _(i):
                part = pl.ds(pl.multiple_of(i * tile, tile), tile)
                sent[a][pl.ds(first, half), :, part] = (
                    jnp.dot(wanted, tokens[:, part], preferred_element_type=jnp.float32)
                    .astype(jnp.bfloat16)
                    .reshape(half, many, tile)
                )

            start_all(outward, a, first, half)
        loads[a].start()
        row += n * many

    for a in range(count):
        loads[a].wait()
        wait_all(outward, a)
        if a == 0:
            for copy in fetches:
                copy.wait()
        many = served[a].shape[1]
        taken = served[a][...].reshape(n * many, features)
        gate = jnp.dot(taken, gate_ref[...], preferred_element_type=jnp.float32)
        upward = jnp.dot(taken, up_ref[...], preferred_element_type=jnp.float32)
        hidden = (gate / (1.0 + jnp.exp(-gate)) * upward).astype(jnp.bfloat16)
        for i in range(features // tile):
            part = slice(i * tile, (i + 1) * tile)
            results[a][:, :, part] = (
                jnp.dot(hidden, down_ref[:, part], preferred_element_type=jnp.float32)
                .astype(jnp.bfloat16)
                .reshape(n, many, tile)
            )
        start_all(homeward, a, far_half, half)
        start_all(homeward, a, half - far_half, half)
        keeps[a].start()

    row = 0
    for a in range(count):
        keeps[a].wait()
        wait_all(homeward, a)
        many = returned[a].shape[1]
        columns_of = slice(row, row + n * many)

        @pl.loop(0, features // tile)
        def _(i):
            part = pl.ds(pl.multiple_of(i * tile, tile), tile)
            block = returned[a][:, :, part].reshape(n * many, tile)
            total = jnp.dot(high_ref[:, columns_of], block, preferred_element_type=jnp.float32) + jnp.dot(
                low_ref[:, columns_of], block, preferred_element_type=jnp.float32
            )
            projected[:, part] = total if a == 0 else projected[:, part] + total

        row += n * many

    @pl.loop(0, rows // 16)
    def _(i):
        part = pl.ds(pl.multiple_of(i * 16, 16), 16)
        out_ref[part] = (
            stream_ref[part].astype(jnp.float32) + normed_token_rows(projected[part], gain_ref[...])
        ).astype(jnp.bfloat16)


def layer(
    query, key, value, weight, residual, mixer_gain, expert_gain, routes, shares, gate, up, down, gain, groups
):
    sp, dp = lax.axis_size("sp"), lax.axis_size("dp")
    n = sp * dp
    rows, heads, width = query.shape
    depth, columns = weight.shape
    features = residual.shape[1]
    local_heads = heads // sp
    ys = max(dp // 2 - 1, 1)
    slots = n * sum(groups)
    whole, anywhere = pl.BlockSpec(memory_space=pltpu.VMEM), pl.BlockSpec(memory_space=pl.ANY)
    dma = pltpu.SemaphoreType.DMA
    bf16 = jnp.bfloat16
    return pl.pallas_call(
        functools.partial(layer_kernel, sp, dp, len(groups)),
        out_shape=jax.ShapeDtypeStruct((rows, features), bf16),
        in_specs=[whole] * 3 + [anywhere] + [whole] * 5 + [anywhere] * 3 + [whole],
        out_specs=whole,
        scratch_shapes=[pltpu.VMEM((n, g, features), bf16) for _ in range(4) for g in groups]
        + [
            pltpu.VMEM((3, heads, rows, width), bf16),
            pltpu.VMEM((3, sp, local_heads, rows, width), bf16),
            pltpu.VMEM((local_heads, sp, rows, width), bf16),
            pltpu.VMEM((sp, local_heads, rows, width), bf16),
            pltpu.VMEM((rows, depth), bf16),
            pltpu.VMEM((dp, depth, columns), bf16),
            pltpu.VMEM((rows, features), jnp.float32),
            pltpu.VMEM((rows, features), bf16),
            pltpu.VMEM((rows, features), bf16),
            pltpu.VMEM((slots, rows), bf16),
            pltpu.VMEM((rows, slots), bf16),
            pltpu.VMEM((rows, slots), bf16),
            pltpu.VMEM(gate.shape, bf16),
            pltpu.VMEM(up.shape, bf16),
            pltpu.VMEM(down.shape, bf16),
            dma((3, local_heads, sp)),
            dma((3, local_heads, sp)),
            dma((local_heads, sp)),
            dma((local_heads, sp)),
            dma((2,)),
            dma((ys, RELAYED + DIRECT)),
            dma((ys, RELAYED + DIRECT)),
            dma((ys, RELAYED)),
            dma((ys, RELAYED)),
            dma((ys, RELAYED + DIRECT)),
            dma((ys, RELAYED + DIRECT)),
            dma((ys, RELAYED)),
            dma((ys, RELAYED)),
            dma((4 + local_heads,)),
            dma((len(groups), n)),
            dma((len(groups), n)),
            dma((len(groups), n)),
            dma((len(groups), n)),
            dma((2 * len(groups),)),
            dma((3,)),
        ],
        compiler_params=pltpu.CompilerParams(
            collective_id=0, has_side_effects=True, vmem_limit_bytes=VMEM_LIMIT
        ),
    )(
        query, key, value, weight, residual, mixer_gain[None], expert_gain[None], routes, shares,
        gate, up, down, gain[None],
    )


def local(
    queries,
    key_rows,
    values,
    residual,
    out_weight,
    mixer_gain,
    expert_gain,
    gate_weight,
    up_weight,
    expert_down_matrix,
    routes,
    route_weight,
    output_gain,
):
    local_rows = queries.shape[1]
    experts = lax.axis_size("sp") * lax.axis_size("dp")
    capacity = max(2, 3 * local_rows // experts)
    groups = [g for g in (capacity // 8 * 8, capacity % 8) if g]
    output = layer(
        queries[0], key_rows[0], values[0], out_weight, residual[0], mixer_gain, expert_gain,
        routes[0].T, route_weight[0].T, gate_weight[0], up_weight[0], expert_down_matrix[0], output_gain, groups,
    )
    return output[None]


def solution(mesh):
    in_specs = (
        P("dp", "sp", None, None),
        P("dp", "sp", None, None),
        P("dp", "sp", None, None),
        P("dp", "sp", None),
        P(None, "dp"),
        P(),
        P(),
        P(("sp", "dp"), None, None),
        P(("sp", "dp"), None, None),
        P(("sp", "dp"), None, None),
        P("dp", "sp", None),
        P("dp", "sp", None),
        P(),
    )
    out_specs = P("dp", "sp", None)
    return jax.shard_map(local, mesh=mesh, in_specs=in_specs, out_specs=out_specs, check_vma=False)
```

```python
import functools

import jax
import jax.numpy as jnp
from jax import lax
from jax.experimental import pallas as pl
from jax.experimental.pallas import tpu as pltpu
from jax.sharding import PartitionSpec as P

EPSILON = 1e-06
MESH = pl.DeviceIdType.MESH
VMEM_LIMIT = 60 * 1024 * 1024


def normed_token_rows(matrix, gain):
    return matrix * lax.rsqrt(jnp.mean(matrix * matrix, axis=-1, keepdims=True) + EPSILON) * gain


PIECES = 2


def place_slots(rows, experts, groups, routes_ref, shares_ref, pick_ref, high_ref, low_ref):
    top_count = routes_ref.shape[0]

    def column(row):
        return jnp.transpose(jnp.broadcast_to(row, (rows, rows)))[:, :1]

    lanes = lax.broadcasted_iota(jnp.int32, (rows, max(experts, 128)), 1).astype(jnp.float32)
    names = [column(routes_ref[k : k + 1].astype(jnp.float32)) for k in range(top_count)]
    shares = [column(shares_ref[k : k + 1]) for k in range(top_count)]
    marks = [jnp.where(name == lanes, 1.0, 0.0) for name in names]
    earlier = lax.broadcasted_iota(jnp.int32, (rows, rows), 1) < lax.broadcasted_iota(jnp.int32, (rows, rows), 0)
    before = jnp.dot(
        jnp.where(earlier, 1.0, 0.0).astype(jnp.bfloat16),
        sum(marks).astype(jnp.bfloat16),
        preferred_element_type=jnp.float32,
    )
    slot_ids = lax.broadcasted_iota(jnp.int32, (rows, experts * sum(groups)), 1).astype(jnp.float32)
    picked, share = 0.0, 0.0
    for k in range(top_count):
        rank = jnp.sum(before * marks[k], axis=1, keepdims=True)
        slot, first, base = jnp.full((rows, 1), -1.0, jnp.float32), 0, 0
        for g in groups:
            inside = (rank >= first) & (rank < first + g)
            slot = jnp.where(inside, base + names[k] * g + rank - first, slot)
            first, base = first + g, base + g * experts
        picked = picked + jnp.where(slot == slot_ids, 1.0, 0.0)
        share = share + jnp.where(slot == slot_ids, shares[k], 0.0)
    pick_ref[...] = jnp.transpose(picked).astype(jnp.bfloat16)
    high = share.astype(jnp.bfloat16)
    high_ref[...] = high
    low_ref[...] = (share - high.astype(jnp.float32)).astype(jnp.bfloat16)


def layer_kernel(sp, dp, count, *refs):
    (
        q_hbm, k_hbm, v_hbm, weight_ref, resid_hbm, mixer_hbm, expert_hbm, routes_hbm, shares_hbm,
        gate_hbm, up_hbm, down_hbm, gain_hbm, out_ref,
    ) = refs[:14]
    boxes = refs[14 : 14 + 4 * count]
    sent, served = boxes[:count], boxes[count : 2 * count]
    results, returned = boxes[2 * count : 3 * count], boxes[3 * count :]
    (
        raw, resid_ref, mixer_ref, expert_ref, gain_ref, routes_ref, shares_ref,
        stage, arrived, out_heads, in_heads, side_heads, flat, full, side_out, side_in,
        projected, tokens, stream_ref, pick_ref, high_ref, low_ref, gate_ref, up_ref, down_ref,
        load_sem, q_send, q_recv, a_send, a_recv, pass_send, pass_recv, near_sem, far_send, far_recv,
        twin_send, twin_recv, side_send, side_recv, local_sem,
        send_sem, recv_sem, back_send, back_recv, keep_sem, fetch_sem,
    ) = refs[14 + 4 * count :]
    _, rows, heads, width = raw.shape
    local_heads = heads // sp
    depth, columns = weight_ref.shape
    me, mate = lax.axis_index("sp"), lax.axis_index("dp")
    parity, core = lax.rem(me, 2), lax.rem(mate, 2)
    side, twin = me + 1 - 2 * parity, mate + 1 - 2 * core
    ys = dp // 2
    own_y = lax.div(mate, 2)
    n, own = sp * dp, me * dp + mate

    barrier = pltpu.get_barrier_semaphore()

    def greet(k, carry):
        other = lax.rem(own + k, n)
        pl.semaphore_signal(
            barrier, inc=1, device_id={"sp": lax.div(other, dp), "dp": lax.rem(other, dp)}, device_id_type=MESH
        )
        return carry

    lax.fori_loop(1, n, greet, 0)
    pairs = [
        (q_hbm, raw.at[0]), (k_hbm, raw.at[1]), (v_hbm, raw.at[2]), (routes_hbm, routes_ref),
        (shares_hbm, shares_ref), (weight_ref, full.at[core]), (resid_hbm, resid_ref), (mixer_hbm, mixer_ref),
        (expert_hbm, expert_ref), (gain_hbm, gain_ref),
    ]
    loads = [pltpu.make_async_copy(src, dst, load_sem.at[i]) for i, (src, dst) in enumerate(pairs)]
    for load in loads:
        load.start()
    for t in range(3):
        loads[t].wait()
        stage[t] = jnp.transpose(raw[t], (1, 0, 2))
    pl.semaphore_wait(barrier, n - 1)

    def await_bytes(ref, sem):
        pltpu.make_async_copy(ref, ref, sem).wait()

    def remote(src, dst, send, recv, device):
        return pltpu.make_async_remote_copy(
            src_ref=src, dst_ref=dst, send_sem=send, recv_sem=recv, device_id=device, device_id_type=MESH
        )

    def send_heads(t, h):
        def push(i, carry):
            k = sp // 2 + (1 - 2 * lax.rem(i, 2)) * lax.div(i + 1, 2)
            target = lax.rem(me + k, sp)
            remote(
                stage.at[t, target * local_heads + h], arrived.at[t, h, me], q_send.at[h], q_recv.at[h],
                {"sp": target},
            ).start()
            return carry

        lax.fori_loop(0, sp - 1, push, 0)

    others = pl.ds(0, sp - 1)
    span = depth // 2 // PIECES

    def piece_rows(owner, j):
        return pl.ds(pl.multiple_of(owner * (depth // 2) + j * span, span), span)

    def far(d, owner, j):
        where = piece_rows(owner, j)
        return remote(
            weight_ref.at[where], full.at[1 + d, where], far_send.at[d - 1, owner, j], far_recv.at[d - 1, j],
            {"dp": lax.rem(own_y + d, ys) * 2 + owner},
        )

    def far_in(d, j):
        where = full.at[1 + d, piece_rows(core, j)]
        return remote(where, where, far_send.at[d - 1, 0, j], far_recv.at[d - 1, j], {"dp": twin})

    def to_twin(d, j):
        where = full.at[1 + d, piece_rows(core, j)]
        return remote(where, where, twin_send.at[d - 1, j], twin_recv.at[d - 1, j], {"dp": twin})

    near = remote(weight_ref, full.at[core], near_sem.at[0], near_sem.at[1], {"dp": twin})
    for t in range(3):
        send_heads(t, 0)

    @pl.when(core == parity)
    def _():
        for j in range(PIECES):
            for d in range(1, ys):
                for owner in range(2):
                    far(d, owner, j).start()

    near.start()
    keep_heads = [
        pltpu.make_async_copy(stage.at[t, me * local_heads + h], arrived.at[t, h, me], local_sem.at[t, h])
        for t in range(3)
        for h in range(local_heads)
    ]
    for copy in keep_heads:
        copy.start()
    for h in range(1, local_heads):
        for t in range(3):
            send_heads(t, h)
    fetches = [
        pltpu.make_async_copy(src, dst, fetch_sem.at[i])
        for i, (src, dst) in enumerate(((gate_hbm, gate_ref), (up_hbm, up_ref), (down_hbm, down_ref)))
    ]
    for copy in fetches:
        copy.start()
    loads[3].wait()
    loads[4].wait()
    place_slots(rows, n, [box.shape[1] for box in sent], routes_ref, shares_ref, pick_ref, high_ref, low_ref)

    block = rows * max(1, min(sp, 256 // rows))
    per = block // rows
    length = sp * rows
    scale = width ** (-0.5)
    tri_row = lax.broadcasted_iota(jnp.int32, (block, block), 0)
    tri_col = lax.broadcasted_iota(jnp.int32, (block, block), 1)
    suffix_ones = (tri_row >= tri_col).astype(jnp.bfloat16)
    is_past = tri_col < tri_row

    def answer(h, target):
        return remote(
            out_heads.at[h, target], in_heads.at[h, me], a_send.at[h], a_recv.at[h, me], {"sp": target}
        )

    def expect(h, source):
        return remote(
            out_heads.at[h, source], in_heads.at[h, source], a_send.at[h], a_recv.at[h, source], {"sp": source}
        )

    def hand_on(h, source):
        return remote(
            in_heads.at[h, source], side_heads.at[h, source], pass_send.at[h], pass_recv.at[h], {"sp": side}
        )

    def attend_head(h):
        def piece(t, index):
            return arrived[t, h, index * per : (index + 1) * per].reshape(block, width)

        for q_block in range(length // block):
            query = piece(0, q_block)
            total = jnp.zeros((block, width), jnp.float32)
            later = jnp.zeros((block, 1), jnp.float32)
            for k_block in range(q_block, -1, -1):
                scores = (
                    lax.dot_general(
                        query, piece(1, k_block), (((1,), (1,)), ((), ())),
                        preferred_element_type=jnp.float32,
                    )
                    * scale
                )
                soft = jnp.maximum(scores, 0.0) + jnp.log(1.0 + jnp.exp(-jnp.abs(scores)))
                if k_block == q_block:
                    soft = jnp.where(is_past, soft, 0.0)
                high = soft.astype(jnp.bfloat16)
                low = (soft - high.astype(jnp.float32)).astype(jnp.bfloat16)
                suffix = jnp.dot(high, suffix_ones, preferred_element_type=jnp.float32) + jnp.dot(
                    low, suffix_ones, preferred_element_type=jnp.float32
                )
                weights = jnp.exp(scores - suffix - later)
                if k_block == q_block:
                    weights = jnp.where(is_past, weights, 0.0)
                total = total + jnp.dot(
                    weights.astype(jnp.bfloat16), piece(2, k_block), preferred_element_type=jnp.float32
                )
                if k_block > 0:
                    later = later + suffix[:, :1]
            out_heads[h, q_block * per : (q_block + 1) * per] = total.astype(jnp.bfloat16).reshape(
                per, rows, width
            )

    def send_answers(h):
        def push(k, carry):
            answer(h, lax.rem(me + k, sp)).start()
            return carry

        lax.fori_loop(1, sp, push, 0)
        keep_answer(h).start()

    def keep_answer(h):
        return pltpu.make_async_copy(out_heads.at[h, me], in_heads.at[h, me], local_sem.at[3, h])

    def pass_on(j):
        for d in range(1, ys):
            far_in(d, j).wait_recv()
            to_twin(d, j).start()

    for copy in keep_heads:
        copy.wait()
    for h in range(local_heads):
        await_bytes(arrived.at[:, h, others], q_recv.at[h])
        attend_head(h)
        send_answers(h)
    for j in range(PIECES - 1):
        pass_on(j)
    for h in range(local_heads):
        keep_answer(h).wait()
        hand_on(h, me).start()

        def follow(k, carry):
            source = lax.rem(me + k, sp)
            expect(h, source).wait_recv()
            hand_on(h, source).start()
            return carry

        lax.fori_loop(1, sp, follow, 0)
    pass_on(PIECES - 1)

    def fill(ref, first):
        for source in range(sp):
            for h in range(local_heads):
                place = (source * local_heads + h) * width
                flat[first : first + rows, place : place + width] = ref[h, source]

    fill(in_heads, 0)
    for h in range(local_heads):
        await_bytes(side_heads.at[h], pass_recv.at[h])
    fill(side_heads, rows)
    for d in range(1, ys):
        for j in range(PIECES):
            to_twin(d, j).wait()

    tile = min(columns, 512)
    many = columns // tile

    def split(i):
        return lax.div(i, many), pl.ds(pl.multiple_of(lax.rem(i, many) * tile, tile), tile)

    def place_of(slice_index, i):
        return pl.ds(pl.multiple_of((slice_index * many + lax.rem(i, many)) * tile, tile), tile)

    def hand_back(d):
        return remote(
            side_out.at[d - 1], side_in.at[d - 1], side_send.at[d - 1], side_recv.at[d - 1], {"sp": side}
        )

    for d in range(1, ys):

        @pl.loop(0, many)
        def _(i):
            _, inner = split(i)
            both = jnp.dot(flat[...], full[1 + d, :, inner], preferred_element_type=jnp.float32)
            projected[:, place_of(lax.rem(own_y + ys - d, ys) * 2 + parity, i)] = both[:rows]
            side_out[d - 1, :, inner] = both[rows:].astype(jnp.bfloat16)

        hand_back(d).start()

    loads[5].wait()
    near.wait()

    @pl.loop(0, 2 * many)
    def _(i):
        which, inner = split(i)
        projected[:, place_of(own_y * 2 + which, i)] = jnp.dot(
            flat[:rows], full[which, :, inner], preferred_element_type=jnp.float32
        )

    for load in loads[6:]:
        load.wait()
    for h in range(local_heads):
        await_bytes(stage.at[:, others], q_send.at[h])
        await_bytes(out_heads.at[h, others], a_send.at[h])
        await_bytes(in_heads.at[h], pass_send.at[h])

    @pl.when(core == parity)
    def _():
        for j in range(PIECES):
            for d in range(1, ys):
                for owner in range(2):
                    far(d, owner, j).wait_send()

    for d in range(1, ys):
        hand_back(d).wait()

        @pl.loop(0, many)
        def _(i):
            _, inner = split(i)
            projected[:, place_of(lax.rem(own_y + ys - d, ys) * 2 + 1 - parity, i)] = side_in[
                d - 1, :, inner
            ].astype(jnp.float32)

    @pl.loop(0, rows // 16)
    def _(i):
        part = pl.ds(pl.multiple_of(i * 16, 16), 16)
        stream = (
            resid_ref[part].astype(jnp.float32) + normed_token_rows(projected[part], mixer_ref[...])
        ).astype(jnp.bfloat16)
        stream_ref[part] = stream
        tokens[part] = normed_token_rows(stream.astype(jnp.float32), expert_ref[...]).astype(jnp.bfloat16)

    features = projected.shape[1]
    tile = 512

    def move(sources, targets, sends, recvs, a, target):
        return remote(
            sources[a].at[target], targets[a].at[own], sends.at[a], recvs.at[a],
            {"sp": lax.div(target, dp), "dp": lax.rem(target, dp)},
        )

    def outward(a, target):
        return move(sent, served, send_sem, recv_sem, a, target)

    def homeward(a, target):
        return move(results, returned, back_send, back_recv, a, target)

    def start_all(make, a, first, number):
        def push(i, carry):
            target = first + lax.rem(lax.rem(own, number) + number // 2 + i, number)

            @pl.when(target != own)
            def _():
                make(a, target).start()

            return carry

        lax.fori_loop(0, number, push, 0)

    peers = pl.ds(0, n - 1)
    half = n // 2
    far_half = (1 - lax.div(own, half)) * half
    own_rows = [pltpu.make_async_copy(sent[a].at[own], served[a].at[own], keep_sem.at[a]) for a in range(count)]
    keeps = [
        pltpu.make_async_copy(results[a].at[own], returned[a].at[own], keep_sem.at[count + a])
        for a in range(count)
    ]
    row = 0
    for a in range(count):
        many = sent[a].shape[1]
        for first in (far_half, half - far_half):
            wanted = pick_ref[pl.ds(pl.multiple_of(row + first * many, half * many), half * many)]

            @pl.loop(0, features // tile)
            def _(i):
                part = pl.ds(pl.multiple_of(i * tile, tile), tile)
                sent[a][pl.ds(first, half), :, part] = (
                    jnp.dot(wanted, tokens[:, part], preferred_element_type=jnp.float32)
                    .astype(jnp.bfloat16)
                    .reshape(half, many, tile)
                )

            start_all(outward, a, first, half)
        own_rows[a].start()
        row += n * many

    for a in range(count):
        own_rows[a].wait()
        await_bytes(served[a].at[peers], recv_sem.at[a])
        if a == 0:
            for copy in fetches:
                copy.wait()
        many = served[a].shape[1]
        taken = served[a][...].reshape(n * many, features)
        gate = jnp.dot(taken, gate_ref[...], preferred_element_type=jnp.float32)
        upward = jnp.dot(taken, up_ref[...], preferred_element_type=jnp.float32)
        hidden = (gate / (1.0 + jnp.exp(-gate)) * upward).astype(jnp.bfloat16)
        for i in range(features // tile):
            part = slice(i * tile, (i + 1) * tile)
            results[a][:, :, part] = (
                jnp.dot(hidden, down_ref[:, part], preferred_element_type=jnp.float32)
                .astype(jnp.bfloat16)
                .reshape(n, many, tile)
            )
        start_all(homeward, a, far_half, half)
        start_all(homeward, a, half - far_half, half)
        keeps[a].start()

    row = 0
    for a in range(count):
        keeps[a].wait()
        await_bytes(returned[a].at[peers], back_recv.at[a])
        many = returned[a].shape[1]
        columns_of = slice(row, row + n * many)

        @pl.loop(0, features // tile)
        def _(i):
            part = pl.ds(pl.multiple_of(i * tile, tile), tile)
            block = returned[a][:, :, part].reshape(n * many, tile)
            total = jnp.dot(high_ref[:, columns_of], block, preferred_element_type=jnp.float32) + jnp.dot(
                low_ref[:, columns_of], block, preferred_element_type=jnp.float32
            )
            projected[:, part] = total if a == 0 else projected[:, part] + total

        row += n * many

    for a in range(count):
        await_bytes(sent[a].at[peers], send_sem.at[a])
        await_bytes(results[a].at[peers], back_send.at[a])

    @pl.loop(0, rows // 16)
    def _(i):
        part = pl.ds(pl.multiple_of(i * 16, 16), 16)
        out_ref[part] = (
            stream_ref[part].astype(jnp.float32) + normed_token_rows(projected[part], gain_ref[...])
        ).astype(jnp.bfloat16)


def layer(
    query, key, value, weight, residual, mixer_gain, expert_gain, routes, shares, gate, up, down, gain, groups
):
    sp, dp = lax.axis_size("sp"), lax.axis_size("dp")
    n = sp * dp
    rows, heads, width = query.shape
    depth, columns = weight.shape
    features = residual.shape[1]
    local_heads = heads // sp
    extra = max(dp // 2 - 1, 1)
    slots = n * sum(groups)
    anywhere = pl.BlockSpec(memory_space=pl.ANY)
    dma = pltpu.SemaphoreType.DMA
    bf16, f32 = jnp.bfloat16, jnp.float32
    return pl.pallas_call(
        functools.partial(layer_kernel, sp, dp, len(groups)),
        out_shape=pltpu.VMEM((rows, features), bf16),
        in_specs=[anywhere] * 13,
        out_specs=pl.BlockSpec(memory_space=pltpu.VMEM),
        scratch_shapes=[pltpu.VMEM((n, g, features), bf16) for _ in range(4) for g in groups]
        + [
            pltpu.VMEM((3, rows, heads, width), bf16),
            pltpu.VMEM((rows, features), bf16),
            pltpu.VMEM((1, features), f32),
            pltpu.VMEM((1, features), f32),
            pltpu.VMEM((1, features), f32),
            pltpu.VMEM(routes.shape, jnp.int32),
            pltpu.VMEM(shares.shape, f32),
            pltpu.VMEM((3, heads, rows, width), bf16),
            pltpu.VMEM((3, local_heads, sp, rows, width), bf16),
            pltpu.VMEM((local_heads, sp, rows, width), bf16),
            pltpu.VMEM((local_heads, sp, rows, width), bf16),
            pltpu.VMEM((local_heads, sp, rows, width), bf16),
            pltpu.VMEM((2 * rows, depth), bf16),
            pltpu.VMEM((2 + extra, depth, columns), bf16),
            pltpu.VMEM((extra, rows, columns), bf16),
            pltpu.VMEM((extra, rows, columns), bf16),
            pltpu.VMEM((rows, features), f32),
            pltpu.VMEM((rows, features), bf16),
            pltpu.VMEM((rows, features), bf16),
            pltpu.VMEM((slots, rows), bf16),
            pltpu.VMEM((rows, slots), bf16),
            pltpu.VMEM((rows, slots), bf16),
            pltpu.VMEM(gate.shape, bf16),
            pltpu.VMEM(up.shape, bf16),
            pltpu.VMEM(down.shape, bf16),
            dma((10,)),
            dma((local_heads,)),
            dma((local_heads,)),
            dma((local_heads,)),
            dma((local_heads, sp)),
            dma((local_heads,)),
            dma((local_heads,)),
            dma((2,)),
            dma((extra, 2, PIECES)),
            dma((extra, PIECES)),
            dma((extra, PIECES)),
            dma((extra, PIECES)),
            dma((extra,)),
            dma((extra,)),
            dma((4, local_heads)),
            dma((len(groups),)),
            dma((len(groups),)),
            dma((len(groups),)),
            dma((len(groups),)),
            dma((2 * len(groups),)),
            dma((3,)),
        ],
        compiler_params=pltpu.CompilerParams(
            collective_id=0, has_side_effects=True, vmem_limit_bytes=VMEM_LIMIT
        ),
    )(
        query, key, value, weight, residual, mixer_gain[None], expert_gain[None], routes, shares,
        gate, up, down, gain[None],
    )


def local(
    queries,
    key_rows,
    values,
    residual,
    out_weight,
    mixer_gain,
    expert_gain,
    gate_weight,
    up_weight,
    expert_down_matrix,
    routes,
    route_weight,
    output_gain,
):
    local_rows = queries.shape[1]
    experts = lax.axis_size("sp") * lax.axis_size("dp")
    capacity = max(2, 3 * local_rows // experts)
    groups = [g for g in (capacity // 8 * 8, capacity % 8) if g]
    output = layer(
        queries[0], key_rows[0], values[0], out_weight, residual[0], mixer_gain, expert_gain,
        routes[0].T, route_weight[0].T, gate_weight[0], up_weight[0], expert_down_matrix[0], output_gain, groups,
    )
    return output[None]


def solution(mesh):
    in_specs = (
        P("dp", "sp", None, None),
        P("dp", "sp", None, None),
        P("dp", "sp", None, None),
        P("dp", "sp", None),
        P(None, "dp"),
        P(),
        P(),
        P(("sp", "dp"), None, None),
        P(("sp", "dp"), None, None),
        P(("sp", "dp"), None, None),
        P("dp", "sp", None),
        P("dp", "sp", None),
        P(),
    )
    out_specs = P("dp", "sp", None)
    return jax.shard_map(local, mesh=mesh, in_specs=in_specs, out_specs=out_specs, check_vma=False)
```

```python
import functools

import jax
import jax.numpy as jnp
from jax import lax
from jax.experimental import pallas as pl
from jax.experimental.pallas import tpu as pltpu
from jax.sharding import PartitionSpec as P

EPSILON = 1e-06
MESH = pl.DeviceIdType.MESH
VMEM_LIMIT = 62 * 1024 * 1024


def normed_token_rows(matrix, gain):
    return matrix * lax.rsqrt(jnp.mean(matrix * matrix, axis=-1, keepdims=True) + EPSILON) * gain


PIECES = 2


def place_slots(rows, experts, groups, halves, routes_ref, shares_ref, pick_refs, high_refs, low_refs):
    top_count = routes_ref.shape[0]
    half = experts // 2

    def column(row):
        return jnp.transpose(jnp.broadcast_to(row, (rows, rows)))[:, :1]

    lanes = lax.broadcasted_iota(jnp.int32, (rows, max(experts, 128)), 1).astype(jnp.float32)
    names = [column(routes_ref[k : k + 1].astype(jnp.float32)) for k in range(top_count)]
    shares = [column(shares_ref[k : k + 1]) for k in range(top_count)]
    marks = [jnp.where(name == lanes, 1.0, 0.0) for name in names]
    earlier = lax.broadcasted_iota(jnp.int32, (rows, rows), 1) < lax.broadcasted_iota(jnp.int32, (rows, rows), 0)
    before = jnp.dot(
        jnp.where(earlier, 1.0, 0.0).astype(jnp.bfloat16),
        sum(marks).astype(jnp.bfloat16),
        preferred_element_type=jnp.float32,
    )
    ranks = [jnp.sum(before * mark, axis=1, keepdims=True) for mark in marks]
    slot_ids = lax.broadcasted_iota(jnp.int32, (rows, half * sum(groups)), 1).astype(jnp.float32)
    for which, pick_ref, high_ref, low_ref in zip(halves, pick_refs, high_refs, low_refs):
        start = jnp.asarray(which * half, jnp.int32).astype(jnp.float32)
        picked, share = 0.0, 0.0
        for k in range(top_count):
            name, rank = names[k] - start, ranks[k]
            here = (name >= 0.0) & (name < half)
            slot, first, base = jnp.full((rows, 1), -1.0, jnp.float32), 0, 0
            for g in groups:
                inside = here & (rank >= first) & (rank < first + g)
                slot = jnp.where(inside, base + name * g + rank - first, slot)
                first, base = first + g, base + g * half
            picked = picked + jnp.where(slot == slot_ids, 1.0, 0.0)
            share = share + jnp.where(slot == slot_ids, shares[k], 0.0)
        pick_ref[...] = jnp.transpose(picked).astype(jnp.bfloat16)
        high = share.astype(jnp.bfloat16)
        high_ref[...] = high
        low_ref[...] = (share - high.astype(jnp.float32)).astype(jnp.bfloat16)


def layer_kernel(sp, dp, count, *refs):
    (
        q_hbm, k_hbm, v_hbm, weight_ref, resid_hbm, mixer_hbm, expert_hbm, routes_hbm, shares_hbm,
        gate_hbm, up_hbm, down_hbm, gain_hbm, out_ref,
    ) = refs[:14]
    boxes = refs[14 : 14 + 6 * count]
    sent, served = boxes[:count], boxes[count : 2 * count]
    results, returned = boxes[2 * count : 3 * count], boxes[3 * count : 4 * count]
    lent, lent_back = boxes[4 * count : 5 * count], boxes[5 * count :]
    (
        raw, resid_ref, mixer_ref, expert_ref, gain_ref, routes_ref, shares_ref,
        stage, arrived, out_heads, in_heads, side_heads, flat, full, side_out, side_in,
        projected, tokens, stream_ref, pick_ref, high_ref, low_ref, gate_ref, up_ref, down_ref,
        far_routes, far_shares, far_pick, far_high, far_low, dense, extra_ref,
        load_sem, q_send, q_recv, a_send, a_recv, pass_send, pass_recv, near_sem, far_send, far_recv,
        twin_send, twin_recv, side_send, side_recv, local_sem,
        send_sem, recv_sem, back_send, back_recv, keep_sem, fetch_sem,
        note_send, note_recv, dense_sem, partial_sem, lend_recv, lend_keep,
    ) = refs[14 + 6 * count :]
    _, rows, heads, width = raw.shape
    local_heads = heads // sp
    depth, columns = weight_ref.shape
    me, mate = lax.axis_index("sp"), lax.axis_index("dp")
    parity, core = lax.rem(me, 2), lax.rem(mate, 2)
    side, twin = me + 1 - 2 * parity, mate + 1 - 2 * core
    ys = dp // 2
    own_y = lax.div(mate, 2)
    n, own = sp * dp, me * dp + mate
    half, plane = n // 2, n // 4
    level = lax.div(own, plane)
    spot = lax.rem(own, plane)
    my_half = lax.div(level, 2)
    near_base, far_base = my_half * half, (1 - my_half) * half
    local = own - near_base
    partner = (3 - level) * plane + spot
    inner = level == 1 + my_half
    outer = level != 1 + my_half

    barrier = pltpu.get_barrier_semaphore()

    def greet(k, carry):
        other = lax.rem(own + k, n)
        pl.semaphore_signal(
            barrier, inc=1, device_id={"sp": lax.div(other, dp), "dp": lax.rem(other, dp)}, device_id_type=MESH
        )
        return carry

    lax.fori_loop(1, n, greet, 0)
    pairs = [
        (q_hbm, raw.at[0]), (k_hbm, raw.at[1]), (v_hbm, raw.at[2]), (routes_hbm, routes_ref),
        (shares_hbm, shares_ref), (weight_ref, full.at[core]), (resid_hbm, resid_ref), (mixer_hbm, mixer_ref),
        (expert_hbm, expert_ref), (gain_hbm, gain_ref),
    ]
    loads = [pltpu.make_async_copy(src, dst, load_sem.at[i]) for i, (src, dst) in enumerate(pairs)]
    for load in loads:
        load.start()
    for t in range(3):
        loads[t].wait()
        stage[t] = jnp.transpose(raw[t], (1, 0, 2))
    pl.semaphore_wait(barrier, n - 1)

    def await_bytes(ref, sem):
        pltpu.make_async_copy(ref, ref, sem).wait()

    def remote(src, dst, send, recv, device):
        return pltpu.make_async_remote_copy(
            src_ref=src, dst_ref=dst, send_sem=send, recv_sem=recv, device_id=device, device_id_type=MESH
        )

    def send_heads(t, h):
        def push(i, carry):
            k = sp // 2 + (1 - 2 * lax.rem(i, 2)) * lax.div(i + 1, 2)
            target = lax.rem(me + k, sp)
            remote(
                stage.at[t, target * local_heads + h], arrived.at[t, h, me], q_send.at[h], q_recv.at[h],
                {"sp": target},
            ).start()
            return carry

        lax.fori_loop(0, sp - 1, push, 0)

    others = pl.ds(0, sp - 1)
    span = depth // 2 // PIECES

    def piece_rows(owner, j):
        return pl.ds(pl.multiple_of(owner * (depth // 2) + j * span, span), span)

    def far(d, owner, j):
        where = piece_rows(owner, j)
        return remote(
            weight_ref.at[where], full.at[1 + d, where], far_send.at[d - 1, owner, j], far_recv.at[d - 1, j],
            {"dp": lax.rem(own_y + d, ys) * 2 + owner},
        )

    def far_in(d, j):
        where = full.at[1 + d, piece_rows(core, j)]
        return remote(where, where, far_send.at[d - 1, 0, j], far_recv.at[d - 1, j], {"dp": twin})

    def to_twin(d, j):
        where = full.at[1 + d, piece_rows(core, j)]
        return remote(where, where, twin_send.at[d - 1, j], twin_recv.at[d - 1, j], {"dp": twin})

    near = remote(weight_ref, full.at[core], near_sem.at[0], near_sem.at[1], {"dp": twin})
    for t in range(3):
        send_heads(t, 0)

    @pl.when(core == parity)
    def _():
        for j in range(PIECES):
            for d in range(1, ys):
                for owner in range(2):
                    far(d, owner, j).start()

    near.start()
    keep_heads = [
        pltpu.make_async_copy(stage.at[t, me * local_heads + h], arrived.at[t, h, me], local_sem.at[t, h])
        for t in range(3)
        for h in range(local_heads)
    ]
    for copy in keep_heads:
        copy.start()
    for h in range(1, local_heads):
        for t in range(3):
            send_heads(t, h)
    fetches = [
        pltpu.make_async_copy(src, dst, fetch_sem.at[i])
        for i, (src, dst) in enumerate(((gate_hbm, gate_ref), (up_hbm, up_ref), (down_hbm, down_ref)))
    ]
    loads[3].wait()
    loads[4].wait()

    def device(target):
        return {"sp": lax.div(target, dp), "dp": lax.rem(target, dp)}

    notes = [
        remote(src, dst, note_send.at[i], note_recv.at[i], device(partner))
        for i, (src, dst) in enumerate(((routes_ref, far_routes), (shares_ref, far_shares)))
    ]
    groups = [box.shape[1] for box in sent]

    @pl.when(inner)
    def _():
        for note in notes:
            note.start()

    place_slots(
        rows, n, groups, [0, 1], routes_ref, shares_ref,
        *[[ref.at[i] for i in range(2)] for ref in (pick_ref, high_ref, low_ref)],
    )

    block = rows * max(1, min(sp, 256 // rows))
    per = block // rows
    length = sp * rows
    scale = width ** (-0.5)
    tri_row = lax.broadcasted_iota(jnp.int32, (block, block), 0)
    tri_col = lax.broadcasted_iota(jnp.int32, (block, block), 1)
    suffix_ones = (tri_row >= tri_col).astype(jnp.bfloat16)
    is_past = tri_col < tri_row

    def answer(h, target):
        return remote(
            out_heads.at[h, target], in_heads.at[h, me], a_send.at[h], a_recv.at[h, me], {"sp": target}
        )

    def expect(h, source):
        return remote(
            out_heads.at[h, source], in_heads.at[h, source], a_send.at[h], a_recv.at[h, source], {"sp": source}
        )

    def hand_on(h, source):
        return remote(
            in_heads.at[h, source], side_heads.at[h, source], pass_send.at[h], pass_recv.at[h], {"sp": side}
        )

    def attend_head(h, between):
        def piece(t, index):
            return arrived[t, h, index * per : (index + 1) * per].reshape(block, width)

        for q_block in range(length // block):
            query = piece(0, q_block)
            total = jnp.zeros((block, width), jnp.float32)
            later = jnp.zeros((block, 1), jnp.float32)
            for k_block in range(q_block, -1, -1):
                scores = (
                    lax.dot_general(
                        query, piece(1, k_block), (((1,), (1,)), ((), ())),
                        preferred_element_type=jnp.float32,
                    )
                    * scale
                )
                soft = jnp.maximum(scores, 0.0) + jnp.log(1.0 + jnp.exp(-jnp.abs(scores)))
                if k_block == q_block:
                    soft = jnp.where(is_past, soft, 0.0)
                high = soft.astype(jnp.bfloat16)
                low = (soft - high.astype(jnp.float32)).astype(jnp.bfloat16)
                suffix = jnp.dot(high, suffix_ones, preferred_element_type=jnp.float32) + jnp.dot(
                    low, suffix_ones, preferred_element_type=jnp.float32
                )
                weights = jnp.exp(scores - suffix - later)
                if k_block == q_block:
                    weights = jnp.where(is_past, weights, 0.0)
                total = total + jnp.dot(
                    weights.astype(jnp.bfloat16), piece(2, k_block), preferred_element_type=jnp.float32
                )
                if k_block > 0:
                    later = later + suffix[:, :1]
            out_heads[h, q_block * per : (q_block + 1) * per] = total.astype(jnp.bfloat16).reshape(
                per, rows, width
            )
            if q_block:
                send_answers(h, q_block - 1)
            if q_block == length // block // 2:
                between()
        send_answers(h, length // block - 1)
        keep_answer(h).start()

    def send_answers(h, q_block):
        for target in range(q_block * per, (q_block + 1) * per):

            @pl.when(me != target)
            def _():
                answer(h, target).start()

    def keep_answer(h):
        return pltpu.make_async_copy(out_heads.at[h, me], in_heads.at[h, me], local_sem.at[3, h])

    def pass_on(j):
        for d in range(1, ys):
            far_in(d, j).wait_recv()
            to_twin(d, j).start()

    for copy in keep_heads:
        copy.wait()
    def follow_all(h):
        keep_answer(h).wait()
        hand_on(h, me).start()

        def follow(k, carry):
            source = lax.rem(me + k, sp)
            expect(h, source).wait_recv()
            hand_on(h, source).start()
            return carry

        lax.fori_loop(1, sp, follow, 0)

    for h in range(local_heads):
        await_bytes(arrived.at[:, h, others], q_recv.at[h])
        attend_head(h, (lambda: follow_all(h - 1)) if h else (lambda: None))
    for j in range(PIECES - 1):
        pass_on(j)
    follow_all(local_heads - 1)
    pass_on(PIECES - 1)
    for copy in fetches:
        copy.start()

    @pl.when(inner)
    def _():
        for note in notes:
            note.wait()
        place_slots(rows, n, groups, [my_half], far_routes, far_shares, [far_pick], [far_high], [far_low])

    def fill(ref, first):
        for source in range(sp):
            for h in range(local_heads):
                place = (source * local_heads + h) * width
                flat[first : first + rows, place : place + width] = ref[h, source]

    fill(in_heads, 0)
    for h in range(local_heads):
        await_bytes(side_heads.at[h], pass_recv.at[h])
    fill(side_heads, rows)
    for d in range(1, ys):
        for j in range(PIECES):
            to_twin(d, j).wait()

    tile = min(columns, 512)
    many = columns // tile

    def split(i):
        return lax.div(i, many), pl.ds(pl.multiple_of(lax.rem(i, many) * tile, tile), tile)

    def place_of(slice_index, i):
        return pl.ds(pl.multiple_of((slice_index * many + lax.rem(i, many)) * tile, tile), tile)

    def hand_back(d):
        return remote(
            side_out.at[d - 1], side_in.at[d - 1], side_send.at[d - 1], side_recv.at[d - 1], {"sp": side}
        )

    for d in range(1, ys):

        @pl.loop(0, many)
        def _(i):
            _, inner = split(i)
            both = jnp.dot(flat[...], full[1 + d, :, inner], preferred_element_type=jnp.float32)
            projected[:, place_of(lax.rem(own_y + ys - d, ys) * 2 + parity, i)] = both[:rows]
            side_out[d - 1, :, inner] = both[rows:].astype(jnp.bfloat16)

        hand_back(d).start()

    loads[5].wait()
    near.wait()

    @pl.loop(0, 2 * many)
    def _(i):
        which, inner = split(i)
        projected[:, place_of(own_y * 2 + which, i)] = jnp.dot(
            flat[:rows], full[which, :, inner], preferred_element_type=jnp.float32
        )

    for load in loads[6:]:
        load.wait()
    for h in range(local_heads):
        await_bytes(stage.at[:, others], q_send.at[h])
        await_bytes(out_heads.at[h, others], a_send.at[h])
        await_bytes(in_heads.at[h], pass_send.at[h])

    @pl.when(core == parity)
    def _():
        for j in range(PIECES):
            for d in range(1, ys):
                for owner in range(2):
                    far(d, owner, j).wait_send()

    for d in range(1, ys):
        hand_back(d).wait()

        @pl.loop(0, many)
        def _(i):
            _, inner = split(i)
            projected[:, place_of(lax.rem(own_y + ys - d, ys) * 2 + 1 - parity, i)] = side_in[
                d - 1, :, inner
            ].astype(jnp.float32)

    def lend(i):
        part = pl.ds(pl.multiple_of(i * 16, 16), 16)
        return remote(tokens.at[part], dense.at[part], dense_sem.at[0], dense_sem.at[1], device(partner))

    @pl.loop(0, rows // 16)
    def _(i):
        part = pl.ds(pl.multiple_of(i * 16, 16), 16)
        stream = (
            resid_ref[part].astype(jnp.float32) + normed_token_rows(projected[part], mixer_ref[...])
        ).astype(jnp.bfloat16)
        stream_ref[part] = stream
        tokens[part] = normed_token_rows(stream.astype(jnp.float32), expert_ref[...]).astype(jnp.bfloat16)

        @pl.when(inner & (i > 0))
        def _():
            lend(i - 1).start()

    @pl.when(inner)
    def _():
        lend(rows // 16 - 1).start()

    features = projected.shape[1]
    tile = 512

    def each(number, turn, make, own_place):
        def push(i, carry):
            place = lax.rem(turn + i, number)

            @pl.when(place != own_place)
            def _():
                make(place).start()

            return carry

        lax.fori_loop(0, number, push, 0)

    def outward(a, target):
        return remote(sent[a].at[target], served[a].at[own], send_sem.at[a], recv_sem.at[a], device(target))

    def outward_lent(a, place):
        return remote(
            lent[a].at[place], served[a].at[partner], send_sem.at[a], recv_sem.at[a], device(near_base + place)
        )

    def homeward(a, source):
        return remote(results[a].at[source], returned[a].at[own], back_send.at[a], back_recv.at[a], device(source))

    def homeward_lent(a, place):
        return remote(
            results[a].at[(2 - my_half) * plane + place], lent_back[a].at[local], back_send.at[a], lend_recv.at[a],
            device((1 + my_half) * plane + place),
        )

    def choose(a, pick, source_ref, out, first):
        row = half * sum(groups[:a])
        wanted = pick[row : row + half * groups[a]]

        @pl.loop(0, features // tile)
        def _(i):
            part = pl.ds(pl.multiple_of(i * tile, tile), tile)
            out[a][pl.ds(first, half), :, part] = (
                jnp.dot(wanted, source_ref[:, part], preferred_element_type=jnp.float32)
                .astype(jnp.bfloat16)
                .reshape(half, groups[a], tile)
            )

    own_rows = [pltpu.make_async_copy(sent[a].at[own], served[a].at[own], keep_sem.at[a]) for a in range(count)]
    keeps = [
        pltpu.make_async_copy(results[a].at[own], returned[a].at[own], keep_sem.at[count + a])
        for a in range(count)
    ]
    lent_rows = [
        pltpu.make_async_copy(lent[a].at[local], served[a].at[partner], lend_keep.at[a]) for a in range(count)
    ]
    lent_keeps = [
        pltpu.make_async_copy(results[a].at[partner], lent_back[a].at[local], lend_keep.at[count + a])
        for a in range(count)
    ]
    for a in range(count):

        @pl.when(outer)
        def _():
            choose(a, pick_ref.at[1 - my_half], tokens, sent, far_base)
            each(half, local + half // 2, lambda place: outward(a, far_base + place), -1)

        choose(a, pick_ref.at[my_half], tokens, sent, near_base)
        each(half, local + half // 2, lambda place: outward(a, near_base + place), local)
        own_rows[a].start()

    @pl.when(inner)
    def _():
        await_bytes(dense, dense_sem.at[1])
        for a in range(count):
            choose(a, far_pick, dense, lent, 0)
            each(half, local + half // 2, lambda place: outward_lent(a, place), local)
            lent_rows[a].start()

    def await_blocks(boxes, sems, a):
        @pl.when(inner)
        def _():
            await_bytes(boxes[a].at[pl.ds(0, n - 2)], sems.at[a])

        @pl.when(outer)
        def _():
            await_bytes(boxes[a].at[pl.ds(0, n - 1)], sems.at[a])

    def give_lent(a):
        each(plane, spot + plane // 2, lambda place: homeward_lent(a, place), jnp.where(inner, spot, -1))

        @pl.when(inner)
        def _():
            lent_keeps[a].start()

    def give_far(a):
        each(plane, spot + plane // 2, lambda place: homeward(a, 3 * (1 - my_half) * plane + place), -1)

    def give_near(a):
        each(half, local + half // 2, lambda place: homeward(a, near_base + place), local)
        keeps[a].start()

    for a in range(count):
        own_rows[a].wait()

        @pl.when(inner)
        def _():
            lent_rows[a].wait()

        await_blocks(served, recv_sem, a)
        if a == 0:
            for copy in fetches:
                copy.wait()
        many = served[a].shape[1]
        taken = served[a][...].reshape(n * many, features)
        gate = jnp.dot(taken, gate_ref[...], preferred_element_type=jnp.float32)
        upward = jnp.dot(taken, up_ref[...], preferred_element_type=jnp.float32)
        hidden = (gate / (1.0 + jnp.exp(-gate)) * upward).astype(jnp.bfloat16)
        for i in range(features // tile):
            part = slice(i * tile, (i + 1) * tile)
            results[a][:, :, part] = (
                jnp.dot(hidden, down_ref[:, part], preferred_element_type=jnp.float32)
                .astype(jnp.bfloat16)
                .reshape(n, many, tile)
            )
        give_lent(a)

        @pl.when(inner)
        def _():
            give_far(a)

    for a in range(count):

        @pl.when(outer)
        def _():
            give_far(a)

        give_near(a)

    def gather(box, first, high, low, a, part):
        columns_of = slice(half * sum(groups[:a]), half * sum(groups[: a + 1]))
        block = box[a][pl.ds(first, half), :, part].reshape(half * groups[a], tile)
        return jnp.dot(high[:, columns_of], block, preferred_element_type=jnp.float32) + jnp.dot(
            low[:, columns_of], block, preferred_element_type=jnp.float32
        )

    def settle_up(i):
        part = pl.ds(pl.multiple_of(i * tile, tile), tile)
        return remote(
            dense.at[:, part], extra_ref.at[:, part], partial_sem.at[0], partial_sem.at[1], device(partner)
        )

    @pl.when(inner)
    def _():
        for a in range(count):
            lent_keeps[a].wait()
            await_bytes(lent_back[a].at[pl.ds(0, half - 1)], lend_recv.at[a])

        @pl.loop(0, features // tile)
        def _(i):
            part = pl.ds(pl.multiple_of(i * tile, tile), tile)
            dense[:, part] = sum(
                gather(lent_back, 0, far_high, far_low, a, part) for a in range(count)
            ).astype(jnp.bfloat16)

            @pl.when(i > 0)
            def _():
                settle_up(i - 1).start()

        settle_up(features // tile - 1).start()

    for a in range(count):
        keeps[a].wait()

        @pl.when(inner)
        def _():
            await_bytes(returned[a].at[pl.ds(0, half - 1)], back_recv.at[a])

        @pl.when(outer)
        def _():
            await_bytes(returned[a].at[pl.ds(0, n - 1)], back_recv.at[a])

        @pl.loop(0, features // tile)
        def _(i):
            part = pl.ds(pl.multiple_of(i * tile, tile), tile)
            total = gather(returned, near_base, high_ref.at[my_half], low_ref.at[my_half], a, part)
            projected[:, part] = total if a == 0 else projected[:, part] + total

        @pl.when(outer)
        def _():
            @pl.loop(0, features // tile)
            def _(i):
                part = pl.ds(pl.multiple_of(i * tile, tile), tile)
                projected[:, part] += gather(
                    returned, far_base, high_ref.at[1 - my_half], low_ref.at[1 - my_half], a, part
                )

    for a in range(count):
        await_blocks(sent, send_sem, a)
        await_blocks(results, back_send, a)

    @pl.when(inner)
    def _():
        await_bytes(tokens, dense_sem.at[0])
        await_bytes(dense, partial_sem.at[0])
        await_bytes(extra_ref, partial_sem.at[1])

        @pl.loop(0, rows // 16)
        def _(i):
            part = pl.ds(pl.multiple_of(i * 16, 16), 16)
            projected[part] += extra_ref[part].astype(jnp.float32)

    @pl.loop(0, rows // 16)
    def _(i):
        part = pl.ds(pl.multiple_of(i * 16, 16), 16)
        out_ref[part] = (
            stream_ref[part].astype(jnp.float32) + normed_token_rows(projected[part], gain_ref[...])
        ).astype(jnp.bfloat16)


def layer(
    query, key, value, weight, residual, mixer_gain, expert_gain, routes, shares, gate, up, down, gain, groups
):
    sp, dp = lax.axis_size("sp"), lax.axis_size("dp")
    n = sp * dp
    rows, heads, width = query.shape
    depth, columns = weight.shape
    features = residual.shape[1]
    local_heads = heads // sp
    extra = max(dp // 2 - 1, 1)
    slots = n // 2 * sum(groups)
    anywhere = pl.BlockSpec(memory_space=pl.ANY)
    dma = pltpu.SemaphoreType.DMA
    bf16, f32 = jnp.bfloat16, jnp.float32
    return pl.pallas_call(
        functools.partial(layer_kernel, sp, dp, len(groups)),
        out_shape=pltpu.VMEM((rows, features), bf16),
        in_specs=[anywhere] * 13,
        out_specs=pl.BlockSpec(memory_space=pltpu.VMEM),
        scratch_shapes=[pltpu.VMEM((n, g, features), bf16) for _ in range(4) for g in groups]
        + [pltpu.VMEM((n // 2, g, features), bf16) for _ in range(2) for g in groups]
        + [
            pltpu.VMEM((3, rows, heads, width), bf16),
            pltpu.VMEM((rows, features), bf16),
            pltpu.VMEM((1, features), f32),
            pltpu.VMEM((1, features), f32),
            pltpu.VMEM((1, features), f32),
            pltpu.VMEM(routes.shape, jnp.int32),
            pltpu.VMEM(shares.shape, f32),
            pltpu.VMEM((3, heads, rows, width), bf16),
            pltpu.VMEM((3, local_heads, sp, rows, width), bf16),
            pltpu.VMEM((local_heads, sp, rows, width), bf16),
            pltpu.VMEM((local_heads, sp, rows, width), bf16),
            pltpu.VMEM((local_heads, sp, rows, width), bf16),
            pltpu.VMEM((2 * rows, depth), bf16),
            pltpu.VMEM((2 + extra, depth, columns), bf16),
            pltpu.VMEM((extra, rows, columns), bf16),
            pltpu.VMEM((extra, rows, columns), bf16),
            pltpu.VMEM((rows, features), f32),
            pltpu.VMEM((rows, features), bf16),
            pltpu.VMEM((rows, features), bf16),
            pltpu.VMEM((2, slots, rows), bf16),
            pltpu.VMEM((2, rows, slots), bf16),
            pltpu.VMEM((2, rows, slots), bf16),
            pltpu.VMEM(gate.shape, bf16),
            pltpu.VMEM(up.shape, bf16),
            pltpu.VMEM(down.shape, bf16),
            pltpu.VMEM(routes.shape, jnp.int32),
            pltpu.VMEM(shares.shape, f32),
            pltpu.VMEM((slots, rows), bf16),
            pltpu.VMEM((rows, slots), bf16),
            pltpu.VMEM((rows, slots), bf16),
            pltpu.VMEM((rows, features), bf16),
            pltpu.VMEM((rows, features), bf16),
            dma((10,)),
            dma((local_heads,)),
            dma((local_heads,)),
            dma((local_heads,)),
            dma((local_heads, sp)),
            dma((local_heads,)),
            dma((local_heads,)),
            dma((2,)),
            dma((extra, 2, PIECES)),
            dma((extra, PIECES)),
            dma((extra, PIECES)),
            dma((extra, PIECES)),
            dma((extra,)),
            dma((extra,)),
            dma((4, local_heads)),
            dma((len(groups),)),
            dma((len(groups),)),
            dma((len(groups),)),
            dma((len(groups),)),
            dma((2 * len(groups),)),
            dma((3,)),
            dma((2,)),
            dma((2,)),
            dma((2,)),
            dma((2,)),
            dma((len(groups),)),
            dma((2 * len(groups),)),
        ],
        compiler_params=pltpu.CompilerParams(
            collective_id=0, has_side_effects=True, vmem_limit_bytes=VMEM_LIMIT
        ),
    )(
        query, key, value, weight, residual, mixer_gain[None], expert_gain[None], routes, shares,
        gate, up, down, gain[None],
    )


def local(
    queries,
    key_rows,
    values,
    residual,
    out_weight,
    mixer_gain,
    expert_gain,
    gate_weight,
    up_weight,
    expert_down_matrix,
    routes,
    route_weight,
    output_gain,
):
    local_rows = queries.shape[1]
    experts = lax.axis_size("sp") * lax.axis_size("dp")
    capacity = max(2, 3 * local_rows // experts)
    groups = [g for g in (capacity // 8 * 8, capacity % 8) if g]
    output = layer(
        queries[0], key_rows[0], values[0], out_weight, residual[0], mixer_gain, expert_gain,
        routes[0].T, route_weight[0].T, gate_weight[0], up_weight[0], expert_down_matrix[0], output_gain, groups,
    )
    return output[None]


def solution(mesh):
    in_specs = (
        P("dp", "sp", None, None),
        P("dp", "sp", None, None),
        P("dp", "sp", None, None),
        P("dp", "sp", None),
        P(None, "dp"),
        P(),
        P(),
        P(("sp", "dp"), None, None),
        P(("sp", "dp"), None, None),
        P(("sp", "dp"), None, None),
        P("dp", "sp", None),
        P("dp", "sp", None),
        P(),
    )
    out_specs = P("dp", "sp", None)
    return jax.shard_map(local, mesh=mesh, in_specs=in_specs, out_specs=out_specs, check_vma=False)
```

```python
import functools

import jax
import jax.numpy as jnp
from jax import lax
from jax.experimental import pallas as pl
from jax.experimental.pallas import tpu as pltpu
from jax.sharding import PartitionSpec as P

EPSILON = 1e-06
MESH = pl.DeviceIdType.MESH
VMEM_LIMIT = 62 * 1024 * 1024


def normed_token_rows(matrix, gain):
    return matrix * lax.rsqrt(jnp.mean(matrix * matrix, axis=-1, keepdims=True) + EPSILON) * gain


PIECES = 2


def place_slots(rows, experts, groups, halves, routes_ref, shares_ref, pick_refs, high_refs, low_refs):
    top_count = routes_ref.shape[0]
    half = experts // 2

    def column(row):
        return jnp.transpose(jnp.broadcast_to(row, (rows, rows)))[:, :1]

    lanes = lax.broadcasted_iota(jnp.int32, (rows, max(experts, 128)), 1).astype(jnp.float32)
    names = [column(routes_ref[k : k + 1].astype(jnp.float32)) for k in range(top_count)]
    shares = [column(shares_ref[k : k + 1]) for k in range(top_count)]
    marks = [jnp.where(name == lanes, 1.0, 0.0) for name in names]
    earlier = lax.broadcasted_iota(jnp.int32, (rows, rows), 1) < lax.broadcasted_iota(jnp.int32, (rows, rows), 0)
    before = jnp.dot(
        jnp.where(earlier, 1.0, 0.0).astype(jnp.bfloat16),
        sum(marks).astype(jnp.bfloat16),
        preferred_element_type=jnp.float32,
    )
    ranks = [jnp.sum(before * mark, axis=1, keepdims=True) for mark in marks]
    slot_ids = lax.broadcasted_iota(jnp.int32, (rows, half * sum(groups)), 1).astype(jnp.float32)
    for which, pick_ref, high_ref, low_ref in zip(halves, pick_refs, high_refs, low_refs):
        start = jnp.asarray(which * half, jnp.int32).astype(jnp.float32)
        picked, share = 0.0, 0.0
        for k in range(top_count):
            name, rank = names[k] - start, ranks[k]
            here = (name >= 0.0) & (name < half)
            slot, first, base = jnp.full((rows, 1), -1.0, jnp.float32), 0, 0
            for g in groups:
                inside = here & (rank >= first) & (rank < first + g)
                slot = jnp.where(inside, base + name * g + rank - first, slot)
                first, base = first + g, base + g * half
            picked = picked + jnp.where(slot == slot_ids, 1.0, 0.0)
            share = share + jnp.where(slot == slot_ids, shares[k], 0.0)
        pick_ref[...] = jnp.transpose(picked).astype(jnp.bfloat16)
        high = share.astype(jnp.bfloat16)
        high_ref[...] = high
        low_ref[...] = (share - high.astype(jnp.float32)).astype(jnp.bfloat16)


def layer_kernel(sp, dp, count, *refs):
    (
        q_hbm, k_hbm, v_hbm, weight_ref, resid_hbm, mixer_hbm, expert_hbm, routes_hbm, shares_hbm,
        gate_hbm, up_hbm, down_hbm, gain_hbm, out_ref,
    ) = refs[:14]
    boxes = refs[14 : 14 + 6 * count]
    sent, served = boxes[:count], boxes[count : 2 * count]
    results, returned = boxes[2 * count : 3 * count], boxes[3 * count : 4 * count]
    lent, lent_back = boxes[4 * count : 5 * count], boxes[5 * count :]
    (
        raw, resid_ref, mixer_ref, expert_ref, gain_ref, routes_ref, shares_ref,
        stage, arrived, out_heads, in_heads, side_heads, flat, full, side_out, side_in,
        projected, tokens, stream_ref, pick_ref, high_ref, low_ref, gate_ref, up_ref, down_ref,
        far_routes, far_shares, far_pick, far_high, far_low, dense, extra_ref,
        load_sem, q_send, q_recv, a_send, a_recv, pass_send, pass_recv, near_sem, far_send, far_recv,
        twin_send, twin_recv, side_send, side_recv, local_sem,
        send_sem, recv_sem, back_send, back_recv, keep_sem, fetch_sem,
        note_send, note_recv, dense_sem, partial_sem, lend_recv, lend_keep, turn_sem,
    ) = refs[14 + 6 * count :]
    _, rows, heads, width = raw.shape
    local_heads = heads // sp
    depth, columns = weight_ref.shape
    me, mate = lax.axis_index("sp"), lax.axis_index("dp")
    parity, core = lax.rem(me, 2), lax.rem(mate, 2)
    side, twin = me + 1 - 2 * parity, mate + 1 - 2 * core
    ys = dp // 2
    own_y = lax.div(mate, 2)
    n, own = sp * dp, me * dp + mate
    half, plane = n // 2, n // 4
    level = lax.div(own, plane)
    spot = lax.rem(own, plane)
    my_half = lax.div(level, 2)
    near_base, far_base = my_half * half, (1 - my_half) * half
    local = own - near_base
    partner = (3 - level) * plane + spot
    inner = level == 1 + my_half
    outer = level != 1 + my_half

    barrier = pltpu.get_barrier_semaphore()

    def greet(k, carry):
        other = lax.rem(own + k, n)
        pl.semaphore_signal(
            barrier, inc=1, device_id={"sp": lax.div(other, dp), "dp": lax.rem(other, dp)}, device_id_type=MESH
        )
        return carry

    lax.fori_loop(1, n, greet, 0)
    pairs = [
        (q_hbm, raw.at[0]), (k_hbm, raw.at[1]), (v_hbm, raw.at[2]), (routes_hbm, routes_ref),
        (shares_hbm, shares_ref), (weight_ref, full.at[core]), (resid_hbm, resid_ref), (mixer_hbm, mixer_ref),
        (expert_hbm, expert_ref), (gain_hbm, gain_ref),
    ]
    loads = [pltpu.make_async_copy(src, dst, load_sem.at[i]) for i, (src, dst) in enumerate(pairs)]
    for load in loads:
        load.start()
    for t in range(3):
        loads[t].wait()
        stage[t] = jnp.transpose(raw[t], (1, 0, 2))
    pl.semaphore_wait(barrier, n - 1)

    def await_bytes(ref, sem):
        pltpu.make_async_copy(ref, ref, sem).wait()

    def remote(src, dst, send, recv, device):
        return pltpu.make_async_remote_copy(
            src_ref=src, dst_ref=dst, send_sem=send, recv_sem=recv, device_id=device, device_id_type=MESH
        )

    def send_heads(t, h):
        def push(i, carry):
            k = sp // 2 + (1 - 2 * lax.rem(i, 2)) * lax.div(i + 1, 2)
            target = lax.rem(me + k, sp)
            remote(
                stage.at[t, target * local_heads + h], arrived.at[t, h, me], q_send.at[h], q_recv.at[h],
                {"sp": target},
            ).start()
            return carry

        lax.fori_loop(0, sp - 1, push, 0)

    others = pl.ds(0, sp - 1)
    span = depth // 2 // PIECES

    def piece_rows(owner, j):
        return pl.ds(pl.multiple_of(owner * (depth // 2) + j * span, span), span)

    def far(d, owner, j):
        where = piece_rows(owner, j)
        return remote(
            weight_ref.at[where], full.at[1 + d, where], far_send.at[d - 1, owner, j], far_recv.at[d - 1, j],
            {"dp": lax.rem(own_y + d, ys) * 2 + owner},
        )

    def far_in(d, j):
        where = full.at[1 + d, piece_rows(core, j)]
        return remote(where, where, far_send.at[d - 1, 0, j], far_recv.at[d - 1, j], {"dp": twin})

    def to_twin(d, j):
        where = full.at[1 + d, piece_rows(core, j)]
        return remote(where, where, twin_send.at[d - 1, j], twin_recv.at[d - 1, j], {"dp": twin})

    near = remote(weight_ref, full.at[core], near_sem.at[0], near_sem.at[1], {"dp": twin})
    for t in range(3):
        send_heads(t, 0)

    @pl.when(core == parity)
    def _():
        for j in range(PIECES):
            for d in range(1, ys):
                for owner in range(2):
                    far(d, owner, j).start()

    near.start()
    keep_heads = [
        pltpu.make_async_copy(stage.at[t, me * local_heads + h], arrived.at[t, h, me], local_sem.at[t, h])
        for t in range(3)
        for h in range(local_heads)
    ]
    for copy in keep_heads:
        copy.start()
    for h in range(1, local_heads):
        for t in range(3):
            send_heads(t, h)
    fetches = [
        pltpu.make_async_copy(src, dst, fetch_sem.at[i])
        for i, (src, dst) in enumerate(((gate_hbm, gate_ref), (up_hbm, up_ref), (down_hbm, down_ref)))
    ]
    loads[3].wait()
    loads[4].wait()

    def device(target):
        return {"sp": lax.div(target, dp), "dp": lax.rem(target, dp)}

    notes = [
        remote(src, dst, note_send.at[i], note_recv.at[i], device(partner))
        for i, (src, dst) in enumerate(((routes_ref, far_routes), (shares_ref, far_shares)))
    ]
    groups = [box.shape[1] for box in sent]

    @pl.when(inner)
    def _():
        for note in notes:
            note.start()

    place_slots(
        rows, n, groups, [0, 1], routes_ref, shares_ref,
        *[[ref.at[i] for i in range(2)] for ref in (pick_ref, high_ref, low_ref)],
    )

    block = rows * max(1, min(sp, 256 // rows))
    per = block // rows
    length = sp * rows
    scale = width ** (-0.5)
    tri_row = lax.broadcasted_iota(jnp.int32, (block, block), 0)
    tri_col = lax.broadcasted_iota(jnp.int32, (block, block), 1)
    suffix_ones = (tri_row >= tri_col).astype(jnp.bfloat16)
    is_past = tri_col < tri_row

    def answer(h, target):
        return remote(
            out_heads.at[h, target], in_heads.at[h, me], a_send.at[h], a_recv.at[h, me], {"sp": target}
        )

    def expect(h, source):
        return remote(
            out_heads.at[h, source], in_heads.at[h, source], a_send.at[h], a_recv.at[h, source], {"sp": source}
        )

    def hand_on(h, source):
        return remote(
            in_heads.at[h, source], side_heads.at[h, source], pass_send.at[h], pass_recv.at[h], {"sp": side}
        )

    def attend_head(h, between):
        def piece(t, index):
            return arrived[t, h, index * per : (index + 1) * per].reshape(block, width)

        for q_block in range(length // block):
            query = piece(0, q_block)
            total = jnp.zeros((block, width), jnp.float32)
            later = jnp.zeros((block, 1), jnp.float32)
            for k_block in range(q_block, -1, -1):
                scores = (
                    lax.dot_general(
                        query, piece(1, k_block), (((1,), (1,)), ((), ())),
                        preferred_element_type=jnp.float32,
                    )
                    * scale
                )
                soft = jnp.maximum(scores, 0.0) + jnp.log(1.0 + jnp.exp(-jnp.abs(scores)))
                if k_block == q_block:
                    soft = jnp.where(is_past, soft, 0.0)
                high = soft.astype(jnp.bfloat16)
                low = (soft - high.astype(jnp.float32)).astype(jnp.bfloat16)
                suffix = jnp.dot(high, suffix_ones, preferred_element_type=jnp.float32) + jnp.dot(
                    low, suffix_ones, preferred_element_type=jnp.float32
                )
                weights = jnp.exp(scores - suffix - later)
                if k_block == q_block:
                    weights = jnp.where(is_past, weights, 0.0)
                total = total + jnp.dot(
                    weights.astype(jnp.bfloat16), piece(2, k_block), preferred_element_type=jnp.float32
                )
                if k_block > 0:
                    later = later + suffix[:, :1]
            out_heads[h, q_block * per : (q_block + 1) * per] = total.astype(jnp.bfloat16).reshape(
                per, rows, width
            )
            if q_block:
                send_answers(h, q_block - 1)
            if q_block == length // block // 2:
                between()
        send_answers(h, length // block - 1)
        keep_answer(h).start()

    def send_answers(h, q_block):
        for target in range(q_block * per, (q_block + 1) * per):

            @pl.when(me != target)
            def _():
                answer(h, target).start()

    def keep_answer(h):
        return pltpu.make_async_copy(out_heads.at[h, me], in_heads.at[h, me], local_sem.at[3, h])

    def pass_on(j):
        for d in range(1, ys):
            far_in(d, j).wait_recv()
            to_twin(d, j).start()

    for copy in keep_heads:
        copy.wait()
    def follow_all(h):
        keep_answer(h).wait()
        hand_on(h, me).start()

        def follow(k, carry):
            source = lax.rem(me + k, sp)
            expect(h, source).wait_recv()
            hand_on(h, source).start()
            return carry

        lax.fori_loop(1, sp, follow, 0)

    for h in range(local_heads):
        await_bytes(arrived.at[:, h, others], q_recv.at[h])
        attend_head(h, (lambda: follow_all(h - 1)) if h else (lambda: None))
    for j in range(PIECES - 1):
        pass_on(j)
    follow_all(local_heads - 1)
    pass_on(PIECES - 1)
    for copy in fetches:
        copy.start()

    @pl.when(inner)
    def _():
        for note in notes:
            note.wait()
        place_slots(rows, n, groups, [my_half], far_routes, far_shares, [far_pick], [far_high], [far_low])

    def fill(ref, first):
        for source in range(sp):
            for h in range(local_heads):
                place = (source * local_heads + h) * width
                flat[first : first + rows, place : place + width] = ref[h, source]

    fill(in_heads, 0)
    for h in range(local_heads):
        await_bytes(side_heads.at[h], pass_recv.at[h])
    fill(side_heads, rows)
    for d in range(1, ys):
        for j in range(PIECES):
            to_twin(d, j).wait()

    tile = min(columns, 512)
    many = columns // tile

    def split(i):
        return lax.div(i, many), pl.ds(pl.multiple_of(lax.rem(i, many) * tile, tile), tile)

    def place_of(slice_index, i):
        return pl.ds(pl.multiple_of((slice_index * many + lax.rem(i, many)) * tile, tile), tile)

    def hand_back(d):
        return remote(
            side_out.at[d - 1], side_in.at[d - 1], side_send.at[d - 1], side_recv.at[d - 1], {"sp": side}
        )

    for d in range(1, ys):

        @pl.loop(0, many)
        def _(i):
            _, inner = split(i)
            both = jnp.dot(flat[...], full[1 + d, :, inner], preferred_element_type=jnp.float32)
            projected[:, place_of(lax.rem(own_y + ys - d, ys) * 2 + parity, i)] = both[:rows]
            side_out[d - 1, :, inner] = both[rows:].astype(jnp.bfloat16)

        hand_back(d).start()

    loads[5].wait()
    near.wait()

    @pl.loop(0, 2 * many)
    def _(i):
        which, inner = split(i)
        projected[:, place_of(own_y * 2 + which, i)] = jnp.dot(
            flat[:rows], full[which, :, inner], preferred_element_type=jnp.float32
        )

    for load in loads[6:]:
        load.wait()
    for h in range(local_heads):
        await_bytes(stage.at[:, others], q_send.at[h])
        await_bytes(out_heads.at[h, others], a_send.at[h])
        await_bytes(in_heads.at[h], pass_send.at[h])

    @pl.when(core == parity)
    def _():
        for j in range(PIECES):
            for d in range(1, ys):
                for owner in range(2):
                    far(d, owner, j).wait_send()

    for d in range(1, ys):
        hand_back(d).wait()

        @pl.loop(0, many)
        def _(i):
            _, inner = split(i)
            projected[:, place_of(lax.rem(own_y + ys - d, ys) * 2 + 1 - parity, i)] = side_in[
                d - 1, :, inner
            ].astype(jnp.float32)

    def lend(i):
        part = pl.ds(pl.multiple_of(i * 16, 16), 16)
        return remote(tokens.at[part], dense.at[part], dense_sem.at[0], dense_sem.at[1], device(partner))

    @pl.loop(0, rows // 16)
    def _(i):
        part = pl.ds(pl.multiple_of(i * 16, 16), 16)
        stream = (
            resid_ref[part].astype(jnp.float32) + normed_token_rows(projected[part], mixer_ref[...])
        ).astype(jnp.bfloat16)
        stream_ref[part] = stream
        tokens[part] = normed_token_rows(stream.astype(jnp.float32), expert_ref[...]).astype(jnp.bfloat16)

        @pl.when(inner & (i > 0))
        def _():
            lend(i - 1).start()

    @pl.when(inner)
    def _():
        lend(rows // 16 - 1).start()

    features = projected.shape[1]
    tile = 512

    def each(number, turn, make, own_place):
        def push(i, carry):
            place = lax.rem(turn + i, number)

            @pl.when(place != own_place)
            def _():
                make(place).start()

            return carry

        lax.fori_loop(0, number, push, 0)

    def outward(a, target):
        return remote(sent[a].at[target], served[a].at[own], send_sem.at[a], recv_sem.at[a], device(target))

    def outward_lent(a, place):
        return remote(
            lent[a].at[place], served[a].at[partner], send_sem.at[a], recv_sem.at[a], device(near_base + place)
        )

    def homeward(a, source):
        return remote(results[a].at[source], returned[a].at[own], back_send.at[a], back_recv.at[a], device(source))

    def homeward_lent(a, place):
        return remote(
            results[a].at[(2 - my_half) * plane + place], lent_back[a].at[local], back_send.at[a], lend_recv.at[a],
            device((1 + my_half) * plane + place),
        )

    def choose(a, pick, source_ref, out, first):
        row = half * sum(groups[:a])
        wanted = pick[row : row + half * groups[a]]

        @pl.loop(0, features // tile)
        def _(i):
            part = pl.ds(pl.multiple_of(i * tile, tile), tile)
            out[a][pl.ds(first, half), :, part] = (
                jnp.dot(wanted, source_ref[:, part], preferred_element_type=jnp.float32)
                .astype(jnp.bfloat16)
                .reshape(half, groups[a], tile)
            )

    own_rows = [pltpu.make_async_copy(sent[a].at[own], served[a].at[own], keep_sem.at[a]) for a in range(count)]
    keeps = [
        pltpu.make_async_copy(results[a].at[own], returned[a].at[own], keep_sem.at[count + a])
        for a in range(count)
    ]
    lent_rows = [
        pltpu.make_async_copy(lent[a].at[local], served[a].at[partner], lend_keep.at[a]) for a in range(count)
    ]
    lent_keeps = [
        pltpu.make_async_copy(results[a].at[partner], lent_back[a].at[local], lend_keep.at[count + a])
        for a in range(count)
    ]
    for a in range(count):
        choose(a, pick_ref.at[my_half], tokens, sent, near_base)
        each(half, local + half // 2, lambda place: outward(a, near_base + place), local)
        own_rows[a].start()

    @pl.when(outer)
    def _():
        for a in range(count):
            choose(a, pick_ref.at[1 - my_half], tokens, sent, far_base)
        pl.semaphore_wait(turn_sem, plane)
        for a in range(count):
            each(half, local + half // 2, lambda place: outward(a, far_base + place), -1)

    @pl.when(inner)
    def _():
        await_bytes(tokens, dense_sem.at[0])

        def release(i, carry):
            pl.semaphore_signal(
                turn_sem, inc=1, device_id=device(3 * my_half * plane + i), device_id_type=MESH
            )
            return carry

        lax.fori_loop(0, plane, release, 0)
        await_bytes(dense, dense_sem.at[1])
        for a in range(count):
            choose(a, far_pick, dense, lent, 0)
            each(half, local + half // 2, lambda place: outward_lent(a, place), local)
            lent_rows[a].start()

    def await_blocks(boxes, sems, a):
        @pl.when(inner)
        def _():
            await_bytes(boxes[a].at[pl.ds(0, n - 2)], sems.at[a])

        @pl.when(outer)
        def _():
            await_bytes(boxes[a].at[pl.ds(0, n - 1)], sems.at[a])

    def give_lent(a):
        each(plane, spot + plane // 2, lambda place: homeward_lent(a, place), jnp.where(inner, spot, -1))

        @pl.when(inner)
        def _():
            lent_keeps[a].start()

    def give_far(a):
        each(plane, spot + plane // 2, lambda place: homeward(a, 3 * (1 - my_half) * plane + place), -1)

    def give_near(a):
        each(half, local + half // 2, lambda place: homeward(a, near_base + place), local)
        keeps[a].start()

    for a in range(count):
        own_rows[a].wait()

        @pl.when(inner)
        def _():
            lent_rows[a].wait()

        await_blocks(served, recv_sem, a)
        if a == 0:
            for copy in fetches:
                copy.wait()
        many = served[a].shape[1]
        taken = served[a][...].reshape(n * many, features)
        gate = jnp.dot(taken, gate_ref[...], preferred_element_type=jnp.float32)
        upward = jnp.dot(taken, up_ref[...], preferred_element_type=jnp.float32)
        hidden = (gate / (1.0 + jnp.exp(-gate)) * upward).astype(jnp.bfloat16)
        for i in range(features // tile):
            part = slice(i * tile, (i + 1) * tile)
            results[a][:, :, part] = (
                jnp.dot(hidden, down_ref[:, part], preferred_element_type=jnp.float32)
                .astype(jnp.bfloat16)
                .reshape(n, many, tile)
            )
        give_lent(a)

        @pl.when(inner)
        def _():
            give_far(a)

    for a in range(count):

        @pl.when(outer)
        def _():
            give_far(a)

        give_near(a)

    def gather(box, first, high, low, a, part):
        columns_of = slice(half * sum(groups[:a]), half * sum(groups[: a + 1]))
        block = box[a][pl.ds(first, half), :, part].reshape(half * groups[a], tile)
        return jnp.dot(high[:, columns_of], block, preferred_element_type=jnp.float32) + jnp.dot(
            low[:, columns_of], block, preferred_element_type=jnp.float32
        )

    def settle_up(i):
        part = pl.ds(pl.multiple_of(i * tile, tile), tile)
        return remote(
            dense.at[:, part], extra_ref.at[:, part], partial_sem.at[0], partial_sem.at[1], device(partner)
        )

    @pl.when(inner)
    def _():
        for a in range(count):
            lent_keeps[a].wait()
            await_bytes(lent_back[a].at[pl.ds(0, half - 1)], lend_recv.at[a])

        @pl.loop(0, features // tile)
        def _(i):
            part = pl.ds(pl.multiple_of(i * tile, tile), tile)
            dense[:, part] = sum(
                gather(lent_back, 0, far_high, far_low, a, part) for a in range(count)
            ).astype(jnp.bfloat16)

            @pl.when(i > 0)
            def _():
                settle_up(i - 1).start()

        settle_up(features // tile - 1).start()

    for a in range(count):
        keeps[a].wait()

        @pl.when(inner)
        def _():
            await_bytes(returned[a].at[pl.ds(0, half - 1)], back_recv.at[a])

        @pl.when(outer)
        def _():
            await_bytes(returned[a].at[pl.ds(0, n - 1)], back_recv.at[a])

        @pl.loop(0, features // tile)
        def _(i):
            part = pl.ds(pl.multiple_of(i * tile, tile), tile)
            total = gather(returned, near_base, high_ref.at[my_half], low_ref.at[my_half], a, part)
            projected[:, part] = total if a == 0 else projected[:, part] + total

        @pl.when(outer)
        def _():
            @pl.loop(0, features // tile)
            def _(i):
                part = pl.ds(pl.multiple_of(i * tile, tile), tile)
                projected[:, part] += gather(
                    returned, far_base, high_ref.at[1 - my_half], low_ref.at[1 - my_half], a, part
                )

    for a in range(count):
        await_blocks(sent, send_sem, a)
        await_blocks(results, back_send, a)

    @pl.when(inner)
    def _():
        await_bytes(dense, partial_sem.at[0])
        await_bytes(extra_ref, partial_sem.at[1])

        @pl.loop(0, rows // 16)
        def _(i):
            part = pl.ds(pl.multiple_of(i * 16, 16), 16)
            projected[part] += extra_ref[part].astype(jnp.float32)

    @pl.loop(0, rows // 16)
    def _(i):
        part = pl.ds(pl.multiple_of(i * 16, 16), 16)
        out_ref[part] = (
            stream_ref[part].astype(jnp.float32) + normed_token_rows(projected[part], gain_ref[...])
        ).astype(jnp.bfloat16)


def layer(
    query, key, value, weight, residual, mixer_gain, expert_gain, routes, shares, gate, up, down, gain, groups
):
    sp, dp = lax.axis_size("sp"), lax.axis_size("dp")
    n = sp * dp
    rows, heads, width = query.shape
    depth, columns = weight.shape
    features = residual.shape[1]
    local_heads = heads // sp
    extra = max(dp // 2 - 1, 1)
    slots = n // 2 * sum(groups)
    anywhere = pl.BlockSpec(memory_space=pl.ANY)
    dma = pltpu.SemaphoreType.DMA
    bf16, f32 = jnp.bfloat16, jnp.float32
    return pl.pallas_call(
        functools.partial(layer_kernel, sp, dp, len(groups)),
        out_shape=pltpu.VMEM((rows, features), bf16),
        in_specs=[anywhere] * 13,
        out_specs=pl.BlockSpec(memory_space=pltpu.VMEM),
        scratch_shapes=[pltpu.VMEM((n, g, features), bf16) for _ in range(4) for g in groups]
        + [pltpu.VMEM((n // 2, g, features), bf16) for _ in range(2) for g in groups]
        + [
            pltpu.VMEM((3, rows, heads, width), bf16),
            pltpu.VMEM((rows, features), bf16),
            pltpu.VMEM((1, features), f32),
            pltpu.VMEM((1, features), f32),
            pltpu.VMEM((1, features), f32),
            pltpu.VMEM(routes.shape, jnp.int32),
            pltpu.VMEM(shares.shape, f32),
            pltpu.VMEM((3, heads, rows, width), bf16),
            pltpu.VMEM((3, local_heads, sp, rows, width), bf16),
            pltpu.VMEM((local_heads, sp, rows, width), bf16),
            pltpu.VMEM((local_heads, sp, rows, width), bf16),
            pltpu.VMEM((local_heads, sp, rows, width), bf16),
            pltpu.VMEM((2 * rows, depth), bf16),
            pltpu.VMEM((2 + extra, depth, columns), bf16),
            pltpu.VMEM((extra, rows, columns), bf16),
            pltpu.VMEM((extra, rows, columns), bf16),
            pltpu.VMEM((rows, features), f32),
            pltpu.VMEM((rows, features), bf16),
            pltpu.VMEM((rows, features), bf16),
            pltpu.VMEM((2, slots, rows), bf16),
            pltpu.VMEM((2, rows, slots), bf16),
            pltpu.VMEM((2, rows, slots), bf16),
            pltpu.VMEM(gate.shape, bf16),
            pltpu.VMEM(up.shape, bf16),
            pltpu.VMEM(down.shape, bf16),
            pltpu.VMEM(routes.shape, jnp.int32),
            pltpu.VMEM(shares.shape, f32),
            pltpu.VMEM((slots, rows), bf16),
            pltpu.VMEM((rows, slots), bf16),
            pltpu.VMEM((rows, slots), bf16),
            pltpu.VMEM((rows, features), bf16),
            pltpu.VMEM((rows, features), bf16),
            dma((10,)),
            dma((local_heads,)),
            dma((local_heads,)),
            dma((local_heads,)),
            dma((local_heads, sp)),
            dma((local_heads,)),
            dma((local_heads,)),
            dma((2,)),
            dma((extra, 2, PIECES)),
            dma((extra, PIECES)),
            dma((extra, PIECES)),
            dma((extra, PIECES)),
            dma((extra,)),
            dma((extra,)),
            dma((4, local_heads)),
            dma((len(groups),)),
            dma((len(groups),)),
            dma((len(groups),)),
            dma((len(groups),)),
            dma((2 * len(groups),)),
            dma((3,)),
            dma((2,)),
            dma((2,)),
            dma((2,)),
            dma((2,)),
            dma((len(groups),)),
            dma((2 * len(groups),)),
            pltpu.SemaphoreType.REGULAR,
        ],
        compiler_params=pltpu.CompilerParams(
            collective_id=0, has_side_effects=True, vmem_limit_bytes=VMEM_LIMIT
        ),
    )(
        query, key, value, weight, residual, mixer_gain[None], expert_gain[None], routes, shares,
        gate, up, down, gain[None],
    )


def local(
    queries,
    key_rows,
    values,
    residual,
    out_weight,
    mixer_gain,
    expert_gain,
    gate_weight,
    up_weight,
    expert_down_matrix,
    routes,
    route_weight,
    output_gain,
):
    local_rows = queries.shape[1]
    experts = lax.axis_size("sp") * lax.axis_size("dp")
    capacity = max(2, 3 * local_rows // experts)
    groups = [g for g in (capacity // 8 * 8, capacity % 8) if g]
    output = layer(
        queries[0], key_rows[0], values[0], out_weight, residual[0], mixer_gain, expert_gain,
        routes[0].T, route_weight[0].T, gate_weight[0], up_weight[0], expert_down_matrix[0], output_gain, groups,
    )
    return output[None]


def solution(mesh):
    in_specs = (
        P("dp", "sp", None, None),
        P("dp", "sp", None, None),
        P("dp", "sp", None, None),
        P("dp", "sp", None),
        P(None, "dp"),
        P(),
        P(),
        P(("sp", "dp"), None, None),
        P(("sp", "dp"), None, None),
        P(("sp", "dp"), None, None),
        P("dp", "sp", None),
        P("dp", "sp", None),
        P(),
    )
    out_specs = P("dp", "sp", None)
    return jax.shard_map(local, mesh=mesh, in_specs=in_specs, out_specs=out_specs, check_vma=False)
```

```python
import functools

import jax
import jax.numpy as jnp
from jax import lax
from jax.experimental import pallas as pl
from jax.experimental.pallas import tpu as pltpu
from jax.sharding import PartitionSpec as P

EPSILON = 1e-06
MESH = pl.DeviceIdType.MESH
VMEM_LIMIT = 62 * 1024 * 1024


def normed_token_rows(matrix, gain):
    return matrix * lax.rsqrt(jnp.mean(matrix * matrix, axis=-1, keepdims=True) + EPSILON) * gain


PIECES = 2


def place_slots(rows, experts, groups, halves, routes_ref, shares_ref, pick_refs, high_refs, low_refs):
    top_count = routes_ref.shape[0]
    half = experts // 2

    def column(row):
        return jnp.transpose(jnp.broadcast_to(row, (rows, rows)))[:, :1]

    lanes = lax.broadcasted_iota(jnp.int32, (rows, max(experts, 128)), 1).astype(jnp.float32)
    names = [column(routes_ref[k : k + 1].astype(jnp.float32)) for k in range(top_count)]
    shares = [column(shares_ref[k : k + 1]) for k in range(top_count)]
    marks = [jnp.where(name == lanes, 1.0, 0.0) for name in names]
    earlier = lax.broadcasted_iota(jnp.int32, (rows, rows), 1) < lax.broadcasted_iota(jnp.int32, (rows, rows), 0)
    before = jnp.dot(
        jnp.where(earlier, 1.0, 0.0).astype(jnp.bfloat16),
        sum(marks).astype(jnp.bfloat16),
        preferred_element_type=jnp.float32,
    )
    ranks = [jnp.sum(before * mark, axis=1, keepdims=True) for mark in marks]
    slot_ids = lax.broadcasted_iota(jnp.int32, (rows, half * sum(groups)), 1).astype(jnp.float32)
    for which, pick_ref, high_ref, low_ref in zip(halves, pick_refs, high_refs, low_refs):
        start = jnp.asarray(which * half, jnp.int32).astype(jnp.float32)
        picked, share = 0.0, 0.0
        for k in range(top_count):
            name, rank = names[k] - start, ranks[k]
            here = (name >= 0.0) & (name < half)
            slot, first, base = jnp.full((rows, 1), -1.0, jnp.float32), 0, 0
            for g in groups:
                inside = here & (rank >= first) & (rank < first + g)
                slot = jnp.where(inside, base + name * g + rank - first, slot)
                first, base = first + g, base + g * half
            picked = picked + jnp.where(slot == slot_ids, 1.0, 0.0)
            share = share + jnp.where(slot == slot_ids, shares[k], 0.0)
        pick_ref[...] = jnp.transpose(picked).astype(jnp.bfloat16)
        high = share.astype(jnp.bfloat16)
        high_ref[...] = high
        low_ref[...] = (share - high.astype(jnp.float32)).astype(jnp.bfloat16)


def layer_kernel(sp, dp, count, *refs):
    (
        q_hbm, k_hbm, v_hbm, weight_ref, resid_hbm, mixer_hbm, expert_hbm, routes_hbm, shares_hbm,
        gate_hbm, up_hbm, down_hbm, gain_hbm, out_ref,
    ) = refs[:14]
    boxes = refs[14 : 14 + 6 * count]
    sent, served = boxes[:count], boxes[count : 2 * count]
    results, returned = boxes[2 * count : 3 * count], boxes[3 * count : 4 * count]
    lent, lent_back = boxes[4 * count : 5 * count], boxes[5 * count :]
    (
        raw, stream_ref, mixer_ref, expert_ref, gain_ref, routes_ref, shares_ref,
        stage, arrived, out_heads, in_heads, side_heads, flat, full, side_out, side_in, peer_heads, peer_out, peer_in,
        projected, tokens, pick_ref, high_ref, low_ref, gate_ref, up_ref, down_ref,
        far_routes, far_shares, far_pick, far_high, far_low, dense, extra_ref,
        load_sem, q_send, q_recv, a_send, a_recv, pass_send, pass_recv, near_sem, far_send, far_recv,
        twin_send, twin_recv, side_send, side_recv, local_sem,
        send_sem, recv_sem, back_send, back_recv, keep_sem, fetch_sem,
        note_send, note_recv, dense_sem, partial_sem, lend_recv, lend_keep, turn_sem,
        ask_send, ask_recv, peer_send, peer_recv,
    ) = refs[14 + 6 * count :]
    _, rows, heads, width = raw.shape
    local_heads = heads // sp
    depth, columns = weight_ref.shape
    me, mate = lax.axis_index("sp"), lax.axis_index("dp")
    parity, core = lax.rem(me, 2), lax.rem(mate, 2)
    side, twin = me + 1 - 2 * parity, mate + 1 - 2 * core
    ys = dp // 2
    own_y = lax.div(mate, 2)
    n, own = sp * dp, me * dp + mate
    half, plane = n // 2, n // 4
    level = lax.div(own, plane)
    spot = lax.rem(own, plane)
    my_half = lax.div(level, 2)
    near_base, far_base = my_half * half, (1 - my_half) * half
    local = own - near_base
    partner = (3 - level) * plane + spot
    inner = level == 1 + my_half
    outer = level != 1 + my_half

    barrier = pltpu.get_barrier_semaphore()

    def greet(k, carry):
        other = lax.rem(own + k, n)
        pl.semaphore_signal(
            barrier, inc=1, device_id={"sp": lax.div(other, dp), "dp": lax.rem(other, dp)}, device_id_type=MESH
        )
        return carry

    lax.fori_loop(1, n, greet, 0)
    pairs = [
        (q_hbm, raw.at[0]), (k_hbm, raw.at[1]), (v_hbm, raw.at[2]), (routes_hbm, routes_ref),
        (shares_hbm, shares_ref), (weight_ref, full.at[core]), (resid_hbm, stream_ref), (mixer_hbm, mixer_ref),
        (expert_hbm, expert_ref), (gain_hbm, gain_ref),
    ]
    loads = [pltpu.make_async_copy(src, dst, load_sem.at[i]) for i, (src, dst) in enumerate(pairs)]
    for load in loads:
        load.start()
    for t in range(3):
        loads[t].wait()
        stage[t] = jnp.transpose(raw[t], (1, 0, 2))
    pl.semaphore_wait(barrier, n - 1)

    def await_bytes(ref, sem):
        pltpu.make_async_copy(ref, ref, sem).wait()

    def remote(src, dst, send, recv, device):
        return pltpu.make_async_remote_copy(
            src_ref=src, dst_ref=dst, send_sem=send, recv_sem=recv, device_id=device, device_id_type=MESH
        )

    def send_heads(t, h):
        def push(i, carry):
            k = sp // 2 + (1 - 2 * lax.rem(i, 2)) * lax.div(i + 1, 2)
            target = lax.rem(me + k, sp)
            remote(
                stage.at[t, target * local_heads + h], arrived.at[t, h, me], q_send.at[h], q_recv.at[h],
                {"sp": target},
            ).start()
            return carry

        lax.fori_loop(0, sp - 1, push, 0)

    others = pl.ds(0, sp - 1)
    span = depth // 2 // PIECES

    def piece_rows(owner, j):
        return pl.ds(pl.multiple_of(owner * (depth // 2) + j * span, span), span)

    def far(d, owner, j):
        where = piece_rows(owner, j)
        return remote(
            weight_ref.at[where], full.at[1 + d, where], far_send.at[d - 1, owner, j], far_recv.at[d - 1, j],
            {"dp": lax.rem(own_y + d, ys) * 2 + owner},
        )

    def far_in(d, j):
        where = full.at[1 + d, piece_rows(core, j)]
        return remote(where, where, far_send.at[d - 1, 0, j], far_recv.at[d - 1, j], {"dp": twin})

    def to_twin(d, j):
        where = full.at[1 + d, piece_rows(core, j)]
        return remote(where, where, twin_send.at[d - 1, j], twin_recv.at[d - 1, j], {"dp": twin})

    near = remote(weight_ref, full.at[core], near_sem.at[0], near_sem.at[1], {"dp": twin})
    for t in range(3):
        send_heads(t, 0)

    @pl.when(core == parity)
    def _():
        for j in range(PIECES):
            for d in range(1, ys):
                for owner in range(2):
                    far(d, owner, j).start()

    near.start()
    keep_heads = [
        pltpu.make_async_copy(stage.at[t, me * local_heads + h], arrived.at[t, h, me], local_sem.at[t, h])
        for t in range(3)
        for h in range(local_heads)
    ]
    for copy in keep_heads:
        copy.start()
    for h in range(1, local_heads):
        for t in range(3):
            send_heads(t, h)
    fetches = [
        pltpu.make_async_copy(src, dst, fetch_sem.at[i])
        for i, (src, dst) in enumerate(((gate_hbm, gate_ref), (up_hbm, up_ref), (down_hbm, down_ref)))
    ]
    loads[3].wait()
    loads[4].wait()

    def device(target):
        return {"sp": lax.div(target, dp), "dp": lax.rem(target, dp)}

    notes = [
        remote(src, dst, note_send.at[i], note_recv.at[i], device(partner))
        for i, (src, dst) in enumerate(((routes_ref, far_routes), (shares_ref, far_shares)))
    ]
    groups = [box.shape[1] for box in sent]

    @pl.when(inner)
    def _():
        for note in notes:
            note.start()

    place_slots(
        rows, n, groups, [0, 1], routes_ref, shares_ref,
        *[[ref.at[i] for i in range(2)] for ref in (pick_ref, high_ref, low_ref)],
    )

    part_rows = rows // 2
    block = rows * max(1, min(sp, 256 // rows))
    per = block // rows
    length = sp * rows
    scale = width ** (-0.5)
    tri_row = lax.broadcasted_iota(jnp.int32, (block, block), 0)
    tri_col = lax.broadcasted_iota(jnp.int32, (block, block), 1)
    suffix_ones = (tri_row >= tri_col).astype(jnp.bfloat16)
    is_past = tri_col < tri_row

    def answer(h, target):
        return remote(
            out_heads.at[h, target], in_heads.at[h, me], a_send.at[h], a_recv.at[h, me], {"sp": target}
        )

    def expect(h, source):
        return remote(
            out_heads.at[h, source], in_heads.at[h, source], a_send.at[h], a_recv.at[h, source], {"sp": source}
        )

    def hand_on(h, source):
        remote(
            in_heads.at[h, source, :part_rows], side_heads.at[h, source], pass_send.at[h], pass_recv.at[h],
            {"sp": side},
        ).start()
        for d in range(1, ys):
            remote(
                in_heads.at[h, source, part_rows:], peer_heads.at[d - 1, h, source], ask_send.at[d - 1, h],
                ask_recv.at[d - 1, h], {"dp": lax.rem(own_y + ys - d, ys) * 2 + core},
            ).start()

    def attend_head(h, between):
        def piece(t, index):
            return arrived[t, h, index * per : (index + 1) * per].reshape(block, width)

        for q_block in range(length // block):
            query = piece(0, q_block)
            total = jnp.zeros((block, width), jnp.float32)
            later = jnp.zeros((block, 1), jnp.float32)
            for k_block in range(q_block, -1, -1):
                scores = (
                    lax.dot_general(
                        query, piece(1, k_block), (((1,), (1,)), ((), ())),
                        preferred_element_type=jnp.float32,
                    )
                    * scale
                )
                soft = jnp.maximum(scores, 0.0) + jnp.log(1.0 + jnp.exp(-jnp.abs(scores)))
                if k_block == q_block:
                    soft = jnp.where(is_past, soft, 0.0)
                high = soft.astype(jnp.bfloat16)
                low = (soft - high.astype(jnp.float32)).astype(jnp.bfloat16)
                suffix = jnp.dot(high, suffix_ones, preferred_element_type=jnp.float32) + jnp.dot(
                    low, suffix_ones, preferred_element_type=jnp.float32
                )
                weights = jnp.exp(scores - suffix - later)
                if k_block == q_block:
                    weights = jnp.where(is_past, weights, 0.0)
                total = total + jnp.dot(
                    weights.astype(jnp.bfloat16), piece(2, k_block), preferred_element_type=jnp.float32
                )
                if k_block > 0:
                    later = later + suffix[:, :1]
            out_heads[h, q_block * per : (q_block + 1) * per] = total.astype(jnp.bfloat16).reshape(
                per, rows, width
            )
            if q_block:
                send_answers(h, q_block - 1)
            if q_block == length // block // 2:
                between()
        send_answers(h, length // block - 1)
        keep_answer(h).start()

    def send_answers(h, q_block):
        for target in range(q_block * per, (q_block + 1) * per):

            @pl.when(me != target)
            def _():
                answer(h, target).start()

    def keep_answer(h):
        return pltpu.make_async_copy(out_heads.at[h, me], in_heads.at[h, me], local_sem.at[3, h])

    def pass_on(j):
        for d in range(1, ys):
            far_in(d, j).wait_recv()
            to_twin(d, j).start()

    for copy in keep_heads:
        copy.wait()
    def follow_all(h):
        keep_answer(h).wait()
        hand_on(h, me)

        def follow(k, carry):
            for source in (me + k, me - k):

                @pl.when((source >= 0) & (source < sp))
                def _():
                    expect(h, source).wait_recv()
                    hand_on(h, source)

            return carry

        lax.fori_loop(1, sp, follow, 0)

    for h in range(local_heads):
        await_bytes(arrived.at[:, h, others], q_recv.at[h])
        attend_head(h, (lambda: follow_all(h - 1)) if h else (lambda: None))
    for j in range(PIECES - 1):
        pass_on(j)
    follow_all(local_heads - 1)
    pass_on(PIECES - 1)
    for copy in fetches:
        copy.start()

    @pl.when(inner)
    def _():
        for note in notes:
            note.wait()
        place_slots(rows, n, groups, [my_half], far_routes, far_shares, [far_pick], [far_high], [far_low])

    def fill(ref, first):
        for source in range(sp):
            for h in range(local_heads):
                place = (source * local_heads + h) * width
                block = ref[h, source]
                flat[first : first + block.shape[0], place : place + width] = block

    fill(in_heads, part_rows)
    for h in range(local_heads):
        await_bytes(side_heads.at[h], pass_recv.at[h])
    fill(side_heads, 0)
    for d in range(1, ys):
        for j in range(PIECES):
            to_twin(d, j).wait()

    tile = min(columns, 512)
    many = columns // tile

    def inner_part(i):
        return pl.ds(pl.multiple_of(i * tile, tile), tile)

    def place_of(slice_index, i):
        return pl.ds(pl.multiple_of((slice_index * many + i) * tile, tile), tile)

    def origin(d):
        return lax.rem(own_y + ys - d, ys) * 2

    def hand_back(d, inner):
        return remote(
            side_out.at[d - 1, :, inner], side_in.at[d - 1, :, inner], side_send.at[d - 1], side_recv.at[d - 1],
            {"sp": side},
        )

    def reply(d, inner):
        return remote(
            peer_out.at[d - 1, :, inner], peer_in.at[d - 1, :, inner], peer_send.at[d - 1], peer_recv.at[d - 1],
            {"dp": lax.rem(own_y + d, ys) * 2 + core},
        )

    for d in range(1, ys):

        @pl.loop(0, many)
        def _(i):
            inner = inner_part(i)
            both = jnp.dot(flat[: part_rows + rows], full[1 + d, :, inner], preferred_element_type=jnp.float32)
            projected[:, place_of(origin(d) + parity, i)] = both[part_rows:]
            side_out[d - 1, :, inner] = both[:part_rows].astype(jnp.bfloat16)

            @pl.when(i > 0)
            def _():
                hand_back(d, inner_part(i - 1)).start()

        hand_back(d, pl.ds((many - 1) * tile, tile)).start()

    for d in range(1, ys):
        for h in range(local_heads):
            await_bytes(peer_heads.at[d - 1, h], ask_recv.at[d - 1, h])
        fill(peer_heads.at[d - 1], part_rows + rows + (d - 1) * part_rows)
    loads[5].wait()
    near.wait()

    @pl.loop(0, many)
    def _(i):
        inner = inner_part(i)
        both = jnp.dot(flat[part_rows:], full[1 - parity, :, inner], preferred_element_type=jnp.float32)
        projected[:, place_of(own_y * 2 + 1 - parity, i)] = both[:rows]
        for d in range(1, ys):
            peer_out[d - 1, :, inner] = both[
                rows + (d - 1) * part_rows : rows + d * part_rows
            ].astype(jnp.bfloat16)

        @pl.when(i > 0)
        def _():
            for d in range(1, ys):
                reply(d, inner_part(i - 1)).start()

    for d in range(1, ys):
        reply(d, pl.ds((many - 1) * tile, tile)).start()

    @pl.loop(0, many)
    def _(i):
        projected[:, place_of(own_y * 2 + parity, i)] = jnp.dot(
            flat[part_rows : part_rows + rows], full[parity, :, inner_part(i)], preferred_element_type=jnp.float32
        )

    for load in loads[6:]:
        load.wait()
    for h in range(local_heads):
        await_bytes(stage.at[:, others], q_send.at[h])
        await_bytes(out_heads.at[h, others], a_send.at[h])
        await_bytes(side_heads.at[h], pass_send.at[h])
        for d in range(1, ys):
            await_bytes(peer_heads.at[d - 1, h], ask_send.at[d - 1, h])

    @pl.when(core == parity)
    def _():
        for j in range(PIECES):
            for d in range(1, ys):
                for owner in range(2):
                    far(d, owner, j).wait_send()

    for d in range(1, ys):
        await_bytes(side_in.at[d - 1], side_recv.at[d - 1])
        await_bytes(side_out.at[d - 1], side_send.at[d - 1])
        await_bytes(peer_in.at[d - 1], peer_recv.at[d - 1])
        await_bytes(peer_out.at[d - 1], peer_send.at[d - 1])

        @pl.loop(0, many)
        def _(i):
            outer_part = place_of(origin(d) + 1 - parity, i)
            projected[:part_rows, outer_part] = side_in[d - 1, :, inner_part(i)].astype(jnp.float32)
            projected[part_rows:, outer_part] = peer_in[d - 1, :, inner_part(i)].astype(jnp.float32)

    def lend(i):
        part = pl.ds(pl.multiple_of(i * 16, 16), 16)
        return remote(tokens.at[part], dense.at[part], dense_sem.at[0], dense_sem.at[1], device(partner))

    @pl.loop(0, rows // 16)
    def _(i):
        part = pl.ds(pl.multiple_of(i * 16, 16), 16)
        stream = (
            stream_ref[part].astype(jnp.float32) + normed_token_rows(projected[part], mixer_ref[...])
        ).astype(jnp.bfloat16)
        stream_ref[part] = stream
        tokens[part] = normed_token_rows(stream.astype(jnp.float32), expert_ref[...]).astype(jnp.bfloat16)

        @pl.when(inner & (i > 0))
        def _():
            lend(i - 1).start()

    @pl.when(inner)
    def _():
        lend(rows // 16 - 1).start()

    features = projected.shape[1]
    tile = 512

    def each(number, turn, make, own_place):
        def push(i, carry):
            place = lax.rem(turn + i, number)

            @pl.when(place != own_place)
            def _():
                make(place).start()

            return carry

        lax.fori_loop(0, number, push, 0)

    def outward(a, target):
        return remote(sent[a].at[target], served[a].at[own], send_sem.at[a], recv_sem.at[a], device(target))

    def outward_lent(a, place):
        return remote(
            lent[a].at[place], served[a].at[partner], send_sem.at[a], recv_sem.at[a], device(near_base + place)
        )

    def homeward(a, source):
        return remote(results[a].at[source], returned[a].at[own], back_send.at[a], back_recv.at[a], device(source))

    def homeward_lent(a, place):
        return remote(
            results[a].at[(2 - my_half) * plane + place], lent_back[a].at[local], back_send.at[a], lend_recv.at[a],
            device((1 + my_half) * plane + place),
        )

    def choose(a, pick, source_ref, out, first):
        row = half * sum(groups[:a])
        wanted = pick[row : row + half * groups[a]]

        @pl.loop(0, features // tile)
        def _(i):
            part = pl.ds(pl.multiple_of(i * tile, tile), tile)
            out[a][pl.ds(first, half), :, part] = (
                jnp.dot(wanted, source_ref[:, part], preferred_element_type=jnp.float32)
                .astype(jnp.bfloat16)
                .reshape(half, groups[a], tile)
            )

    own_rows = [pltpu.make_async_copy(sent[a].at[own], served[a].at[own], keep_sem.at[a]) for a in range(count)]
    keeps = [
        pltpu.make_async_copy(results[a].at[own], returned[a].at[own], keep_sem.at[count + a])
        for a in range(count)
    ]
    lent_rows = [
        pltpu.make_async_copy(lent[a].at[local], served[a].at[partner], lend_keep.at[a]) for a in range(count)
    ]
    lent_keeps = [
        pltpu.make_async_copy(results[a].at[partner], lent_back[a].at[local], lend_keep.at[count + a])
        for a in range(count)
    ]
    for a in range(count):
        choose(a, pick_ref.at[my_half], tokens, sent, near_base)
        each(half, local + half // 2, lambda place: outward(a, near_base + place), local)
        own_rows[a].start()

    @pl.when(outer)
    def _():
        for a in range(count):
            choose(a, pick_ref.at[1 - my_half], tokens, sent, far_base)
        pl.semaphore_wait(turn_sem, plane)
        for a in range(count):
            each(half, local + half // 2, lambda place: outward(a, far_base + place), -1)

    @pl.when(inner)
    def _():
        await_bytes(tokens, dense_sem.at[0])

        def release(i, carry):
            pl.semaphore_signal(
                turn_sem, inc=1, device_id=device(3 * my_half * plane + i), device_id_type=MESH
            )
            return carry

        lax.fori_loop(0, plane, release, 0)
        await_bytes(dense, dense_sem.at[1])
        for a in range(count):
            choose(a, far_pick, dense, lent, 0)
            each(half, local + half // 2, lambda place: outward_lent(a, place), local)
            lent_rows[a].start()

    def await_blocks(boxes, sems, a):
        @pl.when(inner)
        def _():
            await_bytes(boxes[a].at[pl.ds(0, n - 2)], sems.at[a])

        @pl.when(outer)
        def _():
            await_bytes(boxes[a].at[pl.ds(0, n - 1)], sems.at[a])

    def give_lent(a):
        each(plane, spot + plane // 2, lambda place: homeward_lent(a, place), jnp.where(inner, spot, -1))

        @pl.when(inner)
        def _():
            lent_keeps[a].start()

    def give_far(a):
        each(plane, spot + plane // 2, lambda place: homeward(a, 3 * (1 - my_half) * plane + place), -1)

    def give_near(a):
        each(half, local + half // 2, lambda place: homeward(a, near_base + place), local)
        keeps[a].start()

    for a in range(count):
        own_rows[a].wait()

        @pl.when(inner)
        def _():
            lent_rows[a].wait()

        await_blocks(served, recv_sem, a)
        if a == 0:
            for copy in fetches:
                copy.wait()
        many = served[a].shape[1]
        taken = served[a][...].reshape(n * many, features)
        gate = jnp.dot(taken, gate_ref[...], preferred_element_type=jnp.float32)
        upward = jnp.dot(taken, up_ref[...], preferred_element_type=jnp.float32)
        hidden = (gate / (1.0 + jnp.exp(-gate)) * upward).astype(jnp.bfloat16)
        for i in range(features // tile):
            part = slice(i * tile, (i + 1) * tile)
            results[a][:, :, part] = (
                jnp.dot(hidden, down_ref[:, part], preferred_element_type=jnp.float32)
                .astype(jnp.bfloat16)
                .reshape(n, many, tile)
            )
        give_lent(a)

        @pl.when(inner)
        def _():
            give_far(a)

    for a in range(count):

        @pl.when(outer)
        def _():
            give_far(a)

        give_near(a)

    def gather(box, first, high, low, a, part):
        columns_of = slice(half * sum(groups[:a]), half * sum(groups[: a + 1]))
        block = box[a][pl.ds(first, half), :, part].reshape(half * groups[a], tile)
        return jnp.dot(high[:, columns_of], block, preferred_element_type=jnp.float32) + jnp.dot(
            low[:, columns_of], block, preferred_element_type=jnp.float32
        )

    def settle_up(i):
        part = pl.ds(pl.multiple_of(i * tile, tile), tile)
        return remote(
            dense.at[:, part], extra_ref.at[:, part], partial_sem.at[0], partial_sem.at[1], device(partner)
        )

    @pl.when(inner)
    def _():
        for a in range(count):
            lent_keeps[a].wait()
            await_bytes(lent_back[a].at[pl.ds(0, half - 1)], lend_recv.at[a])

        @pl.loop(0, features // tile)
        def _(i):
            part = pl.ds(pl.multiple_of(i * tile, tile), tile)
            dense[:, part] = sum(
                gather(lent_back, 0, far_high, far_low, a, part) for a in range(count)
            ).astype(jnp.bfloat16)

            @pl.when(i > 0)
            def _():
                settle_up(i - 1).start()

        settle_up(features // tile - 1).start()

    for a in range(count):
        keeps[a].wait()

        @pl.when(inner)
        def _():
            await_bytes(returned[a].at[pl.ds(0, half - 1)], back_recv.at[a])

        @pl.when(outer)
        def _():
            await_bytes(returned[a].at[pl.ds(0, n - 1)], back_recv.at[a])

        @pl.loop(0, features // tile)
        def _(i):
            part = pl.ds(pl.multiple_of(i * tile, tile), tile)
            total = gather(returned, near_base, high_ref.at[my_half], low_ref.at[my_half], a, part)
            projected[:, part] = total if a == 0 else projected[:, part] + total

        @pl.when(outer)
        def _():
            @pl.loop(0, features // tile)
            def _(i):
                part = pl.ds(pl.multiple_of(i * tile, tile), tile)
                projected[:, part] += gather(
                    returned, far_base, high_ref.at[1 - my_half], low_ref.at[1 - my_half], a, part
                )

    for a in range(count):
        await_blocks(sent, send_sem, a)
        await_blocks(results, back_send, a)

    def finish(combined):
        @pl.loop(0, rows // 16)
        def _(i):
            part = pl.ds(pl.multiple_of(i * 16, 16), 16)
            out_ref[part] = (
                stream_ref[part].astype(jnp.float32) + normed_token_rows(combined(part), gain_ref[...])
            ).astype(jnp.bfloat16)

    @pl.when(inner)
    def _():
        await_bytes(dense, partial_sem.at[0])
        await_bytes(extra_ref, partial_sem.at[1])

        finish(lambda part: projected[part] + extra_ref[part].astype(jnp.float32))

    @pl.when(outer)
    def _():
        finish(lambda part: projected[part])


def layer(
    query, key, value, weight, residual, mixer_gain, expert_gain, routes, shares, gate, up, down, gain, groups
):
    sp, dp = lax.axis_size("sp"), lax.axis_size("dp")
    n = sp * dp
    rows, heads, width = query.shape
    depth, columns = weight.shape
    features = residual.shape[1]
    local_heads = heads // sp
    extra = max(dp // 2 - 1, 1)
    slots = n // 2 * sum(groups)
    anywhere = pl.BlockSpec(memory_space=pl.ANY)
    dma = pltpu.SemaphoreType.DMA
    bf16, f32 = jnp.bfloat16, jnp.float32
    return pl.pallas_call(
        functools.partial(layer_kernel, sp, dp, len(groups)),
        out_shape=pltpu.VMEM((rows, features), bf16),
        in_specs=[anywhere] * 13,
        out_specs=pl.BlockSpec(memory_space=pltpu.VMEM),
        scratch_shapes=[pltpu.VMEM((n, g, features), bf16) for _ in range(4) for g in groups]
        + [pltpu.VMEM((n // 2, g, features), bf16) for _ in range(2) for g in groups]
        + [
            pltpu.VMEM((3, rows, heads, width), bf16),
            pltpu.VMEM((rows, features), bf16),
            pltpu.VMEM((1, features), f32),
            pltpu.VMEM((1, features), f32),
            pltpu.VMEM((1, features), f32),
            pltpu.VMEM(routes.shape, jnp.int32),
            pltpu.VMEM(shares.shape, f32),
            pltpu.VMEM((3, heads, rows, width), bf16),
            pltpu.VMEM((3, local_heads, sp, rows, width), bf16),
            pltpu.VMEM((local_heads, sp, rows, width), bf16),
            pltpu.VMEM((local_heads, sp, rows, width), bf16),
            pltpu.VMEM((local_heads, sp, rows // 2, width), bf16),
            pltpu.VMEM(((3 + extra) * (rows // 2), depth), bf16),
            pltpu.VMEM((2 + extra, depth, columns), bf16),
            pltpu.VMEM((extra, rows // 2, columns), bf16),
            pltpu.VMEM((extra, rows // 2, columns), bf16),
            pltpu.VMEM((extra, local_heads, sp, rows // 2, width), bf16),
            pltpu.VMEM((extra, rows // 2, columns), bf16),
            pltpu.VMEM((extra, rows // 2, columns), bf16),
            pltpu.VMEM((rows, features), f32),
            pltpu.VMEM((rows, features), bf16),
            pltpu.VMEM((2, slots, rows), bf16),
            pltpu.VMEM((2, rows, slots), bf16),
            pltpu.VMEM((2, rows, slots), bf16),
            pltpu.VMEM(gate.shape, bf16),
            pltpu.VMEM(up.shape, bf16),
            pltpu.VMEM(down.shape, bf16),
            pltpu.VMEM(routes.shape, jnp.int32),
            pltpu.VMEM(shares.shape, f32),
            pltpu.VMEM((slots, rows), bf16),
            pltpu.VMEM((rows, slots), bf16),
            pltpu.VMEM((rows, slots), bf16),
            pltpu.VMEM((rows, features), bf16),
            pltpu.VMEM((rows, features), bf16),
            dma((10,)),
            dma((local_heads,)),
            dma((local_heads,)),
            dma((local_heads,)),
            dma((local_heads, sp)),
            dma((local_heads,)),
            dma((local_heads,)),
            dma((2,)),
            dma((extra, 2, PIECES)),
            dma((extra, PIECES)),
            dma((extra, PIECES)),
            dma((extra, PIECES)),
            dma((extra,)),
            dma((extra,)),
            dma((4, local_heads)),
            dma((len(groups),)),
            dma((len(groups),)),
            dma((len(groups),)),
            dma((len(groups),)),
            dma((2 * len(groups),)),
            dma((3,)),
            dma((2,)),
            dma((2,)),
            dma((2,)),
            dma((2,)),
            dma((len(groups),)),
            dma((2 * len(groups),)),
            pltpu.SemaphoreType.REGULAR,
            dma((extra, local_heads)),
            dma((extra, local_heads)),
            dma((extra,)),
            dma((extra,)),
        ],
        compiler_params=pltpu.CompilerParams(
            collective_id=0, has_side_effects=True, vmem_limit_bytes=VMEM_LIMIT
        ),
    )(
        query, key, value, weight, residual, mixer_gain[None], expert_gain[None], routes, shares,
        gate, up, down, gain[None],
    )


def local(
    queries,
    key_rows,
    values,
    residual,
    out_weight,
    mixer_gain,
    expert_gain,
    gate_weight,
    up_weight,
    expert_down_matrix,
    routes,
    route_weight,
    output_gain,
):
    local_rows = queries.shape[1]
    experts = lax.axis_size("sp") * lax.axis_size("dp")
    capacity = max(2, 3 * local_rows // experts)
    groups = [g for g in (capacity // 8 * 8, capacity % 8) if g]
    output = layer(
        queries[0], key_rows[0], values[0], out_weight, residual[0], mixer_gain, expert_gain,
        routes[0].T, route_weight[0].T, gate_weight[0], up_weight[0], expert_down_matrix[0], output_gain, groups,
    )
    return output[None]


def solution(mesh):
    in_specs = (
        P("dp", "sp", None, None),
        P("dp", "sp", None, None),
        P("dp", "sp", None, None),
        P("dp", "sp", None),
        P(None, "dp"),
        P(),
        P(),
        P(("sp", "dp"), None, None),
        P(("sp", "dp"), None, None),
        P(("sp", "dp"), None, None),
        P("dp", "sp", None),
        P("dp", "sp", None),
        P(),
    )
    out_specs = P("dp", "sp", None)
    return jax.shard_map(local, mesh=mesh, in_specs=in_specs, out_specs=out_specs, check_vma=False)
```

```python
import functools

import jax
import jax.numpy as jnp
from jax import lax
from jax.experimental import pallas as pl
from jax.experimental.pallas import tpu as pltpu
from jax.sharding import PartitionSpec as P

EPSILON = 1e-06
MESH = pl.DeviceIdType.MESH
VMEM_LIMIT = 62 * 1024 * 1024


def normed_token_rows(matrix, gain):
    return matrix * lax.rsqrt(jnp.mean(matrix * matrix, axis=-1, keepdims=True) + EPSILON) * gain


PIECES = 2


def place_slots(rows, experts, groups, halves, routes_ref, shares_ref, pick_refs, part_refs):
    top_count = routes_ref.shape[0]
    half = experts // 2

    def column(row):
        return jnp.transpose(jnp.broadcast_to(row, (rows, rows)))[:, :1]

    lanes = lax.broadcasted_iota(jnp.int32, (rows, max(experts, 128)), 1).astype(jnp.float32)
    names = [column(routes_ref[k : k + 1].astype(jnp.float32)) for k in range(top_count)]
    shares = [column(shares_ref[k : k + 1]) for k in range(top_count)]
    marks = [jnp.where(name == lanes, 1.0, 0.0) for name in names]
    earlier = lax.broadcasted_iota(jnp.int32, (rows, rows), 1) < lax.broadcasted_iota(jnp.int32, (rows, rows), 0)
    before = jnp.dot(
        jnp.where(earlier, 1.0, 0.0).astype(jnp.bfloat16),
        sum(marks).astype(jnp.bfloat16),
        preferred_element_type=jnp.float32,
    )
    ranks = [jnp.sum(before * mark, axis=1, keepdims=True) for mark in marks]
    slot_ids = lax.broadcasted_iota(jnp.int32, (rows, half * sum(groups)), 1).astype(jnp.float32)
    for which, pick_ref, part_ref in zip(halves, pick_refs, part_refs):
        start = jnp.asarray(which * half, jnp.int32).astype(jnp.float32)
        picked, share = 0.0, 0.0
        for k in range(top_count):
            name, rank = names[k] - start, ranks[k]
            here = (name >= 0.0) & (name < half)
            slot, first, base = jnp.full((rows, 1), -1.0, jnp.float32), 0, 0
            for g in groups:
                inside = here & (rank >= first) & (rank < first + g)
                slot = jnp.where(inside, base + name * g + rank - first, slot)
                first, base = first + g, base + g * half
            picked = picked + jnp.where(slot == slot_ids, 1.0, 0.0)
            share = share + jnp.where(slot == slot_ids, shares[k], 0.0)
        pick_ref[...] = jnp.transpose(picked).astype(jnp.bfloat16)
        high = share.astype(jnp.bfloat16)
        part_ref[:rows] = high
        part_ref[rows:] = (share - high.astype(jnp.float32)).astype(jnp.bfloat16)


def layer_kernel(sp, dp, count, *refs):
    (
        q_hbm, k_hbm, v_hbm, weight_ref, resid_hbm, mixer_hbm, expert_hbm, routes_hbm, shares_hbm,
        gate_hbm, up_hbm, down_hbm, gain_hbm, out_ref,
    ) = refs[:14]
    boxes = refs[14 : 14 + 6 * count]
    sent, served = boxes[:count], boxes[count : 2 * count]
    results, returned = boxes[2 * count : 3 * count], boxes[3 * count : 4 * count]
    lent, lent_back = boxes[4 * count : 5 * count], boxes[5 * count :]
    (
        raw, stream_ref, mixer_ref, expert_ref, gain_ref, routes_ref, shares_ref,
        stage, arrived, out_heads, in_heads, side_heads, flat, full, side_out, side_in, peer_heads, peer_out, peer_in,
        projected, tokens, pick_ref, part_ref, gate_ref, up_ref, down_ref,
        far_routes, far_shares, far_pick, far_part, dense, extra_ref,
        load_sem, q_send, q_recv, a_send, a_recv, pass_send, pass_recv, near_sem, far_send, far_recv,
        twin_send, twin_recv, side_send, side_recv, local_sem,
        send_sem, recv_sem, back_send, back_recv, keep_sem, fetch_sem,
        note_send, note_recv, dense_sem, partial_sem, lend_recv, lend_keep, turn_sem,
        ask_send, ask_recv, peer_send, peer_recv,
    ) = refs[14 + 6 * count :]
    _, rows, heads, width = raw.shape
    local_heads = heads // sp
    depth, columns = weight_ref.shape
    me, mate = lax.axis_index("sp"), lax.axis_index("dp")
    parity, core = lax.rem(me, 2), lax.rem(mate, 2)
    side, twin = me + 1 - 2 * parity, mate + 1 - 2 * core
    ys = dp // 2
    own_y = lax.div(mate, 2)
    n, own = sp * dp, me * dp + mate
    half, plane = n // 2, n // 4
    level = lax.div(own, plane)
    spot = lax.rem(own, plane)
    my_half = lax.div(level, 2)
    near_base, far_base = my_half * half, (1 - my_half) * half
    local = own - near_base
    partner = (3 - level) * plane + spot
    inner = level == 1 + my_half
    outer = level != 1 + my_half

    barrier = pltpu.get_barrier_semaphore()

    def greet(k, carry):
        other = lax.rem(own + k, n)
        pl.semaphore_signal(
            barrier, inc=1, device_id={"sp": lax.div(other, dp), "dp": lax.rem(other, dp)}, device_id_type=MESH
        )
        return carry

    lax.fori_loop(1, n, greet, 0)
    pairs = [
        (q_hbm, raw.at[0]), (k_hbm, raw.at[1]), (v_hbm, raw.at[2]), (routes_hbm, routes_ref),
        (shares_hbm, shares_ref), (weight_ref, full.at[core]), (resid_hbm, stream_ref), (mixer_hbm, mixer_ref),
        (expert_hbm, expert_ref), (gain_hbm, gain_ref),
    ]
    loads = [pltpu.make_async_copy(src, dst, load_sem.at[i]) for i, (src, dst) in enumerate(pairs)]
    for load in loads:
        load.start()
    for t in range(3):
        loads[t].wait()
        stage[t] = jnp.transpose(raw[t], (1, 0, 2))
    pl.semaphore_wait(barrier, n - 1)

    def await_bytes(ref, sem):
        pltpu.make_async_copy(ref, ref, sem).wait()

    def remote(src, dst, send, recv, device):
        return pltpu.make_async_remote_copy(
            src_ref=src, dst_ref=dst, send_sem=send, recv_sem=recv, device_id=device, device_id_type=MESH
        )

    def send_heads(t, h):
        def push(i, carry):
            k = sp // 2 + (1 - 2 * lax.rem(i, 2)) * lax.div(i + 1, 2)
            target = lax.rem(me + k, sp)
            remote(
                stage.at[t, target * local_heads + h], arrived.at[t, h, me], q_send.at[h], q_recv.at[h],
                {"sp": target},
            ).start()
            return carry

        lax.fori_loop(0, sp - 1, push, 0)

    others = pl.ds(0, sp - 1)
    span = depth // 2 // PIECES

    def piece_rows(owner, j):
        return pl.ds(pl.multiple_of(owner * (depth // 2) + j * span, span), span)

    def far(d, owner, j):
        where = piece_rows(owner, j)
        return remote(
            weight_ref.at[where], full.at[1 + d, where], far_send.at[d - 1, owner, j], far_recv.at[d - 1, j],
            {"dp": lax.rem(own_y + d, ys) * 2 + owner},
        )

    def far_in(d, j):
        where = full.at[1 + d, piece_rows(core, j)]
        return remote(where, where, far_send.at[d - 1, 0, j], far_recv.at[d - 1, j], {"dp": twin})

    def to_twin(d, j):
        where = full.at[1 + d, piece_rows(core, j)]
        return remote(where, where, twin_send.at[d - 1, j], twin_recv.at[d - 1, j], {"dp": twin})

    near = remote(weight_ref, full.at[core], near_sem.at[0], near_sem.at[1], {"dp": twin})
    for t in range(3):
        send_heads(t, 0)

    @pl.when(core == parity)
    def _():
        for j in range(PIECES):
            for d in range(1, ys):
                for owner in range(2):
                    far(d, owner, j).start()

    near.start()
    keep_heads = [
        pltpu.make_async_copy(stage.at[t, me * local_heads + h], arrived.at[t, h, me], local_sem.at[t, h])
        for t in range(3)
        for h in range(local_heads)
    ]
    for copy in keep_heads:
        copy.start()
    for h in range(1, local_heads):
        for t in range(3):
            send_heads(t, h)
    fetches = [
        pltpu.make_async_copy(src, dst, fetch_sem.at[i])
        for i, (src, dst) in enumerate(((gate_hbm, gate_ref), (up_hbm, up_ref), (down_hbm, down_ref)))
    ]
    loads[3].wait()
    loads[4].wait()

    def device(target):
        return {"sp": lax.div(target, dp), "dp": lax.rem(target, dp)}

    notes = [
        remote(src, dst, note_send.at[i], note_recv.at[i], device(partner))
        for i, (src, dst) in enumerate(((routes_ref, far_routes), (shares_ref, far_shares)))
    ]
    groups = [box.shape[1] for box in sent]

    @pl.when(inner)
    def _():
        for note in notes:
            note.start()

    place_slots(
        rows, n, groups, [0, 1], routes_ref, shares_ref,
        *[[ref.at[i] for i in range(2)] for ref in (pick_ref, part_ref)],
    )

    part_rows = rows // 2
    block = rows * max(1, min(sp, 256 // rows))
    per = block // rows
    length = sp * rows
    scale = width ** (-0.5)
    tri_row = lax.broadcasted_iota(jnp.int32, (block, block), 0)
    tri_col = lax.broadcasted_iota(jnp.int32, (block, block), 1)
    suffix_ones = (tri_row >= tri_col).astype(jnp.bfloat16)
    is_past = tri_col < tri_row

    def answer(h, target):
        return remote(
            out_heads.at[h, target], in_heads.at[h, me], a_send.at[h], a_recv.at[h, me], {"sp": target}
        )

    def expect(h, source):
        return remote(
            out_heads.at[h, source], in_heads.at[h, source], a_send.at[h], a_recv.at[h, source], {"sp": source}
        )

    def hand_on(h, source):
        remote(
            in_heads.at[h, source, :part_rows], side_heads.at[h, source], pass_send.at[h], pass_recv.at[h],
            {"sp": side},
        ).start()
        for d in range(1, ys):
            remote(
                in_heads.at[h, source, part_rows:], peer_heads.at[d - 1, h, source], ask_send.at[d - 1, h],
                ask_recv.at[d - 1, h], {"dp": lax.rem(own_y + ys - d, ys) * 2 + core},
            ).start()

    ends = length // block
    turns = [ends - 1 - i // 2 if i % 2 == 0 else i // 2 for i in range(ends)]

    def attend_head(h, between):
        def piece(t, index):
            return arrived[t, h, index * per : (index + 1) * per].reshape(block, width)

        for step, q_block in enumerate(turns):
            query = piece(0, q_block)
            total = jnp.zeros((block, width), jnp.float32)
            later = jnp.zeros((block, 1), jnp.float32)
            for k_block in range(q_block, -1, -1):
                scores = (
                    lax.dot_general(
                        query, piece(1, k_block), (((1,), (1,)), ((), ())),
                        preferred_element_type=jnp.float32,
                    )
                    * scale
                )
                soft = jnp.maximum(scores, 0.0) + jnp.log(1.0 + jnp.exp(-jnp.abs(scores)))
                if k_block == q_block:
                    soft = jnp.where(is_past, soft, 0.0)
                high = soft.astype(jnp.bfloat16)
                low = (soft - high.astype(jnp.float32)).astype(jnp.bfloat16)
                suffix = jnp.dot(high, suffix_ones, preferred_element_type=jnp.float32) + jnp.dot(
                    low, suffix_ones, preferred_element_type=jnp.float32
                )
                weights = jnp.exp(scores - suffix - later)
                if k_block == q_block:
                    weights = jnp.where(is_past, weights, 0.0)
                total = total + jnp.dot(
                    weights.astype(jnp.bfloat16), piece(2, k_block), preferred_element_type=jnp.float32
                )
                if k_block > 0:
                    later = later + suffix[:, :1]
            out_heads[h, q_block * per : (q_block + 1) * per] = total.astype(jnp.bfloat16).reshape(
                per, rows, width
            )
            if step:
                send_answers(h, turns[step - 1])
            if step == len(turns) // 2:
                between()
        send_answers(h, turns[-1])
        keep_answer(h).start()

    def send_answers(h, q_block):
        for target in range(q_block * per, (q_block + 1) * per):

            @pl.when(me != target)
            def _():
                answer(h, target).start()

    def keep_answer(h):
        return pltpu.make_async_copy(out_heads.at[h, me], in_heads.at[h, me], local_sem.at[3, h])

    def pass_on(j):
        for d in range(1, ys):
            far_in(d, j).wait_recv()
            to_twin(d, j).start()

    for copy in keep_heads:
        copy.wait()
    def follow_all(h):
        keep_answer(h).wait()
        hand_on(h, me)

        def follow(k, carry):
            for source in (me + k, me - k):

                @pl.when((source >= 0) & (source < sp))
                def _():
                    expect(h, source).wait_recv()
                    hand_on(h, source)

            return carry

        lax.fori_loop(1, sp, follow, 0)

    for h in range(local_heads):
        await_bytes(arrived.at[:, h, others], q_recv.at[h])
        attend_head(h, (lambda: follow_all(h - 1)) if h else (lambda: None))
    for j in range(PIECES - 1):
        pass_on(j)
    follow_all(local_heads - 1)
    pass_on(PIECES - 1)
    for copy in fetches:
        copy.start()

    @pl.when(inner)
    def _():
        for note in notes:
            note.wait()
        place_slots(rows, n, groups, [my_half], far_routes, far_shares, [far_pick], [far_part])

    def fill(ref, first):
        for source in range(sp):
            for h in range(local_heads):
                place = (source * local_heads + h) * width
                block = ref[h, source]
                flat[first : first + block.shape[0], place : place + width] = block

    fill(in_heads, part_rows)
    for h in range(local_heads):
        await_bytes(side_heads.at[h], pass_recv.at[h])
    fill(side_heads, 0)
    for d in range(1, ys):
        for j in range(PIECES):
            to_twin(d, j).wait()

    tile = min(columns, 512)
    many = columns // tile

    def inner_part(i):
        return pl.ds(pl.multiple_of(i * tile, tile), tile)

    def place_of(slice_index, i):
        return pl.ds(pl.multiple_of((slice_index * many + i) * tile, tile), tile)

    def origin(d):
        return lax.rem(own_y + ys - d, ys) * 2

    def hand_back(d, inner):
        return remote(
            side_out.at[d - 1, :, inner], side_in.at[d - 1, :, inner], side_send.at[d - 1], side_recv.at[d - 1],
            {"sp": side},
        )

    def reply(d, inner):
        return remote(
            peer_out.at[d - 1, :, inner], peer_in.at[d - 1, :, inner], peer_send.at[d - 1], peer_recv.at[d - 1],
            {"dp": lax.rem(own_y + d, ys) * 2 + core},
        )

    for d in range(1, ys):

        @pl.loop(0, many)
        def _(i):
            inner = inner_part(i)
            both = jnp.dot(flat[: part_rows + rows], full[1 + d, :, inner], preferred_element_type=jnp.float32)
            projected[:, place_of(origin(d) + parity, i)] = both[part_rows:]
            side_out[d - 1, :, inner] = both[:part_rows].astype(jnp.bfloat16)

            @pl.when(i > 0)
            def _():
                hand_back(d, inner_part(i - 1)).start()

        hand_back(d, pl.ds((many - 1) * tile, tile)).start()

    for d in range(1, ys):
        for h in range(local_heads):
            await_bytes(peer_heads.at[d - 1, h], ask_recv.at[d - 1, h])
        fill(peer_heads.at[d - 1], part_rows + rows + (d - 1) * part_rows)
    loads[5].wait()
    near.wait()

    @pl.loop(0, many)
    def _(i):
        inner = inner_part(i)
        both = jnp.dot(flat[part_rows:], full[1 - parity, :, inner], preferred_element_type=jnp.float32)
        projected[:, place_of(own_y * 2 + 1 - parity, i)] = both[:rows]
        for d in range(1, ys):
            peer_out[d - 1, :, inner] = both[
                rows + (d - 1) * part_rows : rows + d * part_rows
            ].astype(jnp.bfloat16)

        @pl.when(i > 0)
        def _():
            for d in range(1, ys):
                reply(d, inner_part(i - 1)).start()

    for d in range(1, ys):
        reply(d, pl.ds((many - 1) * tile, tile)).start()

    @pl.loop(0, many)
    def _(i):
        projected[:, place_of(own_y * 2 + parity, i)] = jnp.dot(
            flat[part_rows : part_rows + rows], full[parity, :, inner_part(i)], preferred_element_type=jnp.float32
        )

    for load in loads[6:]:
        load.wait()
    for h in range(local_heads):
        await_bytes(stage.at[:, others], q_send.at[h])
        await_bytes(out_heads.at[h, others], a_send.at[h])
        await_bytes(side_heads.at[h], pass_send.at[h])
        for d in range(1, ys):
            await_bytes(peer_heads.at[d - 1, h], ask_send.at[d - 1, h])

    @pl.when(core == parity)
    def _():
        for j in range(PIECES):
            for d in range(1, ys):
                for owner in range(2):
                    far(d, owner, j).wait_send()

    for d in range(1, ys):
        await_bytes(side_in.at[d - 1], side_recv.at[d - 1])
        await_bytes(side_out.at[d - 1], side_send.at[d - 1])
        await_bytes(peer_in.at[d - 1], peer_recv.at[d - 1])
        await_bytes(peer_out.at[d - 1], peer_send.at[d - 1])

        @pl.loop(0, many)
        def _(i):
            outer_part = place_of(origin(d) + 1 - parity, i)
            projected[:part_rows, outer_part] = side_in[d - 1, :, inner_part(i)].astype(jnp.float32)
            projected[part_rows:, outer_part] = peer_in[d - 1, :, inner_part(i)].astype(jnp.float32)

    def lend(i):
        part = pl.ds(pl.multiple_of(i * 16, 16), 16)
        return remote(tokens.at[part], dense.at[part], dense_sem.at[0], dense_sem.at[1], device(partner))

    @pl.loop(0, rows // 16)
    def _(i):
        part = pl.ds(pl.multiple_of(i * 16, 16), 16)
        stream = (
            stream_ref[part].astype(jnp.float32) + normed_token_rows(projected[part], mixer_ref[...])
        ).astype(jnp.bfloat16)
        stream_ref[part] = stream
        tokens[part] = normed_token_rows(stream.astype(jnp.float32), expert_ref[...]).astype(jnp.bfloat16)

        @pl.when(inner & (i > 0))
        def _():
            lend(i - 1).start()

    @pl.when(inner)
    def _():
        lend(rows // 16 - 1).start()

    features = projected.shape[1]
    tile = 512

    def each(number, turn, make, own_place):
        def push(i, carry):
            place = lax.rem(turn + i, number)

            @pl.when(place != own_place)
            def _():
                make(place).start()

            return carry

        lax.fori_loop(0, number, push, 0)

    def outward(a, target):
        return remote(sent[a].at[target], served[a].at[own], send_sem.at[a], recv_sem.at[a], device(target))

    def outward_lent(a, place):
        return remote(
            lent[a].at[place], served[a].at[partner], send_sem.at[a], recv_sem.at[a], device(near_base + place)
        )

    def homeward(a, source):
        return remote(results[a].at[source], returned[a].at[own], back_send.at[a], back_recv.at[a], device(source))

    def homeward_lent(a, place):
        return remote(
            results[a].at[(2 - my_half) * plane + place], lent_back[a].at[local], back_send.at[a], lend_recv.at[a],
            device((1 + my_half) * plane + place),
        )

    def choose(a, pick, source_ref, out, first):
        row = half * sum(groups[:a])
        wanted = pick[row : row + half * groups[a]]

        @pl.loop(0, features // tile)
        def _(i):
            part = pl.ds(pl.multiple_of(i * tile, tile), tile)
            out[a][pl.ds(first, half), :, part] = (
                jnp.dot(wanted, source_ref[:, part], preferred_element_type=jnp.float32)
                .astype(jnp.bfloat16)
                .reshape(half, groups[a], tile)
            )

    own_rows = [pltpu.make_async_copy(sent[a].at[own], served[a].at[own], keep_sem.at[a]) for a in range(count)]
    keeps = [
        pltpu.make_async_copy(results[a].at[own], returned[a].at[own], keep_sem.at[count + a])
        for a in range(count)
    ]
    lent_rows = [
        pltpu.make_async_copy(lent[a].at[local], served[a].at[partner], lend_keep.at[a]) for a in range(count)
    ]
    lent_keeps = [
        pltpu.make_async_copy(results[a].at[partner], lent_back[a].at[local], lend_keep.at[count + a])
        for a in range(count)
    ]
    for a in range(count):
        choose(a, pick_ref.at[my_half], tokens, sent, near_base)
        each(half, local + half // 2, lambda place: outward(a, near_base + place), local)
        own_rows[a].start()

    @pl.when(outer)
    def _():
        for a in range(count):
            choose(a, pick_ref.at[1 - my_half], tokens, sent, far_base)
        pl.semaphore_wait(turn_sem, plane)
        for a in range(count):
            each(half, local + half // 2, lambda place: outward(a, far_base + place), -1)

    @pl.when(inner)
    def _():
        await_bytes(tokens, dense_sem.at[0])

        def release(i, carry):
            pl.semaphore_signal(
                turn_sem, inc=1, device_id=device(3 * my_half * plane + i), device_id_type=MESH
            )
            return carry

        lax.fori_loop(0, plane, release, 0)
        await_bytes(dense, dense_sem.at[1])
        for a in range(count):
            choose(a, far_pick, dense, lent, 0)
            each(half, local + half // 2, lambda place: outward_lent(a, place), local)
            lent_rows[a].start()

    def await_blocks(boxes, sems, a):
        @pl.when(inner)
        def _():
            await_bytes(boxes[a].at[pl.ds(0, n - 2)], sems.at[a])

        @pl.when(outer)
        def _():
            await_bytes(boxes[a].at[pl.ds(0, n - 1)], sems.at[a])

    def give_lent(a):
        each(plane, spot + plane // 2, lambda place: homeward_lent(a, place), jnp.where(inner, spot, -1))

        @pl.when(inner)
        def _():
            lent_keeps[a].start()

    def give_far(a):
        each(plane, spot + plane // 2, lambda place: homeward(a, 3 * (1 - my_half) * plane + place), -1)

    def give_near(a):
        each(half, local + half // 2, lambda place: homeward(a, near_base + place), local)
        keeps[a].start()

    for a in range(count):
        own_rows[a].wait()

        @pl.when(inner)
        def _():
            lent_rows[a].wait()

        await_blocks(served, recv_sem, a)
        if a == 0:
            for copy in fetches:
                copy.wait()
        many = served[a].shape[1]
        taken = served[a][...].reshape(n * many, features)
        gate = jnp.dot(taken, gate_ref[...], preferred_element_type=jnp.float32)
        upward = jnp.dot(taken, up_ref[...], preferred_element_type=jnp.float32)
        hidden = (gate / (1.0 + jnp.exp(-gate)) * upward).astype(jnp.bfloat16)
        for i in range(features // tile):
            part = slice(i * tile, (i + 1) * tile)
            results[a][:, :, part] = (
                jnp.dot(hidden, down_ref[:, part], preferred_element_type=jnp.float32)
                .astype(jnp.bfloat16)
                .reshape(n, many, tile)
            )
        give_lent(a)

        @pl.when(inner)
        def _():
            give_far(a)

    for a in range(count):

        @pl.when(outer)
        def _():
            give_far(a)

        give_near(a)

    def gather(box, first, parts, a, part):
        columns_of = slice(half * sum(groups[:a]), half * sum(groups[: a + 1]))
        block = box[a][pl.ds(first, half), :, part].reshape(half * groups[a], tile)
        both = jnp.dot(parts[:, columns_of], block, preferred_element_type=jnp.float32)
        return both[:rows] + both[rows:]

    pieces = [slice(0, part_rows), slice(part_rows, rows)]

    def settle_up(r, i):
        part = pl.ds(pl.multiple_of(i * tile, tile), tile)
        return remote(
            dense.at[pieces[r], part], extra_ref.at[pieces[r], part], partial_sem.at[0], partial_sem.at[1 + r],
            device(partner),
        )

    @pl.when(inner)
    def _():
        for a in range(count):
            lent_keeps[a].wait()
            await_bytes(lent_back[a].at[pl.ds(0, half - 1)], lend_recv.at[a])

        @pl.loop(0, features // tile)
        def _(i):
            part = pl.ds(pl.multiple_of(i * tile, tile), tile)
            dense[:, part] = sum(
                gather(lent_back, 0, far_part, a, part) for a in range(count)
            ).astype(jnp.bfloat16)

            @pl.when(i > 0)
            def _():
                settle_up(0, i - 1).start()

        settle_up(0, features // tile - 1).start()

        @pl.loop(0, features // tile)
        def _(i):
            settle_up(1, i).start()

    for a in range(count):
        keeps[a].wait()

        @pl.when(inner)
        def _():
            await_bytes(returned[a].at[pl.ds(0, half - 1)], back_recv.at[a])

        @pl.when(outer)
        def _():
            await_bytes(returned[a].at[pl.ds(0, n - 1)], back_recv.at[a])

        def add_up(bases):
            @pl.loop(0, features // tile)
            def _(i):
                part = pl.ds(pl.multiple_of(i * tile, tile), tile)
                total = sum(gather(returned, first, part_ref.at[which], a, part) for first, which in bases)
                projected[:, part] = total if a == 0 else projected[:, part] + total

        @pl.when(inner)
        def _():
            add_up([(near_base, my_half)])

        @pl.when(outer)
        def _():
            add_up([(near_base, my_half), (far_base, 1 - my_half)])

    for a in range(count):
        await_blocks(sent, send_sem, a)
        await_blocks(results, back_send, a)

    def finish(combined, piece):
        @pl.loop(piece.start // 16, piece.stop // 16)
        def _(i):
            part = pl.ds(pl.multiple_of(i * 16, 16), 16)
            out_ref[part] = (
                stream_ref[part].astype(jnp.float32) + normed_token_rows(combined(part), gain_ref[...])
            ).astype(jnp.bfloat16)

    @pl.when(inner)
    def _():
        for r in range(2):
            await_bytes(extra_ref.at[pieces[r]], partial_sem.at[1 + r])
            finish(lambda part: projected[part] + extra_ref[part].astype(jnp.float32), pieces[r])
        await_bytes(dense, partial_sem.at[0])

    @pl.when(outer)
    def _():
        finish(lambda part: projected[part], slice(0, rows))


def layer(
    query, key, value, weight, residual, mixer_gain, expert_gain, routes, shares, gate, up, down, gain, groups
):
    sp, dp = lax.axis_size("sp"), lax.axis_size("dp")
    n = sp * dp
    rows, heads, width = query.shape
    depth, columns = weight.shape
    features = residual.shape[1]
    local_heads = heads // sp
    extra = max(dp // 2 - 1, 1)
    slots = n // 2 * sum(groups)
    anywhere = pl.BlockSpec(memory_space=pl.ANY)
    dma = pltpu.SemaphoreType.DMA
    bf16, f32 = jnp.bfloat16, jnp.float32
    return pl.pallas_call(
        functools.partial(layer_kernel, sp, dp, len(groups)),
        out_shape=pltpu.VMEM((rows, features), bf16),
        in_specs=[anywhere] * 13,
        out_specs=pl.BlockSpec(memory_space=pltpu.VMEM),
        scratch_shapes=[pltpu.VMEM((n, g, features), bf16) for _ in range(4) for g in groups]
        + [pltpu.VMEM((n // 2, g, features), bf16) for _ in range(2) for g in groups]
        + [
            pltpu.VMEM((3, rows, heads, width), bf16),
            pltpu.VMEM((rows, features), bf16),
            pltpu.VMEM((1, features), f32),
            pltpu.VMEM((1, features), f32),
            pltpu.VMEM((1, features), f32),
            pltpu.VMEM(routes.shape, jnp.int32),
            pltpu.VMEM(shares.shape, f32),
            pltpu.VMEM((3, heads, rows, width), bf16),
            pltpu.VMEM((3, local_heads, sp, rows, width), bf16),
            pltpu.VMEM((local_heads, sp, rows, width), bf16),
            pltpu.VMEM((local_heads, sp, rows, width), bf16),
            pltpu.VMEM((local_heads, sp, rows // 2, width), bf16),
            pltpu.VMEM(((3 + extra) * (rows // 2), depth), bf16),
            pltpu.VMEM((2 + extra, depth, columns), bf16),
            pltpu.VMEM((extra, rows // 2, columns), bf16),
            pltpu.VMEM((extra, rows // 2, columns), bf16),
            pltpu.VMEM((extra, local_heads, sp, rows // 2, width), bf16),
            pltpu.VMEM((extra, rows // 2, columns), bf16),
            pltpu.VMEM((extra, rows // 2, columns), bf16),
            pltpu.VMEM((rows, features), f32),
            pltpu.VMEM((rows, features), bf16),
            pltpu.VMEM((2, slots, rows), bf16),
            pltpu.VMEM((2, 2 * rows, slots), bf16),
            pltpu.VMEM(gate.shape, bf16),
            pltpu.VMEM(up.shape, bf16),
            pltpu.VMEM(down.shape, bf16),
            pltpu.VMEM(routes.shape, jnp.int32),
            pltpu.VMEM(shares.shape, f32),
            pltpu.VMEM((slots, rows), bf16),
            pltpu.VMEM((2 * rows, slots), bf16),
            pltpu.VMEM((rows, features), bf16),
            pltpu.VMEM((rows, features), bf16),
            dma((10,)),
            dma((local_heads,)),
            dma((local_heads,)),
            dma((local_heads,)),
            dma((local_heads, sp)),
            dma((local_heads,)),
            dma((local_heads,)),
            dma((2,)),
            dma((extra, 2, PIECES)),
            dma((extra, PIECES)),
            dma((extra, PIECES)),
            dma((extra, PIECES)),
            dma((extra,)),
            dma((extra,)),
            dma((4, local_heads)),
            dma((len(groups),)),
            dma((len(groups),)),
            dma((len(groups),)),
            dma((len(groups),)),
            dma((2 * len(groups),)),
            dma((3,)),
            dma((2,)),
            dma((2,)),
            dma((2,)),
            dma((3,)),
            dma((len(groups),)),
            dma((2 * len(groups),)),
            pltpu.SemaphoreType.REGULAR,
            dma((extra, local_heads)),
            dma((extra, local_heads)),
            dma((extra,)),
            dma((extra,)),
        ],
        compiler_params=pltpu.CompilerParams(
            collective_id=0, has_side_effects=True, vmem_limit_bytes=VMEM_LIMIT
        ),
    )(
        query, key, value, weight, residual, mixer_gain[None], expert_gain[None], routes, shares,
        gate, up, down, gain[None],
    )


def local(
    queries,
    key_rows,
    values,
    residual,
    out_weight,
    mixer_gain,
    expert_gain,
    gate_weight,
    up_weight,
    expert_down_matrix,
    routes,
    route_weight,
    output_gain,
):
    local_rows = queries.shape[1]
    experts = lax.axis_size("sp") * lax.axis_size("dp")
    capacity = max(2, 3 * local_rows // experts)
    groups = [g for g in (capacity // 8 * 8, capacity % 8) if g]
    output = layer(
        queries[0], key_rows[0], values[0], out_weight, residual[0], mixer_gain, expert_gain,
        routes[0].T, route_weight[0].T, gate_weight[0], up_weight[0], expert_down_matrix[0], output_gain, groups,
    )
    return output[None]


def solution(mesh):
    in_specs = (
        P("dp", "sp", None, None),
        P("dp", "sp", None, None),
        P("dp", "sp", None, None),
        P("dp", "sp", None),
        P(None, "dp"),
        P(),
        P(),
        P(("sp", "dp"), None, None),
        P(("sp", "dp"), None, None),
        P(("sp", "dp"), None, None),
        P("dp", "sp", None),
        P("dp", "sp", None),
        P(),
    )
    out_specs = P("dp", "sp", None)
    return jax.shard_map(local, mesh=mesh, in_specs=in_specs, out_specs=out_specs, check_vma=False)
```

```python
import functools

import jax
import jax.numpy as jnp
from jax import lax
from jax.experimental import pallas as pl
from jax.experimental.pallas import tpu as pltpu
from jax.sharding import PartitionSpec as P

EPSILON = 1e-06
MESH = pl.DeviceIdType.MESH
VMEM_LIMIT = 62 * 1024 * 1024


def normed_token_rows(matrix, gain):
    return matrix * lax.rsqrt(jnp.mean(matrix * matrix, axis=-1, keepdims=True) + EPSILON) * gain


PIECES = 2


def place_slots(rows, experts, groups, halves, routes_ref, shares_ref, pick_refs, part_refs):
    top_count = routes_ref.shape[0]
    half = experts // 2

    def column(row):
        return jnp.transpose(jnp.broadcast_to(row, (rows, rows)))[:, :1]

    lanes = lax.broadcasted_iota(jnp.int32, (rows, max(experts, 128)), 1).astype(jnp.float32)
    names = [column(routes_ref[k : k + 1].astype(jnp.float32)) for k in range(top_count)]
    shares = [column(shares_ref[k : k + 1]) for k in range(top_count)]
    marks = [jnp.where(name == lanes, 1.0, 0.0) for name in names]
    earlier = lax.broadcasted_iota(jnp.int32, (rows, rows), 1) < lax.broadcasted_iota(jnp.int32, (rows, rows), 0)
    before = jnp.dot(
        jnp.where(earlier, 1.0, 0.0).astype(jnp.bfloat16),
        sum(marks).astype(jnp.bfloat16),
        preferred_element_type=jnp.float32,
    )
    ranks = [jnp.sum(before * mark, axis=1, keepdims=True) for mark in marks]
    slot_ids = lax.broadcasted_iota(jnp.int32, (rows, half * sum(groups)), 1).astype(jnp.float32)
    for which, pick_ref, part_ref in zip(halves, pick_refs, part_refs):
        start = jnp.asarray(which * half, jnp.int32).astype(jnp.float32)
        picked, share = 0.0, 0.0
        for k in range(top_count):
            name, rank = names[k] - start, ranks[k]
            here = (name >= 0.0) & (name < half)
            slot, first, base = jnp.full((rows, 1), -1.0, jnp.float32), 0, 0
            for g in groups:
                inside = here & (rank >= first) & (rank < first + g)
                slot = jnp.where(inside, base + name * g + rank - first, slot)
                first, base = first + g, base + g * half
            picked = picked + jnp.where(slot == slot_ids, 1.0, 0.0)
            share = share + jnp.where(slot == slot_ids, shares[k], 0.0)
        pick_ref[...] = jnp.transpose(picked).astype(jnp.bfloat16)
        high = share.astype(jnp.bfloat16)
        part_ref[:rows] = high
        part_ref[rows:] = (share - high.astype(jnp.float32)).astype(jnp.bfloat16)


def layer_kernel(sp, dp, count, *refs):
    (
        q_hbm, k_hbm, v_hbm, weight_ref, resid_hbm, mixer_hbm, expert_hbm, routes_hbm, shares_hbm,
        gate_hbm, up_hbm, down_hbm, gain_hbm, out_ref,
    ) = refs[:14]
    boxes = refs[14 : 14 + 6 * count]
    sent, served = boxes[:count], boxes[count : 2 * count]
    results, returned = boxes[2 * count : 3 * count], boxes[3 * count : 4 * count]
    lent, lent_back = boxes[4 * count : 5 * count], boxes[5 * count :]
    (
        raw, stream_ref, mixer_ref, expert_ref, gain_ref, routes_ref, shares_ref,
        stage, arrived, out_heads, in_heads, side_heads, flat, full, side_out, side_in, peer_heads, peer_out, peer_in,
        projected, tokens, pick_ref, part_ref, gate_ref, up_ref, down_ref,
        far_routes, far_shares, far_pick, far_part, dense, extra_ref,
        load_sem, q_send, q_recv, a_send, a_recv, pass_send, pass_recv, near_sem, far_send, far_recv,
        twin_send, twin_recv, side_send, side_recv, local_sem,
        send_sem, recv_sem, back_send, back_recv, keep_sem, fetch_sem,
        note_send, note_recv, dense_sem, partial_sem, lend_recv, lend_keep, turn_sem,
        ask_send, ask_recv, peer_send, peer_recv,
    ) = refs[14 + 6 * count :]
    _, rows, heads, width = raw.shape
    local_heads = heads // sp
    depth, columns = weight_ref.shape
    me, mate = lax.axis_index("sp"), lax.axis_index("dp")
    parity, core = lax.rem(me, 2), lax.rem(mate, 2)
    side, twin = me + 1 - 2 * parity, mate + 1 - 2 * core
    ys = dp // 2
    own_y = lax.div(mate, 2)
    n, own = sp * dp, me * dp + mate
    half, plane = n // 2, n // 4
    level = lax.div(own, plane)
    spot = lax.rem(own, plane)
    my_half = lax.div(level, 2)
    near_base, far_base = my_half * half, (1 - my_half) * half
    local = own - near_base
    partner = (3 - level) * plane + spot
    inner = level == 1 + my_half
    outer = level != 1 + my_half

    barrier = pltpu.get_barrier_semaphore()

    def greet(k, carry):
        other = lax.rem(own + k, n)
        pl.semaphore_signal(
            barrier, inc=1, device_id={"sp": lax.div(other, dp), "dp": lax.rem(other, dp)}, device_id_type=MESH
        )
        return carry

    lax.fori_loop(1, n, greet, 0)
    pairs = [
        (q_hbm, raw.at[0]), (k_hbm, raw.at[1]), (v_hbm, raw.at[2]), (routes_hbm, routes_ref),
        (shares_hbm, shares_ref), (weight_ref, full.at[core]), (resid_hbm, stream_ref), (mixer_hbm, mixer_ref),
        (expert_hbm, expert_ref), (gain_hbm, gain_ref),
    ]
    loads = [pltpu.make_async_copy(src, dst, load_sem.at[i]) for i, (src, dst) in enumerate(pairs)]
    for load in loads:
        load.start()
    for t in range(3):
        loads[t].wait()
        stage[t] = jnp.transpose(raw[t], (1, 0, 2))
    pl.semaphore_wait(barrier, n - 1)

    def await_bytes(ref, sem):
        pltpu.make_async_copy(ref, ref, sem).wait()

    def remote(src, dst, send, recv, device):
        return pltpu.make_async_remote_copy(
            src_ref=src, dst_ref=dst, send_sem=send, recv_sem=recv, device_id=device, device_id_type=MESH
        )

    def send_heads(t, h):
        def push(i, carry):
            k = sp // 2 + (1 - 2 * lax.rem(i, 2)) * lax.div(i + 1, 2)
            target = lax.rem(me + k, sp)
            remote(
                stage.at[t, target * local_heads + h], arrived.at[t, h, me], q_send.at[h], q_recv.at[h],
                {"sp": target},
            ).start()
            return carry

        lax.fori_loop(0, sp - 1, push, 0)

    others = pl.ds(0, sp - 1)
    span = depth // 2 // PIECES

    def piece_rows(owner, j):
        return pl.ds(pl.multiple_of(owner * (depth // 2) + j * span, span), span)

    def far(d, owner, j):
        where = piece_rows(owner, j)
        return remote(
            weight_ref.at[where], full.at[1 + d, where], far_send.at[d - 1, owner, j], far_recv.at[d - 1, j],
            {"dp": lax.rem(own_y + d, ys) * 2 + owner},
        )

    def far_in(d, j):
        where = full.at[1 + d, piece_rows(core, j)]
        return remote(where, where, far_send.at[d - 1, 0, j], far_recv.at[d - 1, j], {"dp": twin})

    def to_twin(d, j):
        where = full.at[1 + d, piece_rows(core, j)]
        return remote(where, where, twin_send.at[d - 1, j], twin_recv.at[d - 1, j], {"dp": twin})

    near = remote(weight_ref, full.at[core], near_sem.at[0], near_sem.at[1], {"dp": twin})
    for t in range(3):
        send_heads(t, 0)

    @pl.when(core == parity)
    def _():
        for j in range(PIECES):
            for d in range(1, ys):
                for owner in range(2):
                    far(d, owner, j).start()

    near.start()
    keep_heads = [
        pltpu.make_async_copy(stage.at[t, me * local_heads + h], arrived.at[t, h, me], local_sem.at[t, h])
        for t in range(3)
        for h in range(local_heads)
    ]
    for copy in keep_heads:
        copy.start()
    for h in range(1, local_heads):
        for t in range(3):
            send_heads(t, h)
    fetches = [
        pltpu.make_async_copy(src, dst, fetch_sem.at[i])
        for i, (src, dst) in enumerate(((gate_hbm, gate_ref), (up_hbm, up_ref), (down_hbm, down_ref)))
    ]
    loads[3].wait()
    loads[4].wait()

    def device(target):
        return {"sp": lax.div(target, dp), "dp": lax.rem(target, dp)}

    notes = [
        remote(src, dst, note_send.at[i], note_recv.at[i], device(partner))
        for i, (src, dst) in enumerate(((routes_ref, far_routes), (shares_ref, far_shares)))
    ]
    groups = [box.shape[1] for box in sent]

    @pl.when(inner)
    def _():
        for note in notes:
            note.start()

    place_slots(
        rows, n, groups, [0, 1], routes_ref, shares_ref,
        *[[ref.at[i] for i in range(2)] for ref in (pick_ref, part_ref)],
    )

    part_rows = rows // 2
    block = rows * max(1, min(sp, 256 // rows))
    per = block // rows
    length = sp * rows
    scale = width ** (-0.5)
    tri_row = lax.broadcasted_iota(jnp.int32, (block, block), 0)
    tri_col = lax.broadcasted_iota(jnp.int32, (block, block), 1)
    suffix_ones = (tri_row >= tri_col).astype(jnp.bfloat16)
    is_past = tri_col < tri_row

    def answer(h, target):
        return remote(
            out_heads.at[h, target], in_heads.at[h, me], a_send.at[h], a_recv.at[h, me], {"sp": target}
        )

    def expect(h, source):
        return remote(
            out_heads.at[h, source], in_heads.at[h, source], a_send.at[h], a_recv.at[h, source], {"sp": source}
        )

    def hand_on(h, source):
        remote(
            in_heads.at[h, source, :part_rows], side_heads.at[h, source], pass_send.at[h], pass_recv.at[h],
            {"sp": side},
        ).start()
        for d in range(1, ys):
            remote(
                in_heads.at[h, source, part_rows:], peer_heads.at[d - 1, h, source], ask_send.at[d - 1, h],
                ask_recv.at[d - 1, h], {"dp": lax.rem(own_y + ys - d, ys) * 2 + core},
            ).start()

    ends = length // block
    turns = [ends - 1 - i // 2 if i % 2 == 0 else i // 2 for i in range(ends)]

    def attend_head(h, between):
        def piece(t, index):
            return arrived[t, h, index * per : (index + 1) * per].reshape(block, width)

        for step, q_block in enumerate(turns):
            query = piece(0, q_block)
            total = jnp.zeros((block, width), jnp.float32)
            later = jnp.zeros((block, 1), jnp.float32)
            for k_block in range(q_block, -1, -1):
                scores = (
                    lax.dot_general(
                        query, piece(1, k_block), (((1,), (1,)), ((), ())),
                        preferred_element_type=jnp.float32,
                    )
                    * scale
                )
                soft = jnp.maximum(scores, 0.0) + jnp.log(1.0 + jnp.exp(-jnp.abs(scores)))
                if k_block == q_block:
                    soft = jnp.where(is_past, soft, 0.0)
                high = soft.astype(jnp.bfloat16)
                low = (soft - high.astype(jnp.float32)).astype(jnp.bfloat16)
                suffix = jnp.dot(high, suffix_ones, preferred_element_type=jnp.float32) + jnp.dot(
                    low, suffix_ones, preferred_element_type=jnp.float32
                )
                weights = jnp.exp(scores - suffix - later)
                if k_block == q_block:
                    weights = jnp.where(is_past, weights, 0.0)
                total = total + jnp.dot(
                    weights.astype(jnp.bfloat16), piece(2, k_block), preferred_element_type=jnp.float32
                )
                if k_block > 0:
                    later = later + suffix[:, :1]
            out_heads[h, q_block * per : (q_block + 1) * per] = total.astype(jnp.bfloat16).reshape(
                per, rows, width
            )
            if step:
                send_answers(h, turns[step - 1])
            if step == len(turns) // 2:
                between()
        send_answers(h, turns[-1])
        keep_answer(h).start()

    def send_answers(h, q_block):
        for target in range(q_block * per, (q_block + 1) * per):

            @pl.when(me != target)
            def _():
                answer(h, target).start()

    def keep_answer(h):
        return pltpu.make_async_copy(out_heads.at[h, me], in_heads.at[h, me], local_sem.at[3, h])

    def pass_on(j):
        for d in range(1, ys):
            far_in(d, j).wait_recv()
            to_twin(d, j).start()

    for copy in keep_heads:
        copy.wait()
    def follow_all(h):
        keep_answer(h).wait()
        hand_on(h, me)

        def follow(k, carry):
            for source in (me + k, me - k):

                @pl.when((source >= 0) & (source < sp))
                def _():
                    expect(h, source).wait_recv()
                    hand_on(h, source)

            return carry

        lax.fori_loop(1, sp, follow, 0)

    for h in range(local_heads):
        await_bytes(arrived.at[:, h, others], q_recv.at[h])
        attend_head(h, (lambda: follow_all(h - 1)) if h else (lambda: None))
    for j in range(PIECES - 1):
        pass_on(j)
    follow_all(local_heads - 1)
    pass_on(PIECES - 1)
    @pl.when(inner)
    def _():
        for note in notes:
            note.wait()
        place_slots(rows, n, groups, [my_half], far_routes, far_shares, [far_pick], [far_part])

    def fill(ref, first):
        for source in range(sp):
            for h in range(local_heads):
                place = (source * local_heads + h) * width
                block = ref[h, source]
                flat[first : first + block.shape[0], place : place + width] = block

    fill(in_heads, part_rows)
    for h in range(local_heads):
        await_bytes(side_heads.at[h], pass_recv.at[h])
    fill(side_heads, 0)
    for d in range(1, ys):
        for j in range(PIECES):
            to_twin(d, j).wait()

    tile = min(columns, 512)
    many = columns // tile

    def inner_part(i):
        return pl.ds(pl.multiple_of(i * tile, tile), tile)

    def place_of(slice_index, i):
        return pl.ds(pl.multiple_of((slice_index * many + i) * tile, tile), tile)

    def origin(d):
        return lax.rem(own_y + ys - d, ys) * 2

    def hand_back(d, inner):
        return remote(
            side_out.at[d - 1, :, inner], side_in.at[d - 1, :, inner], side_send.at[d - 1], side_recv.at[d - 1],
            {"sp": side},
        )

    def reply(d, inner):
        return remote(
            peer_out.at[d - 1, :, inner], peer_in.at[d - 1, :, inner], peer_send.at[d - 1], peer_recv.at[d - 1],
            {"dp": lax.rem(own_y + d, ys) * 2 + core},
        )

    for d in range(1, ys):

        @pl.loop(0, many)
        def _(i):
            inner = inner_part(i)
            both = jnp.dot(flat[: part_rows + rows], full[1 + d, :, inner], preferred_element_type=jnp.float32)
            projected[:, place_of(origin(d) + parity, i)] = both[part_rows:]
            side_out[d - 1, :, inner] = both[:part_rows].astype(jnp.bfloat16)

            @pl.when(i > 0)
            def _():
                hand_back(d, inner_part(i - 1)).start()

        hand_back(d, pl.ds((many - 1) * tile, tile)).start()

    for d in range(1, ys):
        for h in range(local_heads):
            await_bytes(peer_heads.at[d - 1, h], ask_recv.at[d - 1, h])
        fill(peer_heads.at[d - 1], part_rows + rows + (d - 1) * part_rows)
    loads[5].wait()
    near.wait()

    @pl.loop(0, many)
    def _(i):
        inner = inner_part(i)
        both = jnp.dot(flat[part_rows:], full[1 - parity, :, inner], preferred_element_type=jnp.float32)
        projected[:, place_of(own_y * 2 + 1 - parity, i)] = both[:rows]
        for d in range(1, ys):
            peer_out[d - 1, :, inner] = both[
                rows + (d - 1) * part_rows : rows + d * part_rows
            ].astype(jnp.bfloat16)

        @pl.when(i > 0)
        def _():
            for d in range(1, ys):
                reply(d, inner_part(i - 1)).start()

    for d in range(1, ys):
        reply(d, pl.ds((many - 1) * tile, tile)).start()

    @pl.loop(0, many)
    def _(i):
        projected[:, place_of(own_y * 2 + parity, i)] = jnp.dot(
            flat[part_rows : part_rows + rows], full[parity, :, inner_part(i)], preferred_element_type=jnp.float32
        )

    for load in loads[6:]:
        load.wait()
    for h in range(local_heads):
        await_bytes(stage.at[:, others], q_send.at[h])
        await_bytes(out_heads.at[h, others], a_send.at[h])
        await_bytes(side_heads.at[h], pass_send.at[h])
        for d in range(1, ys):
            await_bytes(peer_heads.at[d - 1, h], ask_send.at[d - 1, h])

    @pl.when(core == parity)
    def _():
        for j in range(PIECES):
            for d in range(1, ys):
                for owner in range(2):
                    far(d, owner, j).wait_send()

    for d in range(1, ys):
        await_bytes(side_in.at[d - 1], side_recv.at[d - 1])
        await_bytes(side_out.at[d - 1], side_send.at[d - 1])
        await_bytes(peer_in.at[d - 1], peer_recv.at[d - 1])
        await_bytes(peer_out.at[d - 1], peer_send.at[d - 1])

        @pl.loop(0, many)
        def _(i):
            outer_part = place_of(origin(d) + 1 - parity, i)
            projected[:part_rows, outer_part] = side_in[d - 1, :, inner_part(i)].astype(jnp.float32)
            projected[part_rows:, outer_part] = peer_in[d - 1, :, inner_part(i)].astype(jnp.float32)

    def lend(i):
        part = pl.ds(pl.multiple_of(i * 16, 16), 16)
        return remote(tokens.at[part], dense.at[part], dense_sem.at[0], dense_sem.at[1], device(partner))

    @pl.loop(0, rows // 16)
    def _(i):
        part = pl.ds(pl.multiple_of(i * 16, 16), 16)
        stream = (
            stream_ref[part].astype(jnp.float32) + normed_token_rows(projected[part], mixer_ref[...])
        ).astype(jnp.bfloat16)
        stream_ref[part] = stream
        tokens[part] = normed_token_rows(stream.astype(jnp.float32), expert_ref[...]).astype(jnp.bfloat16)

        @pl.when(inner & (i > 0))
        def _():
            lend(i - 1).start()

    @pl.when(inner)
    def _():
        lend(rows // 16 - 1).start()

    for copy in fetches:
        copy.start()
    features = projected.shape[1]
    tile = 512

    def each(number, turn, make, own_place):
        def push(i, carry):
            place = lax.rem(turn + i, number)

            @pl.when(place != own_place)
            def _():
                make(place).start()

            return carry

        lax.fori_loop(0, number, push, 0)

    def outward(a, target):
        return remote(sent[a].at[target], served[a].at[own], send_sem.at[a], recv_sem.at[a], device(target))

    def outward_lent(a, place):
        return remote(
            lent[a].at[place], served[a].at[partner], send_sem.at[a], recv_sem.at[a], device(near_base + place)
        )

    def homeward(a, source):
        return remote(results[a].at[source], returned[a].at[own], back_send.at[a], back_recv.at[a], device(source))

    def homeward_lent(a, place):
        return remote(
            results[a].at[(2 - my_half) * plane + place], lent_back[a].at[local], back_send.at[a], lend_recv.at[a],
            device((1 + my_half) * plane + place),
        )

    def choose(a, pick, source_ref, out, first):
        row = half * sum(groups[:a])
        wanted = pick[row : row + half * groups[a]]

        @pl.loop(0, features // tile)
        def _(i):
            part = pl.ds(pl.multiple_of(i * tile, tile), tile)
            out[a][pl.ds(first, half), :, part] = (
                jnp.dot(wanted, source_ref[:, part], preferred_element_type=jnp.float32)
                .astype(jnp.bfloat16)
                .reshape(half, groups[a], tile)
            )

    own_rows = [pltpu.make_async_copy(sent[a].at[own], served[a].at[own], keep_sem.at[a]) for a in range(count)]
    keeps = [
        pltpu.make_async_copy(results[a].at[own], returned[a].at[own], keep_sem.at[count + a])
        for a in range(count)
    ]
    lent_rows = [
        pltpu.make_async_copy(lent[a].at[local], served[a].at[partner], lend_keep.at[a]) for a in range(count)
    ]
    lent_keeps = [
        pltpu.make_async_copy(results[a].at[partner], lent_back[a].at[local], lend_keep.at[count + a])
        for a in range(count)
    ]
    for a in range(count):
        choose(a, pick_ref.at[my_half], tokens, sent, near_base)
        each(half, local + half // 2, lambda place: outward(a, near_base + place), local)
        own_rows[a].start()

    @pl.when(outer)
    def _():
        for a in range(count):
            choose(a, pick_ref.at[1 - my_half], tokens, sent, far_base)
        pl.semaphore_wait(turn_sem, plane)
        for a in range(count):
            each(half, local + half // 2, lambda place: outward(a, far_base + place), -1)

    @pl.when(inner)
    def _():
        await_bytes(tokens, dense_sem.at[0])

        def release(i, carry):
            pl.semaphore_signal(
                turn_sem, inc=1, device_id=device(3 * my_half * plane + i), device_id_type=MESH
            )
            return carry

        lax.fori_loop(0, plane, release, 0)
        await_bytes(dense, dense_sem.at[1])
        for a in range(count):
            choose(a, far_pick, dense, lent, 0)
            each(half, local + half // 2, lambda place: outward_lent(a, place), local)
            lent_rows[a].start()

    def await_blocks(boxes, sems, a):
        @pl.when(inner)
        def _():
            await_bytes(boxes[a].at[pl.ds(0, n - 2)], sems.at[a])

        @pl.when(outer)
        def _():
            await_bytes(boxes[a].at[pl.ds(0, n - 1)], sems.at[a])

    def give_lent(a):
        each(plane, spot + plane // 2, lambda place: homeward_lent(a, place), jnp.where(inner, spot, -1))

        @pl.when(inner)
        def _():
            lent_keeps[a].start()

    def give_far(a):
        each(plane, spot + plane // 2, lambda place: homeward(a, 3 * (1 - my_half) * plane + place), -1)

    def give_near(a):
        each(half, local + half // 2, lambda place: homeward(a, near_base + place), local)
        keeps[a].start()

    for a in range(count):
        own_rows[a].wait()

        @pl.when(inner)
        def _():
            lent_rows[a].wait()

        await_blocks(served, recv_sem, a)
        if a == 0:
            for copy in fetches:
                copy.wait()
        many = served[a].shape[1]
        taken = served[a][...].reshape(n * many, features)
        gate = jnp.dot(taken, gate_ref[...], preferred_element_type=jnp.float32)
        upward = jnp.dot(taken, up_ref[...], preferred_element_type=jnp.float32)
        hidden = (gate / (1.0 + jnp.exp(-gate)) * upward).astype(jnp.bfloat16)
        for i in range(features // tile):
            part = slice(i * tile, (i + 1) * tile)
            results[a][:, :, part] = (
                jnp.dot(hidden, down_ref[:, part], preferred_element_type=jnp.float32)
                .astype(jnp.bfloat16)
                .reshape(n, many, tile)
            )
        give_lent(a)

        @pl.when(inner)
        def _():
            give_far(a)

    for a in range(count):

        @pl.when(outer)
        def _():
            give_far(a)

        give_near(a)

    def gather(box, first, parts, a, part):
        columns_of = slice(half * sum(groups[:a]), half * sum(groups[: a + 1]))
        block = box[a][pl.ds(first, half), :, part].reshape(half * groups[a], tile)
        both = jnp.dot(parts[:, columns_of], block, preferred_element_type=jnp.float32)
        return both[:rows] + both[rows:]

    pieces = [slice(0, part_rows), slice(part_rows, rows)]

    def settle_up(r, i):
        part = pl.ds(pl.multiple_of(i * tile, tile), tile)
        return remote(
            dense.at[pieces[r], part], extra_ref.at[pieces[r], part], partial_sem.at[0], partial_sem.at[1 + r],
            device(partner),
        )

    @pl.when(inner)
    def _():
        for a in range(count):
            lent_keeps[a].wait()
            await_bytes(lent_back[a].at[pl.ds(0, half - 1)], lend_recv.at[a])

        @pl.loop(0, features // tile)
        def _(i):
            part = pl.ds(pl.multiple_of(i * tile, tile), tile)
            dense[:, part] = sum(
                gather(lent_back, 0, far_part, a, part) for a in range(count)
            ).astype(jnp.bfloat16)

            @pl.when(i > 0)
            def _():
                settle_up(0, i - 1).start()

        settle_up(0, features // tile - 1).start()

        @pl.loop(0, features // tile)
        def _(i):
            settle_up(1, i).start()

    for a in range(count):
        keeps[a].wait()

        @pl.when(inner)
        def _():
            await_bytes(returned[a].at[pl.ds(0, half - 1)], back_recv.at[a])

        @pl.when(outer)
        def _():
            await_bytes(returned[a].at[pl.ds(0, n - 1)], back_recv.at[a])

        def add_up(bases):
            @pl.loop(0, features // tile)
            def _(i):
                part = pl.ds(pl.multiple_of(i * tile, tile), tile)
                total = sum(gather(returned, first, part_ref.at[which], a, part) for first, which in bases)
                projected[:, part] = total if a == 0 else projected[:, part] + total

        @pl.when(inner)
        def _():
            add_up([(near_base, my_half)])

        @pl.when(outer)
        def _():
            add_up([(near_base, my_half), (far_base, 1 - my_half)])

    for a in range(count):
        await_blocks(sent, send_sem, a)
        await_blocks(results, back_send, a)

    def finish(combined, piece):
        @pl.loop(piece.start // 16, piece.stop // 16)
        def _(i):
            part = pl.ds(pl.multiple_of(i * 16, 16), 16)
            out_ref[part] = (
                stream_ref[part].astype(jnp.float32) + normed_token_rows(combined(part), gain_ref[...])
            ).astype(jnp.bfloat16)

    @pl.when(inner)
    def _():
        for r in range(2):
            await_bytes(extra_ref.at[pieces[r]], partial_sem.at[1 + r])
            finish(lambda part: projected[part] + extra_ref[part].astype(jnp.float32), pieces[r])
        await_bytes(dense, partial_sem.at[0])

    @pl.when(outer)
    def _():
        finish(lambda part: projected[part], slice(0, rows))


def layer(
    query, key, value, weight, residual, mixer_gain, expert_gain, routes, shares, gate, up, down, gain, groups
):
    sp, dp = lax.axis_size("sp"), lax.axis_size("dp")
    n = sp * dp
    rows, heads, width = query.shape
    depth, columns = weight.shape
    features = residual.shape[1]
    local_heads = heads // sp
    extra = max(dp // 2 - 1, 1)
    slots = n // 2 * sum(groups)
    anywhere = pl.BlockSpec(memory_space=pl.ANY)
    dma = pltpu.SemaphoreType.DMA
    bf16, f32 = jnp.bfloat16, jnp.float32
    return pl.pallas_call(
        functools.partial(layer_kernel, sp, dp, len(groups)),
        out_shape=pltpu.VMEM((rows, features), bf16),
        in_specs=[anywhere] * 13,
        out_specs=pl.BlockSpec(memory_space=pltpu.VMEM),
        scratch_shapes=[pltpu.VMEM((n, g, features), bf16) for _ in range(4) for g in groups]
        + [pltpu.VMEM((n // 2, g, features), bf16) for _ in range(2) for g in groups]
        + [
            pltpu.VMEM((3, rows, heads, width), bf16),
            pltpu.VMEM((rows, features), bf16),
            pltpu.VMEM((1, features), f32),
            pltpu.VMEM((1, features), f32),
            pltpu.VMEM((1, features), f32),
            pltpu.VMEM(routes.shape, jnp.int32),
            pltpu.VMEM(shares.shape, f32),
            pltpu.VMEM((3, heads, rows, width), bf16),
            pltpu.VMEM((3, local_heads, sp, rows, width), bf16),
            pltpu.VMEM((local_heads, sp, rows, width), bf16),
            pltpu.VMEM((local_heads, sp, rows, width), bf16),
            pltpu.VMEM((local_heads, sp, rows // 2, width), bf16),
            pltpu.VMEM(((3 + extra) * (rows // 2), depth), bf16),
            pltpu.VMEM((2 + extra, depth, columns), bf16),
            pltpu.VMEM((extra, rows // 2, columns), bf16),
            pltpu.VMEM((extra, rows // 2, columns), bf16),
            pltpu.VMEM((extra, local_heads, sp, rows // 2, width), bf16),
            pltpu.VMEM((extra, rows // 2, columns), bf16),
            pltpu.VMEM((extra, rows // 2, columns), bf16),
            pltpu.VMEM((rows, features), f32),
            pltpu.VMEM((rows, features), bf16),
            pltpu.VMEM((2, slots, rows), bf16),
            pltpu.VMEM((2, 2 * rows, slots), bf16),
            pltpu.VMEM(gate.shape, bf16),
            pltpu.VMEM(up.shape, bf16),
            pltpu.VMEM(down.shape, bf16),
            pltpu.VMEM(routes.shape, jnp.int32),
            pltpu.VMEM(shares.shape, f32),
            pltpu.VMEM((slots, rows), bf16),
            pltpu.VMEM((2 * rows, slots), bf16),
            pltpu.VMEM((rows, features), bf16),
            pltpu.VMEM((rows, features), bf16),
            dma((10,)),
            dma((local_heads,)),
            dma((local_heads,)),
            dma((local_heads,)),
            dma((local_heads, sp)),
            dma((local_heads,)),
            dma((local_heads,)),
            dma((2,)),
            dma((extra, 2, PIECES)),
            dma((extra, PIECES)),
            dma((extra, PIECES)),
            dma((extra, PIECES)),
            dma((extra,)),
            dma((extra,)),
            dma((4, local_heads)),
            dma((len(groups),)),
            dma((len(groups),)),
            dma((len(groups),)),
            dma((len(groups),)),
            dma((2 * len(groups),)),
            dma((3,)),
            dma((2,)),
            dma((2,)),
            dma((2,)),
            dma((3,)),
            dma((len(groups),)),
            dma((2 * len(groups),)),
            pltpu.SemaphoreType.REGULAR,
            dma((extra, local_heads)),
            dma((extra, local_heads)),
            dma((extra,)),
            dma((extra,)),
        ],
        compiler_params=pltpu.CompilerParams(
            collective_id=0, has_side_effects=True, vmem_limit_bytes=VMEM_LIMIT
        ),
    )(
        query, key, value, weight, residual, mixer_gain[None], expert_gain[None], routes, shares,
        gate, up, down, gain[None],
    )


def local(
    queries,
    key_rows,
    values,
    residual,
    out_weight,
    mixer_gain,
    expert_gain,
    gate_weight,
    up_weight,
    expert_down_matrix,
    routes,
    route_weight,
    output_gain,
):
    local_rows = queries.shape[1]
    experts = lax.axis_size("sp") * lax.axis_size("dp")
    capacity = max(2, 3 * local_rows // experts)
    groups = [g for g in (capacity // 8 * 8, capacity % 8) if g]
    output = layer(
        queries[0], key_rows[0], values[0], out_weight, residual[0], mixer_gain, expert_gain,
        routes[0].T, route_weight[0].T, gate_weight[0], up_weight[0], expert_down_matrix[0], output_gain, groups,
    )
    return output[None]


def solution(mesh):
    in_specs = (
        P("dp", "sp", None, None),
        P("dp", "sp", None, None),
        P("dp", "sp", None, None),
        P("dp", "sp", None),
        P(None, "dp"),
        P(),
        P(),
        P(("sp", "dp"), None, None),
        P(("sp", "dp"), None, None),
        P(("sp", "dp"), None, None),
        P("dp", "sp", None),
        P("dp", "sp", None),
        P(),
    )
    out_specs = P("dp", "sp", None)
    return jax.shard_map(local, mesh=mesh, in_specs=in_specs, out_specs=out_specs, check_vma=False)
```
